32 devices in a mesh: sp: 16 (over z, y, x), tp: 2 (over core).
Axes of the slice: x: 2, y: 2, z: 4, core: 2. Of those that a mesh axis runs over, the one named last changes fastest.
Arguments:
- normed: bfloat16 [4096, 2048], P(('sp', 'tp')), may hold values from -40 to 40
- query_weight: bfloat16 [2048, 2048], P(None, 'tp'), may hold values from -1.5 to 1.5
- key_weight: bfloat16 [2048, 2048], P(None, 'tp'), may hold values from -1 to 1
- value_weight: bfloat16 [2048, 2048], P(None, 'tp'), may hold values from -0.125 to 0.125
- pool_in_weight: bfloat16 [2048, 1024], P(None, 'tp'), may hold values from -0.125 to 0.125
- pool_weight: bfloat16 [8, 128, 128], P('tp'), may hold values from -0.5 to 0.5
- map_balance: float32 [8], replicated, may hold values from 0.3 to 0.8
- head_gain: float32 [256], replicated, may hold values from 0.1 to 1.9
- contrast_out_weight: bfloat16 [2048, 2048], P('tp'), may hold values from -0.109375 to 0.109375
- pool_out_weight: bfloat16 [1024, 2048], P('tp'), may hold values from -0.109375 to 0.109375
Outputs:
- layer_out: bfloat16 [4096, 2048], P(('sp', 'tp'))
The draws below stay inside these ranges and needn't reach their ends.
All inputs are finite; a program needn't handle non-finite values.
Results may differ from the reference program's by a relative error of at most 0.03.
Values may be sent and summed in bfloat16 or wider, within the bound.
A program may use at most 128 MiB of HBM per device.

```python
import math
import jax
import jax.numpy as jnp
from jax import lax

D = 2048
HEADS = 8
HEAD_DIM = 128
GROUPS = 8
GROUP_WIDTH = 128
TOKENS = 4096
N_TP = 2


def shared_keys(key):
    gaussian = jnp.clip(jax.random.normal(jax.random.fold_in(key, 11), (D, 2 * HEADS * HEAD_DIM), jnp.float32), -6.0, 6.0)
    return gaussian * (1.3 / math.sqrt(D))


def draw_key_weight(key, part):
    return shared_keys(key).astype(jnp.bfloat16)


def draw_query_weight(key, part):
    independent = jnp.clip(jax.random.normal(jax.random.fold_in(key, 12), (D, 2 * HEADS * HEAD_DIM), jnp.float32), -6.0, 6.0) * (1.3 / math.sqrt(D))
    aligned = independent
    return aligned.astype(jnp.bfloat16)


def draw_normed(key, part):
    gaussian = jax.random.normal(jax.random.fold_in(key, 21), (TOKENS, D), jnp.float32)
    return jnp.clip(gaussian, -6.0, 6.0).astype(jnp.bfloat16)


def level_of(own_key, dims, pieces, smallest, high):
    def one(dim, parts):
        heights = jax.random.uniform(jax.random.fold_in(jax.random.fold_in(own_key, 6), dim), (parts,), jnp.float32, smallest / len(pieces), high / len(pieces))
        return jnp.repeat(jnp.exp(heights), dims[dim] // parts).reshape((-1,) + (1,) * (len(dims) - dim - 1))

    gain = one(*pieces[0])
    for cut in pieces[1:]:
        gain = gain * one(*cut)
    return gain


def noise(own_key, dims, scale, most, shards=(), held_as=jnp.bfloat16):
    array = jax.random.normal(own_key, dims, jnp.float32) * scale
    if len(shards) > 0:
        array = level_of(own_key, dims, shards, -0.22, 0.18) * array
    return jnp.clip(array, min=-most, max=most).astype(held_as)


def setup_inputs(seed: int = 0) -> dict:
    streams_of = jax.random.split(jax.random.key(seed), 11)
    normed = draw_normed(jax.random.fold_in(streams_of[10], 71), 0)
    query_weight = draw_query_weight(jax.random.fold_in(streams_of[10], 71), 0)
    key_weight = draw_key_weight(jax.random.fold_in(streams_of[10], 71), 0)
    value_weight = noise(streams_of[3], (D, 2 * HEADS * HEAD_DIM), D ** -0.5, 0.125, ((1, 2),))
    pool_in_weight = noise(streams_of[4], (D, GROUPS * GROUP_WIDTH), D ** -0.5, 0.125, ((1, 2),))
    pool_weight = noise(streams_of[5], (GROUPS, GROUP_WIDTH, GROUP_WIDTH), GROUP_WIDTH ** -0.5, 0.5, ((0, 2),))
    map_balance = jnp.clip(jax.random.uniform(streams_of[6], (HEADS,), jnp.float32, 0.3, 0.8), 0.3, 0.8)
    head_gain = jnp.clip(1.0 + 0.18 * jax.random.normal(streams_of[7], (2 * HEAD_DIM,), jnp.float32), 0.1, 1.9)
    contrast_out_weight = noise(streams_of[8], (2 * HEADS * HEAD_DIM, D), (2 * HEADS * HEAD_DIM + GROUPS * GROUP_WIDTH) ** -0.5, 0.109375, ((0, 2),))
    pool_out_weight = noise(streams_of[9], (GROUPS * GROUP_WIDTH, D), (2 * HEADS * HEAD_DIM + GROUPS * GROUP_WIDTH) ** -0.5, 0.109375, ((0, 2),))
    return {"normed": normed, "query_weight": query_weight, "key_weight": key_weight, "value_weight": value_weight, "pool_in_weight": pool_in_weight, "pool_weight": pool_weight, "map_balance": map_balance, "head_gain": head_gain, "contrast_out_weight": contrast_out_weight, "pool_out_weight": pool_out_weight}


reach_back = 15
norm_epsilon = 1e-06

def map_output(queries, key_rows, value_rows):
    total_rows = queries.shape[0]
    block_rows = math.gcd(total_rows, 1024)
    score_scale = HEAD_DIM ** (-0.5)
    outputs = []
    for block_index in range(total_rows // block_rows):
        first_row = block_index * block_rows
        last_row = first_row + block_rows
        scores = jnp.dot(queries[first_row:last_row], key_rows[:last_row].T, preferred_element_type=jnp.float32) * score_scale
        query_order = first_row + jnp.arange(block_rows, dtype=jnp.int32)
        key_order = jnp.arange(last_row, dtype=jnp.int32)
        scores = jnp.where(key_order[None, :] <= query_order[:, None], scores, -jnp.inf)
        row_peak = lax.optimization_barrier(jnp.max(scores, axis=1, keepdims=True))
        raised = jnp.exp(scores - row_peak)
        row_total = lax.optimization_barrier(jnp.sum(raised, axis=1, keepdims=True))
        weighted = jnp.dot(raised.astype(jnp.bfloat16), value_rows[:last_row], preferred_element_type=jnp.float32)
        outputs.append((weighted / row_total).astype(jnp.bfloat16))
    return jnp.concatenate(outputs, axis=0)

def reference(normed, query_weight, key_weight, value_weight, pool_in_weight, pool_weight, map_balance, head_gain, contrast_out_weight, pool_out_weight):
    queries = jnp.dot(normed, query_weight, preferred_element_type=jnp.float32).astype(jnp.bfloat16)
    key_rows = jnp.dot(normed, key_weight, preferred_element_type=jnp.float32).astype(jnp.bfloat16)
    value_rows = jnp.dot(normed, value_weight, preferred_element_type=jnp.float32).astype(jnp.bfloat16)
    pool_input = jnp.dot(normed, pool_in_weight, preferred_element_type=jnp.float32).astype(jnp.bfloat16)
    value_width = 2 * HEAD_DIM
    head_outputs = []
    for head in range(HEADS):
        maps = []
        for which in range(2):
            column = (2 * head + which) * HEAD_DIM
            result_map = map_output(queries[:, column:column + HEAD_DIM], key_rows[:, column:column + HEAD_DIM], value_rows[:, head * value_width:(head + 1) * value_width])
            maps.append(lax.optimization_barrier(result_map).astype(jnp.float32))
        contrast = maps[0] - map_balance[head] * maps[1]
        mean_square = lax.optimization_barrier(jnp.mean(contrast * contrast, axis=1, keepdims=True))
        head_outputs.append((contrast * lax.rsqrt(mean_square + norm_epsilon) * head_gain).astype(jnp.bfloat16))
    contrast_out = jnp.concatenate(head_outputs, axis=1)
    total_rows = normed.shape[0]
    pool_width = GROUPS * GROUP_WIDTH
    extended = jnp.concatenate([jnp.zeros((reach_back, pool_width), jnp.float32), pool_input.astype(jnp.float32)], axis=0)
    group_index = jnp.arange(pool_width, dtype=jnp.int32) // GROUP_WIDTH
    widths = jnp.left_shift(jnp.int32(2), group_index % 4)
    window_sum = jnp.zeros((total_rows, pool_width), jnp.float32)
    for offset in range(reach_back + 1):
        window_sum = window_sum + extended[reach_back - offset:reach_back - offset + total_rows] * (offset < widths)[None, :].astype(jnp.float32)
    position = jnp.arange(total_rows, dtype=jnp.int32)
    counts = jnp.minimum(position[:, None] + 1, widths[None, :]).astype(jnp.float32)
    spread = (window_sum / counts - extended[reach_back:]).astype(jnp.bfloat16)
    spread = lax.optimization_barrier(spread).astype(jnp.float32)
    mixed_groups = jnp.einsum('sgc,gce->sge', spread.reshape(total_rows, GROUPS, GROUP_WIDTH), pool_weight.astype(jnp.float32))
    pool_out = mixed_groups.reshape(total_rows, pool_width).astype(jnp.bfloat16)
    diff_rows = 2 * HEADS * HEAD_DIM // N_TP
    pool_rows = GROUPS * GROUP_WIDTH // N_TP
    summed = jnp.zeros((total_rows, D), jnp.float32)
    for part_index in range(N_TP):
        low_diff = part_index * diff_rows
        low_pool = part_index * pool_rows
        partial_value = jnp.dot(contrast_out[:, low_diff:low_diff + diff_rows], contrast_out_weight[low_diff:low_diff + diff_rows], preferred_element_type=jnp.float32)
        partial_value = partial_value + jnp.dot(pool_out[:, low_pool:low_pool + pool_rows], pool_out_weight[low_pool:low_pool + pool_rows], preferred_element_type=jnp.float32)
        summed = summed + lax.optimization_barrier(partial_value.astype(jnp.bfloat16)).astype(jnp.float32)
    return summed.astype(jnp.bfloat16)
```

```python
import functools
import math

import jax
import jax.numpy as jnp
from jax import lax
from jax.experimental import pallas as pl
from jax.experimental.pallas import tpu as pltpu
from jax.sharding import PartitionSpec as P

reach_back = 15
norm_epsilon = 1e-06


def passed_along(block, axis, distance):
    devices = range(lax.axis_size(axis))
    route = [(i - distance, i) for i in devices if i - distance in devices]
    return lax.ppermute(block, axis, route)


def from_partner(block, axis, stride):
    count = lax.axis_size(axis)
    route = []
    for low in range(count):
        high = low | 1 << stride
        if high != low and high < count:
            route += [(low, high), (high, low)]
    return lax.ppermute(block, axis, route)


def shifted(array, axis, by):
    size = lax.axis_size(axis)
    return lax.ppermute(array, axis, [(i, (i + by) % size) for i in range(size)])


def as_sent(array):

    def short(part):
        return part.astype(jnp.bfloat16) if part.dtype == jnp.float32 else part

    return jax.tree.map(short, array)


def attend(running, queries, key_rows, value_rows, query_first, key_first, score_scale):
    key_count = key_rows.shape[0]
    key_block = math.gcd(key_count, 1024)
    unit_count = queries.shape[1]
    heads_here = value_rows.shape[1]
    per_head = unit_count // heads_here
    query_count = queries.shape[0]
    query_order = query_first + lax.iota(jnp.int32, query_count)

    def key_step(block_index, carried):
        block_start = block_index * key_block

        def block_work(current):
            row_peak, row_total, weighted = current
            scores = (
                jnp.einsum("qud,kud->uqk", queries, key_rows, preferred_element_type=jnp.float32)
                * score_scale
            )
            key_order = key_first + block_start + lax.iota(jnp.int32, key_block)
            scores = jnp.where(
                key_order[None, None, :] <= query_order[None, :, None], scores, -jnp.inf
            )
            new_peak = jnp.maximum(row_peak, jnp.max(scores, axis=2))
            shrink = jnp.exp(row_peak - new_peak)
            raised = jnp.exp(scores - new_peak[:, :, None])
            row_total = row_total * shrink + jnp.sum(raised, axis=2)
            map_weights = raised.astype(jnp.bfloat16).reshape(
                heads_here, per_head, query_count, key_block
            )
            update = jnp.einsum(
                "hmqk,khe->hmqe", map_weights, value_rows, preferred_element_type=jnp.float32
            )
            weighted = weighted * shrink[:, :, None] + update.reshape(unit_count, query_count, -1)
            return (new_peak, row_total, weighted)

        def keep_state(current):
            return current

        return lax.cond(
            key_first + block_start <= query_first + query_count - 1,
            block_work,
            keep_state,
            carried,
        )

    return lax.fori_loop(0, key_count // key_block, key_step, running)


def fresh_state(unit_count, row_count, value_width):
    return (
        jnp.full((unit_count, row_count), -1e30, jnp.float32),
        jnp.zeros((unit_count, row_count), jnp.float32),
        jnp.zeros((unit_count, row_count, value_width), jnp.float32),
    )


def finished(running):
    row_peak, row_total, weighted = running
    return (weighted / row_total[:, :, None]).astype(jnp.bfloat16)


def joined_state(first, second):
    first_peak, first_total, first_weighted = first
    second_peak, second_total, second_weighted = second
    new_peak = jnp.maximum(first_peak, second_peak)
    first_shrink = jnp.exp(first_peak - new_peak)
    second_shrink = jnp.exp(second_peak - new_peak)
    new_total = first_total * first_shrink + second_total * second_shrink
    new_weighted = (
        first_weighted * first_shrink[:, :, None] + second_weighted * second_shrink[:, :, None]
    )
    return (new_peak, new_total, new_weighted)


def per_device(
    normed,
    query_weight,
    key_weight,
    value_weight,
    pool_in_weight,
    pool_weight,
    map_balance,
    head_gain,
    contrast_out_weight,
    pool_out_weight,
):
    tp_index = lax.axis_index("tp")
    sp_count = lax.axis_size("sp")
    sp_index = lax.axis_index("sp")
    head_dim = head_gain.shape[0] // 2
    value_width = 2 * head_dim
    query_cols = query_weight.shape[1]
    value_cols = value_weight.shape[1]
    unit_count = query_cols // head_dim
    heads_here = unit_count // 2
    project_incoming = lax.all_gather(normed, "tp", axis=0, tiled=True)
    products = [
        jnp.dot(project_incoming, weight_part, preferred_element_type=jnp.float32)
        for weight_part in (query_weight, key_weight, value_weight, pool_in_weight)
    ]
    joined = jnp.concatenate(products, axis=1).astype(jnp.bfloat16)
    row_count = joined.shape[0]
    queries = joined[:, :query_cols].reshape(row_count, unit_count, head_dim)
    key_rows = joined[:, query_cols : 2 * query_cols].reshape(row_count, unit_count, head_dim)
    value_rows = joined[:, 2 * query_cols : 2 * query_cols + value_cols].reshape(
        row_count, heads_here, value_width
    )
    pool_input = joined[:, 2 * query_cols + value_cols :]
    pool_cols = pool_input.shape[1]
    upper_rim = passed_along(pool_input[row_count - reach_back :], "sp", 1)
    extended = jnp.concatenate([upper_rim, pool_input], axis=0).astype(jnp.float32)
    groups_here = pool_weight.shape[0]
    group_width = pool_weight.shape[1]
    group_index = tp_index * groups_here + lax.iota(jnp.int32, pool_cols) // group_width
    widths = jnp.left_shift(jnp.int32(2), group_index % 4)
    window_sum = jnp.zeros((row_count, pool_cols), jnp.float32)
    for offset in range(reach_back + 1):
        window_sum = window_sum + extended[
            reach_back - offset : reach_back - offset + row_count
        ] * (offset < widths)[None, :].astype(jnp.float32)
    position = sp_index * row_count + lax.iota(jnp.int32, row_count)
    counts = jnp.minimum(position[:, None] + 1, widths[None, :]).astype(jnp.float32)
    spread = (window_sum / counts - extended[reach_back:]).astype(jnp.bfloat16)
    mixed_groups = jnp.einsum(
        "tgc,gce->tge",
        spread.reshape(row_count, groups_here, group_width),
        pool_weight,
        preferred_element_type=jnp.float32,
    )
    pool_out = mixed_groups.reshape(row_count, pool_cols).astype(jnp.bfloat16)
    score_scale = head_dim ** (-0.5)
    level_count = sp_count.bit_length() - 1
    low_levels = level_count // 2
    band_size = 1 << low_levels
    band_count = sp_count // band_size
    member = sp_index % band_size
    band = sp_index // band_size
    band_queries = queries
    for bit in range(low_levels):
        received = from_partner(band_queries, "sp", bit)
        upper = member >> bit & 1 == 1
        band_queries = jnp.where(
            upper,
            jnp.concatenate([received, band_queries], axis=0),
            jnp.concatenate([band_queries, received], axis=0),
        )
    band_first = band * band_size * row_count
    running = fresh_state(unit_count, band_size * row_count, value_width)
    for step in range(band_count):
        if step == 0:
            key_piece, value_piece = (key_rows, value_rows)
        else:
            key_piece, value_piece = shifted((key_rows, value_rows), "sp", step * band_size)
        source = (sp_index - step * band_size) % sp_count
        running = attend(
            running,
            band_queries,
            key_piece,
            value_piece,
            band_first,
            source * row_count,
            score_scale,
        )
    for bit in range(low_levels - 1, -1, -1):
        half = running[0].shape[1] // 2
        upper = member >> bit & 1 == 1
        lower_part = jax.tree.map(lambda item: item[:, :half], running)
        upper_part = jax.tree.map(lambda item: item[:, half:], running)
        outgoing = jax.tree.map(
            lambda low, high: jnp.where(upper, low, high), lower_part, upper_part
        )
        kept = jax.tree.map(lambda low, high: jnp.where(upper, high, low), lower_part, upper_part)
        incoming = from_partner(
            (as_sent(outgoing[0]), as_sent(outgoing[1]), as_sent(outgoing[2])), "sp", bit
        )
        running = joined_state(kept, incoming)
    maps = finished(running)
    paired = maps.reshape(heads_here, 2, row_count, value_width)
    paired = lax.optimization_barrier(paired).astype(jnp.float32)
    head_first = tp_index * heads_here
    balance_here = lax.dynamic_slice_in_dim(map_balance, head_first, heads_here, 0)
    contrast = paired[:, 0] - balance_here[:, None, None] * paired[:, 1]
    mean_square = jnp.mean(contrast * contrast, axis=2, keepdims=True)
    contrast = contrast * lax.rsqrt(mean_square + norm_epsilon) * head_gain
    contrast_out = (
        contrast.astype(jnp.bfloat16)
        .transpose(1, 0, 2)
        .reshape(row_count, heads_here * value_width)
    )
    partial_value = jnp.dot(contrast_out, contrast_out_weight, preferred_element_type=jnp.float32)
    return lax.psum_scatter(
        (
            partial_value + jnp.dot(pool_out, pool_out_weight, preferred_element_type=jnp.float32)
        ).astype(jnp.bfloat16),
        "tp",
        scatter_dimension=0,
        tiled=True,
    )


MESH = pl.DeviceIdType.MESH


def layer_kernel(
    sp_count,
    members,
    x_ref,
    pool_weight,
    balance,
    gain,
    query_hbm,
    key_hbm,
    value_hbm,
    pool_in_hbm,
    contrast_hbm,
    pool_out_hbm,
    out_ref,
    out_recv,
    query_w,
    key_w,
    value_w,
    pool_in_w,
    contrast_w,
    pool_out_w,
    rows_in,
    kv,
    kv_stage,
    queries,
    query_stage,
    peaks,
    totals,
    weighted,
    contrasts,
    contrast_stage,
    rim,
    rim_stage,
    pool_part,
    out_stage,
    weight_sem,
    local_sem,
    pair_send,
    pair_recv,
    relay_send,
    relay_recv,
    kv_send,
    kv_recv,
    forward_send,
    query_send,
    query_recv,
    contrast_send,
    contrast_recv,
    rim_send,
    rim_recv,
    out_send,
    out_recv_sem,
):
    f32 = jnp.float32
    bf16 = jnp.bfloat16
    sp = lax.axis_index("sp")
    tp = lax.axis_index("tp")
    other = 1 - tp
    plane = lax.div(sp, members)
    member = lax.rem(sp, members)
    upper = lax.div(plane, 2)
    side = lax.rem(plane, 2)
    across = lax.div(member, 2)
    along = lax.rem(member, 2)
    half_count = 2 * members
    half, model = x_ref.shape
    rows = 2 * half
    width = gain.shape[1]
    head_dim = width // 2
    chunks = 2
    piece = half // chunks
    in_lower = upper == 0
    in_upper = upper == 1
    crosses = plane == 1
    relays = plane == 2
    query_band = 2 * upper + tp
    bands_of = (plane, plane + 1 - 2 * side, jnp.int32(1), jnp.int32(0))

    half_columns = pl.ds(pl.multiple_of(side * 2 * width, 2 * width), 2 * width)
    loads = [
        pltpu.make_async_copy(src, dst, weight_sem.at[i])
        for i, (src, dst) in enumerate(
            (
                (key_hbm.at[:, half_columns], key_w),
                (value_hbm.at[:, half_columns], value_w),
                (query_hbm.at[:, half_columns], query_w),
                (pool_in_hbm, pool_in_w),
                (pool_out_hbm, pool_out_w),
                (contrast_hbm, contrast_w),
            )
        )
    ]
    for load in loads:
        load.start()
    keep = pltpu.make_async_copy(x_ref, rows_in.at[0, tp], local_sem)
    keep.start()

    barrier = pltpu.get_barrier_semaphore()

    def greet(target):
        pl.semaphore_signal(barrier, inc=1, device_id=target, device_id_type=MESH)

    place = (side * members + member) * 2 + tp
    for d in range(1, 2 * half_count):
        goal = lax.rem(place + d, 2 * half_count)
        greet((upper * half_count + lax.div(goal, 2), lax.rem(goal, 2)))

    @pl.when(crosses)
    def _():
        greet((sp + members, tp))

    @pl.when(relays)
    def _():
        greet((sp - members, tp))

    @pl.when(sp == half_count - 1)
    def _():
        greet((sp + 1, tp))

    @pl.when(sp == half_count)
    def _():
        greet((sp - 1, tp))

    extra = jnp.where(jnp.logical_or(crosses, relays), 1, 0)
    extra = extra + jnp.where(jnp.logical_or(sp == half_count - 1, sp == half_count), 1, 0)
    pl.semaphore_wait(barrier, 2 * half_count - 1 + extra)

    def cut(ch):
        return pl.ds(ch * piece, piece)

    pair_first = pltpu.make_async_remote_copy(
        src_ref=x_ref,
        dst_ref=rows_in.at[0, tp],
        send_sem=pair_send.at[0, 0],
        recv_sem=pair_recv.at[0, 0],
        device_id=(sp, other),
        device_id_type=MESH,
    )

    def pair_copy(step, ch):
        return pltpu.make_async_remote_copy(
            src_ref=rows_in.at[step, tp, cut(ch)],
            dst_ref=rows_in.at[step, tp, cut(ch)],
            send_sem=pair_send.at[step, ch],
            recv_sem=pair_recv.at[step, ch],
            device_id=(sp, other),
            device_id_type=MESH,
        )

    def relay_copy(src, step, ch, target):
        return pltpu.make_async_remote_copy(
            src_ref=src.at[cut(ch)],
            dst_ref=rows_in.at[step, tp, cut(ch)],
            send_sem=relay_send.at[step, ch],
            recv_sem=relay_recv.at[step, ch],
            device_id=(target, tp),
            device_id_type=MESH,
        )

    def swap(ch):
        return relay_copy(x_ref, 1, ch, sp + members * (1 - 2 * side))

    def own_up(ch):
        return relay_copy(x_ref, 2, ch, sp + members)

    def low_up(ch):
        return relay_copy(rows_in.at[1, tp], 3, ch, sp + members)

    def pass_up(step, ch):
        return relay_copy(rows_in.at[step, tp], step, ch, sp + members)

    def top(step):
        if step == 0:
            return side == 1
        if step == 1:
            return side == 0
        return jnp.bool_(False)

    def kv_copy(step, j):
        goal = 2 * tp + j
        first = jnp.where(top(step), 1, along)
        return pltpu.make_async_remote_copy(
            src_ref=kv_stage.at[step, j],
            dst_ref=kv.at[step, member],
            send_sem=kv_send.at[step, j],
            recv_sem=kv_recv.at[step, member],
            device_id=(plane * members + goal, first),
            device_id_type=MESH,
        )

    def forward_copy(step, source):
        return pltpu.make_async_remote_copy(
            src_ref=kv.at[step, source],
            dst_ref=kv.at[step, source],
            send_sem=forward_send.at[step, source],
            recv_sem=kv_recv.at[step, source],
            device_id=(sp, other),
            device_id_type=MESH,
        )

    def query_copy(step, j):
        core = jnp.where(top(step), 1, 0)
        return pltpu.make_async_remote_copy(
            src_ref=query_stage.at[step, j],
            dst_ref=queries.at[member],
            send_sem=query_send.at[step, j],
            recv_sem=query_recv.at[member],
            device_id=(plane * members + 2 * tp + j, core),
            device_id_type=MESH,
        )

    own_goal = across == tp

    def own_stays(step, j):
        return jnp.logical_and(own_goal, j == along)

    def query_stays(step, j):
        return jnp.logical_and(own_stays(step, j), jnp.where(top(step), 1, 0) == tp)

    def own_forwards(step):
        return jnp.logical_and(
            own_goal, jnp.logical_or(jnp.logical_not(top(step)), tp == 0)
        )

    def passes_on(step, source):
        mine = jnp.logical_and(source % 2 == tp, jnp.logical_not(top(step)))
        return jnp.logical_and(source != member, mine)

    def awaits(step, source):
        needed = jnp.logical_or(tp == 1, jnp.logical_not(top(step)))
        made_here = jnp.logical_and(source == member, own_goal)
        return jnp.logical_and(needed, jnp.logical_not(made_here))

    def contrast_stays(i):
        return jnp.logical_and(
            jnp.logical_and(query_band == plane, i == member), across == tp
        )

    head_here = 2 * side + along

    def contrast_copy(i):
        return pltpu.make_async_remote_copy(
            src_ref=contrast_stage.at[i],
            dst_ref=contrasts.at[head_here],
            send_sem=contrast_send.at[i],
            recv_sem=contrast_recv.at[head_here],
            device_id=(query_band * members + i, across),
            device_id_type=MESH,
        )

    def contrast_incoming(head):
        return pltpu.make_async_remote_copy(
            src_ref=contrast_stage.at[0],
            dst_ref=contrasts.at[head],
            send_sem=contrast_send.at[0],
            recv_sem=contrast_recv.at[head],
            device_id=(sp, other),
            device_id_type=MESH,
        )

    def contrast_local(head):
        same = jnp.logical_and(head // 2 == side, 2 * tp + head % 2 == member)
        return jnp.logical_and(same, side == tp)

    rim_copy = pltpu.make_async_remote_copy(
        src_ref=rim_stage,
        dst_ref=rim,
        send_sem=rim_send,
        recv_sem=rim_recv,
        device_id=(lax.rem(sp + 1, sp_count), tp),
        device_id_type=MESH,
    )
    out_copy = pltpu.make_async_remote_copy(
        src_ref=out_stage,
        dst_ref=out_recv,
        send_sem=out_send,
        recv_sem=out_recv_sem,
        device_id=(sp, other),
        device_id_type=MESH,
    )

    pair_first.start()
    for ch in range(chunks):
        swap(ch).start()

        @pl.when(crosses)
        def _(ch=ch):
            own_up(ch).start()

    peaks[...] = jnp.full(peaks.shape, -1e30, f32)
    totals[...] = jnp.zeros(totals.shape, f32)
    weighted[...] = jnp.zeros(weighted.shape, f32)

    def project(step):
        def one(t, carry):
            j = jnp.where(t == 0, 1 - along, along)
            columns = pl.ds(pl.multiple_of(j * width, width), width)
            x = rows_in[step].reshape(rows, model)
            keys = jnp.dot(x, key_w[:, columns], preferred_element_type=f32).astype(bf16)
            values = jnp.dot(x, value_w[:, columns], preferred_element_type=f32).astype(bf16)
            stays = own_stays(step, j)

            @pl.when(jnp.logical_not(stays))
            def _():
                kv_stage[step, j, :, :width] = keys
                kv_stage[step, j, :, width:] = values
                kv_copy(step, j).start()

            @pl.when(stays)
            def _():
                kv[step, member, :, :width] = keys
                kv[step, member, :, width:] = values

                @pl.when(own_forwards(step))
                def _():
                    forward_copy(step, member).start()

            if step < 2:
                mine = jnp.dot(x, query_w[:, columns], preferred_element_type=f32).astype(bf16)
                kept = query_stays(step, j)

                @pl.when(jnp.logical_not(kept))
                def _():
                    query_stage[step, j] = mine
                    query_copy(step, j).start()

                @pl.when(kept)
                def _():
                    queries[member] = mine

            return carry

        lax.fori_loop(0, 2, one, 0)

    def take_swap(ch):
        swap(ch).wait_recv()

        @pl.when(crosses)
        def _():
            low_up(ch).start()

        pair_copy(1, ch).start()

    def take_far(step, ch):
        pass_up(step, ch).wait_recv()

        @pl.when(relays)
        def _():
            pass_up(step, ch).start()

        pair_copy(step, ch).start()

    def paired(step):
        for ch in range(chunks):
            pair_copy(step, ch).wait_recv()

    log_scale = head_dim ** (-0.5) * math.log2(math.e)

    def attend_block(step, i, seen, masked):
        for u in range(2):
            cols = slice(u * head_dim, (u + 1) * head_dim)
            keys = kv[step, :seen, :, cols].reshape(seen * rows, head_dim)
            values = kv[step, :seen, :, width:].reshape(seen * rows, width)
            scores = lax.dot_general(
                queries[i, :, cols], keys, (((1,), (1,)), ((), ())), preferred_element_type=f32
            )
            if masked:
                query_order = lax.broadcasted_iota(jnp.int32, scores.shape, 0) + (seen - 1) * rows
                key_order = lax.broadcasted_iota(jnp.int32, scores.shape, 1)
                scores = jnp.where(key_order <= query_order, scores, -jnp.inf)
            old = peaks[u, i][:, :1]
            peak = jnp.maximum(jnp.max(scores, axis=1, keepdims=True), old)
            shrink = jnp.exp2((old - peak) * log_scale)
            raised = jnp.exp2((scores - peak) * log_scale)
            total = jnp.sum(raised, axis=1, keepdims=True)
            update = jnp.dot(raised.astype(bf16), values, preferred_element_type=f32)
            total = total + totals[u, i][:, :1] * shrink
            update = update + weighted[u, i] * shrink
            peaks[u, i] = jnp.broadcast_to(peak, peaks.shape[2:])
            totals[u, i] = jnp.broadcast_to(total, totals.shape[2:])
            weighted[u, i] = update

    weight = balance[across * members + head_here]

    def finish(i):
        first = (weighted[0, i] / totals[0, i][:, :1]).astype(bf16).astype(f32)
        second = (weighted[1, i] / totals[1, i][:, :1]).astype(bf16).astype(f32)
        contrast = first - weight * second
        mean_square = jnp.mean(contrast * contrast, axis=1, keepdims=True)
        result = (contrast * lax.rsqrt(mean_square + norm_epsilon) * gain[...]).astype(bf16)
        stays = contrast_stays(i)

        @pl.when(jnp.logical_not(stays))
        def _():
            contrast_stage[i] = result
            contrast_copy(i).start()

        @pl.when(stays)
        def _():
            contrasts[head_here] = result

    def each_block(work):
        def one(t, carry):
            work(lax.rem(member + 1 + t, members))
            return carry

        lax.fori_loop(0, members, one, 0)

    def arrive(step):
        for source in range(members):

            @pl.when(awaits(step, source))
            def _(source=source):
                forward_copy(step, source).wait_recv()

            @pl.when(passes_on(step, source))
            def _(source=source):
                forward_copy(step, source).start()

    def attend(step):
        band = bands_of[step]
        arrive(step)

        if step < 2:

            @pl.when(band == query_band)
            def _():
                for i in range(members):
                    attend_block(step, i, i + 1, True)

        @pl.when(band < query_band)
        def _():
            def work(i):
                attend_block(step, i, members, False)
                if step == 3:
                    finish(i)

            each_block(work)

    keep.wait()
    loads[0].wait()
    loads[1].wait()
    loads[2].wait()
    pair_first.wait_recv()
    project(0)

    loads[3].wait()
    pool_input = jnp.dot(
        rows_in[0].reshape(rows, model), pool_in_w[...], preferred_element_type=f32
    ).astype(bf16)
    rim_stage[...] = pool_input[rows - rim.shape[0] :]

    @pl.when(sp + 1 < sp_count)
    def _():
        rim_copy.start()

    for ch in range(chunks):
        take_swap(ch)

        @pl.when(relays)
        def _(ch=ch):
            take_far(2, ch)

    paired(1)
    project(1)

    @pl.when(sp > 0)
    def _():
        rim_copy.wait_recv()

    @pl.when(sp == 0)
    def _():
        rim[...] = jnp.zeros_like(rim)

    loads[4].wait()
    extended = jnp.concatenate([rim[...], pool_input], axis=0).astype(f32)
    group_width = pool_weight.shape[1]
    skirt = rim.shape[0]
    position = sp * rows + lax.broadcasted_iota(jnp.int32, (rows, group_width), 0)
    mixed = []
    for group in range(pool_weight.shape[0]):
        block = extended[:, group * group_width : (group + 1) * group_width]
        window = block
        reach = 1
        span = 2 ** (1 + group % 4)
        while reach < span:
            window = window + pltpu.roll(window, reach, 0)
            reach *= 2
        counts = jnp.minimum(position + 1, span).astype(f32)
        spread = (window[skirt:] / counts - block[skirt:]).astype(bf16)
        mixed.append(
            jnp.dot(spread, pool_weight[group], preferred_element_type=f32).astype(bf16)
        )
    pool_out = jnp.concatenate(mixed, axis=1)
    chunk = math.gcd(model, 512)
    for start in range(0, model, chunk):
        pool_part[:, start : start + chunk] = jnp.dot(
            pool_out, pool_out_w[:, start : start + chunk], preferred_element_type=f32
        )

    def query_incoming(source):
        return pltpu.make_async_remote_copy(
            src_ref=query_stage.at[0, 0],
            dst_ref=queries.at[source],
            send_sem=query_send.at[0, 0],
            recv_sem=query_recv.at[source],
            device_id=(sp, other),
            device_id_type=MESH,
        )

    def take_queries():
        for source in range(members):

            @pl.when(jnp.logical_not(jnp.logical_and(source == member, own_goal)))
            def _(source=source):
                query_incoming(source).wait_recv()

    take_queries()
    attend(0)

    @pl.when(in_upper)
    def _():
        @pl.when(jnp.logical_not(relays))
        def _():
            for ch in range(chunks):
                take_far(2, ch)

        paired(2)
        project(2)

        @pl.when(relays)
        def _():
            for ch in range(chunks):
                take_far(3, ch)

    attend(1)

    @pl.when(in_lower)
    def _():
        each_block(finish)

    @pl.when(in_upper)
    def _():
        @pl.when(jnp.logical_not(relays))
        def _():
            for ch in range(chunks):
                take_far(3, ch)

        paired(3)
        project(3)
        attend(2)
        attend(3)

    loads[5].wait()
    for head in range(members):

        @pl.when(jnp.logical_not(contrast_local(head)))
        def _(head=head):
            contrast_incoming(head).wait_recv()

    def projected(taken_side, store):
        taken = pl.ds(pl.multiple_of(taken_side * half, half), half)
        left = jnp.concatenate([contrasts[h, taken, :] for h in range(members)], axis=1)
        for start in range(0, model, chunk):
            span = slice(start, start + chunk)
            part = jnp.dot(left, contrast_w[:, span], preferred_element_type=f32)
            store(span, (part + pool_part[taken, span]).astype(bf16))

    def to_partner(span, part):
        out_stage[:, span] = part

    def to_self(span, part):
        out_ref[:, span] = part

    projected(other, to_partner)
    out_copy.start()
    projected(tp, to_self)
    out_copy.wait()

    pair_first.wait_send()
    for ch in range(chunks):
        swap(ch).wait_send()
        pair_copy(1, ch).wait_send()

        @pl.when(crosses)
        def _(ch=ch):
            own_up(ch).wait_send()
            low_up(ch).wait_send()

        @pl.when(relays)
        def _(ch=ch):
            pass_up(2, ch).wait_send()
            pass_up(3, ch).wait_send()

        @pl.when(in_upper)
        def _(ch=ch):
            pair_copy(2, ch).wait_send()
            pair_copy(3, ch).wait_send()

    def drain(step):
        for j in range(2):

            @pl.when(jnp.logical_not(own_stays(step, j)))
            def _(j=j):
                kv_copy(step, j).wait_send()

            if step < 2:

                @pl.when(jnp.logical_not(query_stays(step, j)))
                def _(j=j):
                    query_copy(step, j).wait_send()

        @pl.when(own_forwards(step))
        def _():
            forward_copy(step, member).wait_send()

        for source in range(members):

            @pl.when(passes_on(step, source))
            def _(source=source):
                forward_copy(step, source).wait_send()

    drain(0)
    drain(1)

    @pl.when(in_upper)
    def _():
        drain(2)
        drain(3)

    for i in range(members):

        @pl.when(jnp.logical_not(contrast_stays(i)))
        def _(i=i):
            contrast_copy(i).wait_send()

    @pl.when(sp + 1 < sp_count)
    def _():
        rim_copy.wait_send()


def kernel_scratch(members, half, model, width, pool_cols):
    bf16 = jnp.bfloat16
    rows = 2 * half
    dma = pltpu.SemaphoreType.DMA
    return [
        pltpu.VMEM((model, 2 * width), bf16),
        pltpu.VMEM((model, 2 * width), bf16),
        pltpu.VMEM((model, 2 * width), bf16),
        pltpu.VMEM((model, pool_cols), bf16),
        pltpu.VMEM((members * width, model), bf16),
        pltpu.VMEM((pool_cols, model), bf16),
        pltpu.VMEM((4, 2, half, model), bf16),
        pltpu.VMEM((4, members, rows, 2 * width), bf16),
        pltpu.VMEM((4, 2, rows, 2 * width), bf16),
        pltpu.VMEM((members, rows, width), bf16),
        pltpu.VMEM((2, 2, rows, width), bf16),
        pltpu.VMEM((2, members, rows, 128), jnp.float32),
        pltpu.VMEM((2, members, rows, 128), jnp.float32),
        pltpu.VMEM((2, members, rows, width), jnp.float32),
        pltpu.VMEM((members, rows, width), bf16),
        pltpu.VMEM((members, rows, width), bf16),
        pltpu.VMEM((reach_back + 1, pool_cols), bf16),
        pltpu.VMEM((reach_back + 1, pool_cols), bf16),
        pltpu.VMEM((rows, model), jnp.float32),
        pltpu.VMEM((half, model), bf16),
        dma((6,)),
        dma,
        dma((4, 2)),
        dma((4, 2)),
        dma((4, 2)),
        dma((4, 2)),
        dma((4, 2)),
        dma((4, members)),
        dma((4, members)),
        dma((2, 2)),
        dma((members,)),
        dma((members,)),
        dma((members,)),
        dma,
        dma,
        dma,
        dma,
    ]


vmem_most = 67043328


def scratch_bytes(scratch):
    return sum(
        math.prod(item.shape) * jnp.dtype(item.dtype).itemsize
        for item in scratch
        if getattr(item, "memory_space", None) == pltpu.VMEM
    )


def whole_layer(
    normed,
    query_weight,
    key_weight,
    value_weight,
    pool_in_weight,
    pool_weight,
    map_balance,
    head_gain,
    contrast_out_weight,
    pool_out_weight,
):
    sp_count = lax.axis_size("sp")
    width = head_gain.shape[0]
    members = query_weight.shape[1] // width
    half, model = normed.shape
    pool_cols = pool_in_weight.shape[1]
    groups_here = pool_weight.shape[0]
    scratch = kernel_scratch(max(members, 1), half, model, width, pool_cols)
    fits = (
        lax.axis_size("tp") == 2
        and members == 4
        and sp_count == 4 * members
        and groups_here % 4 == 0
        and scratch_bytes(scratch) < vmem_most * 3 // 4
    )
    if not fits:
        return per_device(
            normed,
            query_weight,
            key_weight,
            value_weight,
            pool_in_weight,
            pool_weight,
            map_balance,
            head_gain,
            contrast_out_weight,
            pool_out_weight,
        )
    vmem = pl.BlockSpec(memory_space=pltpu.VMEM)
    hbm = pl.BlockSpec(memory_space=pl.ANY)
    own_part, partner_part = pl.pallas_call(
        functools.partial(layer_kernel, sp_count, members),
        out_shape=[jax.ShapeDtypeStruct((half, model), jnp.bfloat16)] * 2,
        in_specs=[vmem, vmem, pl.BlockSpec(memory_space=pltpu.SMEM), vmem] + [hbm] * 6,
        out_specs=[vmem, vmem],
        scratch_shapes=scratch,
        compiler_params=pltpu.CompilerParams(
            collective_id=0, has_side_effects=True, vmem_limit_bytes=vmem_most
        ),
    )(
        normed,
        pool_weight,
        map_balance,
        head_gain.reshape(1, width),
        query_weight,
        key_weight,
        value_weight,
        pool_in_weight,
        contrast_out_weight,
        pool_out_weight,
    )
    return (own_part.astype(jnp.float32) + partner_part.astype(jnp.float32)).astype(jnp.bfloat16)


def solution(mesh):
    return jax.shard_map(
        whole_layer,
        mesh=mesh,
        in_specs=(
            P(("sp", "tp"), None),
            P(None, "tp"),
            P(None, "tp"),
            P(None, "tp"),
            P(None, "tp"),
            P("tp", None, None),
            P(),
            P(),
            P("tp", None),
            P("tp", None),
        ),
        out_specs=P(("sp", "tp"), None),
        check_vma=False,
    )
```

```python
import functools
import math

import jax
import jax.numpy as jnp
from jax import lax
from jax.experimental import pallas as pl
from jax.experimental.pallas import tpu as pltpu
from jax.sharding import PartitionSpec as P

reach_back = 15
norm_epsilon = 1e-06


def passed_along(block, axis, distance):
    devices = range(lax.axis_size(axis))
    route = [(i - distance, i) for i in devices if i - distance in devices]
    return lax.ppermute(block, axis, route)


def from_partner(block, axis, stride):
    count = lax.axis_size(axis)
    route = []
    for low in range(count):
        high = low | 1 << stride
        if high != low and high < count:
            route += [(low, high), (high, low)]
    return lax.ppermute(block, axis, route)


def shifted(array, axis, by):
    size = lax.axis_size(axis)
    return lax.ppermute(array, axis, [(i, (i + by) % size) for i in range(size)])


def as_sent(array):

    def short(part):
        return part.astype(jnp.bfloat16) if part.dtype == jnp.float32 else part

    return jax.tree.map(short, array)


def attend(running, queries, key_rows, value_rows, query_first, key_first, score_scale):
    key_count = key_rows.shape[0]
    key_block = math.gcd(key_count, 1024)
    unit_count = queries.shape[1]
    heads_here = value_rows.shape[1]
    per_head = unit_count // heads_here
    query_count = queries.shape[0]
    query_order = query_first + lax.iota(jnp.int32, query_count)

    def key_step(block_index, carried):
        block_start = block_index * key_block

        def block_work(current):
            row_peak, row_total, weighted = current
            scores = (
                jnp.einsum("qud,kud->uqk", queries, key_rows, preferred_element_type=jnp.float32)
                * score_scale
            )
            key_order = key_first + block_start + lax.iota(jnp.int32, key_block)
            scores = jnp.where(
                key_order[None, None, :] <= query_order[None, :, None], scores, -jnp.inf
            )
            new_peak = jnp.maximum(row_peak, jnp.max(scores, axis=2))
            shrink = jnp.exp(row_peak - new_peak)
            raised = jnp.exp(scores - new_peak[:, :, None])
            row_total = row_total * shrink + jnp.sum(raised, axis=2)
            map_weights = raised.astype(jnp.bfloat16).reshape(
                heads_here, per_head, query_count, key_block
            )
            update = jnp.einsum(
                "hmqk,khe->hmqe", map_weights, value_rows, preferred_element_type=jnp.float32
            )
            weighted = weighted * shrink[:, :, None] + update.reshape(unit_count, query_count, -1)
            return (new_peak, row_total, weighted)

        def keep_state(current):
            return current

        return lax.cond(
            key_first + block_start <= query_first + query_count - 1,
            block_work,
            keep_state,
            carried,
        )

    return lax.fori_loop(0, key_count // key_block, key_step, running)


def fresh_state(unit_count, row_count, value_width):
    return (
        jnp.full((unit_count, row_count), -1e30, jnp.float32),
        jnp.zeros((unit_count, row_count), jnp.float32),
        jnp.zeros((unit_count, row_count, value_width), jnp.float32),
    )


def finished(running):
    row_peak, row_total, weighted = running
    return (weighted / row_total[:, :, None]).astype(jnp.bfloat16)


def joined_state(first, second):
    first_peak, first_total, first_weighted = first
    second_peak, second_total, second_weighted = second
    new_peak = jnp.maximum(first_peak, second_peak)
    first_shrink = jnp.exp(first_peak - new_peak)
    second_shrink = jnp.exp(second_peak - new_peak)
    new_total = first_total * first_shrink + second_total * second_shrink
    new_weighted = (
        first_weighted * first_shrink[:, :, None] + second_weighted * second_shrink[:, :, None]
    )
    return (new_peak, new_total, new_weighted)


def per_device(
    normed,
    query_weight,
    key_weight,
    value_weight,
    pool_in_weight,
    pool_weight,
    map_balance,
    head_gain,
    contrast_out_weight,
    pool_out_weight,
):
    tp_index = lax.axis_index("tp")
    sp_count = lax.axis_size("sp")
    sp_index = lax.axis_index("sp")
    head_dim = head_gain.shape[0] // 2
    value_width = 2 * head_dim
    query_cols = query_weight.shape[1]
    value_cols = value_weight.shape[1]
    unit_count = query_cols // head_dim
    heads_here = unit_count // 2
    project_incoming = lax.all_gather(normed, "tp", axis=0, tiled=True)
    products = [
        jnp.dot(project_incoming, weight_part, preferred_element_type=jnp.float32)
        for weight_part in (query_weight, key_weight, value_weight, pool_in_weight)
    ]
    joined = jnp.concatenate(products, axis=1).astype(jnp.bfloat16)
    row_count = joined.shape[0]
    queries = joined[:, :query_cols].reshape(row_count, unit_count, head_dim)
    key_rows = joined[:, query_cols : 2 * query_cols].reshape(row_count, unit_count, head_dim)
    value_rows = joined[:, 2 * query_cols : 2 * query_cols + value_cols].reshape(
        row_count, heads_here, value_width
    )
    pool_input = joined[:, 2 * query_cols + value_cols :]
    pool_cols = pool_input.shape[1]
    upper_rim = passed_along(pool_input[row_count - reach_back :], "sp", 1)
    extended = jnp.concatenate([upper_rim, pool_input], axis=0).astype(jnp.float32)
    groups_here = pool_weight.shape[0]
    group_width = pool_weight.shape[1]
    group_index = tp_index * groups_here + lax.iota(jnp.int32, pool_cols) // group_width
    widths = jnp.left_shift(jnp.int32(2), group_index % 4)
    window_sum = jnp.zeros((row_count, pool_cols), jnp.float32)
    for offset in range(reach_back + 1):
        window_sum = window_sum + extended[
            reach_back - offset : reach_back - offset + row_count
        ] * (offset < widths)[None, :].astype(jnp.float32)
    position = sp_index * row_count + lax.iota(jnp.int32, row_count)
    counts = jnp.minimum(position[:, None] + 1, widths[None, :]).astype(jnp.float32)
    spread = (window_sum / counts - extended[reach_back:]).astype(jnp.bfloat16)
    mixed_groups = jnp.einsum(
        "tgc,gce->tge",
        spread.reshape(row_count, groups_here, group_width),
        pool_weight,
        preferred_element_type=jnp.float32,
    )
    pool_out = mixed_groups.reshape(row_count, pool_cols).astype(jnp.bfloat16)
    score_scale = head_dim ** (-0.5)
    level_count = sp_count.bit_length() - 1
    low_levels = level_count // 2
    band_size = 1 << low_levels
    band_count = sp_count // band_size
    member = sp_index % band_size
    band = sp_index // band_size
    band_queries = queries
    for bit in range(low_levels):
        received = from_partner(band_queries, "sp", bit)
        upper = member >> bit & 1 == 1
        band_queries = jnp.where(
            upper,
            jnp.concatenate([received, band_queries], axis=0),
            jnp.concatenate([band_queries, received], axis=0),
        )
    band_first = band * band_size * row_count
    running = fresh_state(unit_count, band_size * row_count, value_width)
    for step in range(band_count):
        if step == 0:
            key_piece, value_piece = (key_rows, value_rows)
        else:
            key_piece, value_piece = shifted((key_rows, value_rows), "sp", step * band_size)
        source = (sp_index - step * band_size) % sp_count
        running = attend(
            running,
            band_queries,
            key_piece,
            value_piece,
            band_first,
            source * row_count,
            score_scale,
        )
    for bit in range(low_levels - 1, -1, -1):
        half = running[0].shape[1] // 2
        upper = member >> bit & 1 == 1
        lower_part = jax.tree.map(lambda item: item[:, :half], running)
        upper_part = jax.tree.map(lambda item: item[:, half:], running)
        outgoing = jax.tree.map(
            lambda low, high: jnp.where(upper, low, high), lower_part, upper_part
        )
        kept = jax.tree.map(lambda low, high: jnp.where(upper, high, low), lower_part, upper_part)
        incoming = from_partner(
            (as_sent(outgoing[0]), as_sent(outgoing[1]), as_sent(outgoing[2])), "sp", bit
        )
        running = joined_state(kept, incoming)
    maps = finished(running)
    paired = maps.reshape(heads_here, 2, row_count, value_width)
    paired = lax.optimization_barrier(paired).astype(jnp.float32)
    head_first = tp_index * heads_here
    balance_here = lax.dynamic_slice_in_dim(map_balance, head_first, heads_here, 0)
    contrast = paired[:, 0] - balance_here[:, None, None] * paired[:, 1]
    mean_square = jnp.mean(contrast * contrast, axis=2, keepdims=True)
    contrast = contrast * lax.rsqrt(mean_square + norm_epsilon) * head_gain
    contrast_out = (
        contrast.astype(jnp.bfloat16)
        .transpose(1, 0, 2)
        .reshape(row_count, heads_here * value_width)
    )
    partial_value = jnp.dot(contrast_out, contrast_out_weight, preferred_element_type=jnp.float32)
    return lax.psum_scatter(
        (
            partial_value + jnp.dot(pool_out, pool_out_weight, preferred_element_type=jnp.float32)
        ).astype(jnp.bfloat16),
        "tp",
        scatter_dimension=0,
        tiled=True,
    )


MESH = pl.DeviceIdType.MESH


def layer_kernel(
    sp_count,
    members,
    x_ref,
    pool_weight,
    balance,
    gain,
    query_hbm,
    key_hbm,
    value_hbm,
    pool_in_hbm,
    contrast_hbm,
    pool_out_hbm,
    out_ref,
    out_recv,
    query_w,
    key_w,
    value_w,
    pool_in_w,
    contrast_w,
    pool_out_w,
    rows_in,
    kv,
    kv_stage,
    far_stage,
    queries,
    query_stage,
    peaks,
    totals,
    weighted,
    contrasts,
    contrast_stage,
    rim,
    rim_stage,
    pool_part,
    out_stage,
    weight_sem,
    local_sem,
    pair_send,
    pair_recv,
    relay_send,
    relay_recv,
    kv_send,
    kv_recv,
    forward_send,
    far_send,
    far_recv,
    far_forward,
    query_send,
    query_recv,
    contrast_send,
    contrast_recv,
    rim_send,
    rim_recv,
    out_send,
    out_recv_sem,
):
    f32 = jnp.float32
    bf16 = jnp.bfloat16
    sp = lax.axis_index("sp")
    tp = lax.axis_index("tp")
    other = 1 - tp
    plane = lax.div(sp, members)
    member = lax.rem(sp, members)
    upper = lax.div(plane, 2)
    side = lax.rem(plane, 2)
    across = lax.div(member, 2)
    along = lax.rem(member, 2)
    half_count = 2 * members
    half, model = x_ref.shape
    rows = 2 * half
    width = gain.shape[1]
    head_dim = width // 2
    chunks = 2
    piece = half // chunks
    in_lower = upper == 0
    in_upper = upper == 1
    crosses = plane == 1
    relays = plane == 2
    query_band = 2 * upper + tp
    bands_of = (plane, plane + 1 - 2 * side)

    loads = [
        pltpu.make_async_copy(src, dst, weight_sem.at[i])
        for i, (src, dst) in enumerate(
            (
                (key_hbm, key_w),
                (value_hbm, value_w),
                (query_hbm, query_w),
                (pool_in_hbm, pool_in_w),
                (pool_out_hbm, pool_out_w),
                (contrast_hbm, contrast_w),
            )
        )
    ]
    for load in loads:
        load.start()
    keep = pltpu.make_async_copy(x_ref, rows_in.at[0, tp], local_sem)
    keep.start()

    barrier = pltpu.get_barrier_semaphore()

    def greet(target):
        pl.semaphore_signal(barrier, inc=1, device_id=target, device_id_type=MESH)

    place = (side * members + member) * 2 + tp
    for d in range(1, 2 * half_count):
        goal = lax.rem(place + d, 2 * half_count)
        greet((upper * half_count + lax.div(goal, 2), lax.rem(goal, 2)))

    @pl.when(crosses)
    def _():
        greet((sp + members, tp))

    @pl.when(relays)
    def _():
        greet((sp - members, tp))

    @pl.when(sp == half_count - 1)
    def _():
        greet((sp + 1, tp))

    @pl.when(sp == half_count)
    def _():
        greet((sp - 1, tp))

    extra = jnp.where(jnp.logical_or(crosses, relays), 1, 0)
    extra = extra + jnp.where(jnp.logical_or(sp == half_count - 1, sp == half_count), 1, 0)
    pl.semaphore_wait(barrier, 2 * half_count - 1 + extra)

    def cut(ch):
        return pl.ds(ch * piece, piece)

    pair_first = pltpu.make_async_remote_copy(
        src_ref=x_ref,
        dst_ref=rows_in.at[0, tp],
        send_sem=pair_send.at[0, 0],
        recv_sem=pair_recv.at[0, 0],
        device_id=(sp, other),
        device_id_type=MESH,
    )

    def pair_copy(step, ch):
        return pltpu.make_async_remote_copy(
            src_ref=rows_in.at[step, tp, cut(ch)],
            dst_ref=rows_in.at[step, tp, cut(ch)],
            send_sem=pair_send.at[step, ch],
            recv_sem=pair_recv.at[step, ch],
            device_id=(sp, other),
            device_id_type=MESH,
        )

    def relay_copy(src, step, ch, target):
        return pltpu.make_async_remote_copy(
            src_ref=src.at[cut(ch)],
            dst_ref=rows_in.at[step, tp, cut(ch)],
            send_sem=relay_send.at[step, ch],
            recv_sem=relay_recv.at[step, ch],
            device_id=(target, tp),
            device_id_type=MESH,
        )

    def swap(ch):
        return relay_copy(x_ref, 1, ch, sp + members * (1 - 2 * side))

    def own_up(ch):
        return relay_copy(x_ref, 2, ch, sp + members)

    def low_up(ch):
        return relay_copy(rows_in.at[1, tp], 3, ch, sp + members)

    def top(step):
        return side == (1 if step == 0 else 0)

    def kv_copy(step, j):
        goal = 2 * tp + j
        first = jnp.where(top(step), 1, along)
        return pltpu.make_async_remote_copy(
            src_ref=kv_stage.at[step, j],
            dst_ref=kv.at[step, member],
            send_sem=kv_send.at[step, j],
            recv_sem=kv_recv.at[step, member],
            device_id=(plane * members + goal, first),
            device_id_type=MESH,
        )

    def forward_copy(step, source):
        return pltpu.make_async_remote_copy(
            src_ref=kv.at[step, source],
            dst_ref=kv.at[step, source],
            send_sem=forward_send.at[step, source],
            recv_sem=kv_recv.at[step, source],
            device_id=(sp, other),
            device_id_type=MESH,
        )

    def query_copy(step, j):
        core = jnp.where(top(step), 1, 0)
        return pltpu.make_async_remote_copy(
            src_ref=query_stage.at[step, j],
            dst_ref=queries.at[member],
            send_sem=query_send.at[step, j],
            recv_sem=query_recv.at[member],
            device_id=(plane * members + 2 * tp + j, core),
            device_id_type=MESH,
        )

    own_goal = across == tp

    def part(ch):
        return pl.ds(ch * half, half)

    def far_copy(step, ch, goal_side, j):
        slot = goal_side * 2 + j
        goal = (2 * upper + goal_side) * members + 2 * tp + j
        return pltpu.make_async_remote_copy(
            src_ref=far_stage.at[step - 2, slot, part(ch)],
            dst_ref=kv.at[step, member, part(ch)],
            send_sem=far_send.at[step - 2, slot, ch],
            recv_sem=far_recv.at[step - 2, member, ch],
            device_id=(goal, along),
            device_id_type=MESH,
        )

    def far_pass(step, source, ch):
        return pltpu.make_async_remote_copy(
            src_ref=kv.at[step, source, part(ch)],
            dst_ref=kv.at[step, source, part(ch)],
            send_sem=far_forward.at[step - 2, source, ch],
            recv_sem=far_recv.at[step - 2, source, ch],
            device_id=(sp, other),
            device_id_type=MESH,
        )

    def far_stays(goal_side, j):
        return jnp.logical_and(goal_side == side, jnp.logical_and(own_goal, j == along))

    def far_here(source):
        return jnp.logical_and(relays, source == member)

    def far_passes(source):
        return jnp.logical_and(source % 2 == tp, jnp.logical_not(far_here(source)))

    def far_awaits(source):
        return jnp.logical_not(jnp.logical_and(far_here(source), own_goal))

    def own_stays(step, j):
        return jnp.logical_and(own_goal, j == along)

    def query_stays(step, j):
        return jnp.logical_and(own_stays(step, j), jnp.where(top(step), 1, 0) == tp)

    def own_forwards(step):
        return jnp.logical_and(
            own_goal, jnp.logical_or(jnp.logical_not(top(step)), tp == 0)
        )

    def passes_on(step, source):
        mine = jnp.logical_and(source % 2 == tp, jnp.logical_not(top(step)))
        return jnp.logical_and(source != member, mine)

    def awaits(step, source):
        needed = jnp.logical_or(tp == 1, jnp.logical_not(top(step)))
        made_here = jnp.logical_and(source == member, own_goal)
        return jnp.logical_and(needed, jnp.logical_not(made_here))

    def contrast_stays(i):
        return jnp.logical_and(
            jnp.logical_and(query_band == plane, i == member), across == tp
        )

    head_here = 2 * side + along

    def contrast_copy(i):
        return pltpu.make_async_remote_copy(
            src_ref=contrast_stage.at[i],
            dst_ref=contrasts.at[head_here],
            send_sem=contrast_send.at[i],
            recv_sem=contrast_recv.at[head_here],
            device_id=(query_band * members + i, across),
            device_id_type=MESH,
        )

    def contrast_incoming(head):
        return pltpu.make_async_remote_copy(
            src_ref=contrast_stage.at[0],
            dst_ref=contrasts.at[head],
            send_sem=contrast_send.at[0],
            recv_sem=contrast_recv.at[head],
            device_id=(sp, other),
            device_id_type=MESH,
        )

    def contrast_local(head):
        same = jnp.logical_and(head // 2 == side, 2 * tp + head % 2 == member)
        return jnp.logical_and(same, side == tp)

    rim_copy = pltpu.make_async_remote_copy(
        src_ref=rim_stage,
        dst_ref=rim,
        send_sem=rim_send,
        recv_sem=rim_recv,
        device_id=(lax.rem(sp + 1, sp_count), tp),
        device_id_type=MESH,
    )
    out_copy = pltpu.make_async_remote_copy(
        src_ref=out_stage,
        dst_ref=out_recv,
        send_sem=out_send,
        recv_sem=out_recv_sem,
        device_id=(sp, other),
        device_id_type=MESH,
    )

    pair_first.start()
    for ch in range(chunks):
        swap(ch).start()

        @pl.when(crosses)
        def _(ch=ch):
            own_up(ch).start()

    peaks[...] = jnp.full(peaks.shape, -1e30, f32)
    totals[...] = jnp.zeros(totals.shape, f32)
    weighted[...] = jnp.zeros(weighted.shape, f32)

    def project(step):
        def one(t, carry):
            j = jnp.where(t == 0, 1 - along, along)
            columns = pl.ds(pl.multiple_of((2 * side + j) * width, width), width)
            x = rows_in[step].reshape(rows, model)
            mine = jnp.dot(x, query_w[:, columns], preferred_element_type=f32).astype(bf16)
            keys = jnp.dot(x, key_w[:, columns], preferred_element_type=f32).astype(bf16)
            values = jnp.dot(x, value_w[:, columns], preferred_element_type=f32).astype(bf16)
            kept = query_stays(step, j)
            stays = own_stays(step, j)

            @pl.when(jnp.logical_not(kept))
            def _():
                query_stage[step, j] = mine
                query_copy(step, j).start()

            @pl.when(kept)
            def _():
                queries[member] = mine

            @pl.when(jnp.logical_not(stays))
            def _():
                kv_stage[step, j, :, :width] = keys
                kv_stage[step, j, :, width:] = values
                kv_copy(step, j).start()

            @pl.when(stays)
            def _():
                kv[step, member, :, :width] = keys
                kv[step, member, :, width:] = values

                @pl.when(own_forwards(step))
                def _():
                    forward_copy(step, member).start()

            return carry

        lax.fori_loop(0, 2, one, 0)

    def project_far(step, ch):
        pair_copy(step, ch).wait_recv()

        def one(t, carry):
            goal_side = 1 - lax.div(t, 2)
            j = jnp.where(lax.rem(t, 2) == 0, 1 - along, along)
            columns = pl.ds(pl.multiple_of((2 * goal_side + j) * width, width), width)
            x = rows_in[step, :, cut(ch), :].reshape(half, model)
            keys = jnp.dot(x, key_w[:, columns], preferred_element_type=f32).astype(bf16)
            values = jnp.dot(x, value_w[:, columns], preferred_element_type=f32).astype(bf16)
            stays = far_stays(goal_side, j)

            @pl.when(jnp.logical_not(stays))
            def _():
                far_stage[step - 2, goal_side * 2 + j, part(ch), :width] = keys
                far_stage[step - 2, goal_side * 2 + j, part(ch), width:] = values
                far_copy(step, ch, goal_side, j).start()

            @pl.when(stays)
            def _():
                kv[step, member, part(ch), :width] = keys
                kv[step, member, part(ch), width:] = values
                far_pass(step, member, ch).start()

            return carry

        lax.fori_loop(0, 4, one, 0)

    def take_swap(ch):
        swap(ch).wait_recv()

        @pl.when(crosses)
        def _():
            low_up(ch).start()

        pair_copy(1, ch).start()

    def take_far(step, ch):
        (own_up(ch) if step == 2 else low_up(ch)).wait_recv()
        pair_copy(step, ch).start()

    def paired(step):
        for ch in range(chunks):
            pair_copy(step, ch).wait_recv()

    log_scale = head_dim ** (-0.5) * math.log2(math.e)

    def attend_block(step, i, seen, masked, span=slice(None)):
        for u in range(2):
            cols = slice(u * head_dim, (u + 1) * head_dim)
            keys = kv[step, :seen, span, cols].reshape(-1, head_dim)
            values = kv[step, :seen, span, width:].reshape(-1, width)
            scores = lax.dot_general(
                queries[i, :, cols], keys, (((1,), (1,)), ((), ())), preferred_element_type=f32
            )
            if masked:
                query_order = lax.broadcasted_iota(jnp.int32, scores.shape, 0) + (seen - 1) * rows
                key_order = lax.broadcasted_iota(jnp.int32, scores.shape, 1)
                scores = jnp.where(key_order <= query_order, scores, -jnp.inf)
            old = peaks[u, i][:, :1]
            peak = jnp.maximum(jnp.max(scores, axis=1, keepdims=True), old)
            shrink = jnp.exp2((old - peak) * log_scale)
            raised = jnp.exp2((scores - peak) * log_scale)
            total = jnp.sum(raised, axis=1, keepdims=True)
            update = jnp.dot(raised.astype(bf16), values, preferred_element_type=f32)
            total = total + totals[u, i][:, :1] * shrink
            update = update + weighted[u, i] * shrink
            peaks[u, i] = jnp.broadcast_to(peak, peaks.shape[2:])
            totals[u, i] = jnp.broadcast_to(total, totals.shape[2:])
            weighted[u, i] = update

    weight = balance[across * members + head_here]

    def finish(i):
        first = (weighted[0, i] / totals[0, i][:, :1]).astype(bf16).astype(f32)
        second = (weighted[1, i] / totals[1, i][:, :1]).astype(bf16).astype(f32)
        contrast = first - weight * second
        mean_square = jnp.mean(contrast * contrast, axis=1, keepdims=True)
        result = (contrast * lax.rsqrt(mean_square + norm_epsilon) * gain[...]).astype(bf16)
        stays = contrast_stays(i)

        @pl.when(jnp.logical_not(stays))
        def _():
            contrast_stage[i] = result
            contrast_copy(i).start()

        @pl.when(stays)
        def _():
            contrasts[head_here] = result

    def each_block(work):
        def one(t, carry):
            work(lax.rem(member + 1 + t, members))
            return carry

        lax.fori_loop(0, members, one, 0)

    def arrive(step):
        for source in range(members):

            @pl.when(awaits(step, source))
            def _(source=source):
                forward_copy(step, source).wait_recv()

            @pl.when(passes_on(step, source))
            def _(source=source):
                forward_copy(step, source).start()

    def attend(step):
        band = bands_of[step]

        @pl.when(band == query_band)
        def _():
            for i in range(members):
                attend_block(step, i, i + 1, True)

        @pl.when(band < query_band)
        def _():
            each_block(lambda i: attend_block(step, i, members, False))

    def far_arrive(step, ch):
        for source in range(members):

            @pl.when(far_awaits(source))
            def _(source=source):
                far_pass(step, source, ch).wait_recv()

            @pl.when(far_passes(source))
            def _(source=source):
                far_pass(step, source, ch).start()

    keep.wait()
    loads[0].wait()
    loads[1].wait()
    loads[2].wait()
    pair_first.wait_recv()
    project(0)

    loads[3].wait()
    pool_input = jnp.dot(
        rows_in[0].reshape(rows, model), pool_in_w[...], preferred_element_type=f32
    ).astype(bf16)
    rim_stage[...] = pool_input[rows - rim.shape[0] :]

    @pl.when(sp + 1 < sp_count)
    def _():
        rim_copy.start()

    take_swap(0)

    @pl.when(relays)
    def _():
        take_far(2, 0)
        project_far(2, 0)

    take_swap(1)

    @pl.when(relays)
    def _():
        take_far(2, 1)

    paired(1)
    project(1)

    @pl.when(relays)
    def _():
        project_far(2, 1)
        take_far(3, 0)
        project_far(3, 0)

    @pl.when(sp > 0)
    def _():
        rim_copy.wait_recv()

    @pl.when(sp == 0)
    def _():
        rim[...] = jnp.zeros_like(rim)

    loads[4].wait()
    extended = jnp.concatenate([rim[...], pool_input], axis=0).astype(f32)
    group_width = pool_weight.shape[1]
    skirt = rim.shape[0]
    position = sp * rows + lax.broadcasted_iota(jnp.int32, (rows, group_width), 0)
    mixed = []
    for group in range(pool_weight.shape[0]):
        block = extended[:, group * group_width : (group + 1) * group_width]
        window = block
        reach = 1
        span = 2 ** (1 + group % 4)
        while reach < span:
            window = window + pltpu.roll(window, reach, 0)
            reach *= 2
        counts = jnp.minimum(position + 1, span).astype(f32)
        spread = (window[skirt:] / counts - block[skirt:]).astype(bf16)
        mixed.append(
            jnp.dot(spread, pool_weight[group], preferred_element_type=f32).astype(bf16)
        )
    pool_out = jnp.concatenate(mixed, axis=1)
    chunk = math.gcd(model, 512)
    for start in range(0, model, chunk):
        pool_part[:, start : start + chunk] = jnp.dot(
            pool_out, pool_out_w[:, start : start + chunk], preferred_element_type=f32
        )

    def query_incoming(source):
        return pltpu.make_async_remote_copy(
            src_ref=query_stage.at[0, 0],
            dst_ref=queries.at[source],
            send_sem=query_send.at[0, 0],
            recv_sem=query_recv.at[source],
            device_id=(sp, other),
            device_id_type=MESH,
        )

    def take_queries():
        for source in range(members):

            @pl.when(jnp.logical_not(jnp.logical_and(source == member, own_goal)))
            def _(source=source):
                query_incoming(source).wait_recv()

    arrive(0)
    take_queries()
    attend(0)

    @pl.when(relays)
    def _():
        take_far(3, 1)
        project_far(3, 1)

    arrive(1)
    attend(1)

    @pl.when(in_lower)
    def _():
        each_block(finish)

    @pl.when(in_upper)
    def _():
        far_arrive(2, 0)
        far_arrive(2, 1)
        each_block(lambda i: attend_block(2, i, members, False))
        far_arrive(3, 0)
        each_block(lambda i: attend_block(3, i, members, False, slice(0, half)))
        far_arrive(3, 1)

        def last(i):
            attend_block(3, i, members, False, slice(half, rows))
            finish(i)

        each_block(last)

    loads[5].wait()
    for head in range(members):

        @pl.when(jnp.logical_not(contrast_local(head)))
        def _(head=head):
            contrast_incoming(head).wait_recv()

    def projected(taken_side, store):
        taken = pl.ds(pl.multiple_of(taken_side * half, half), half)
        left = jnp.concatenate([contrasts[h, taken, :] for h in range(members)], axis=1)
        for start in range(0, model, chunk):
            span = slice(start, start + chunk)
            part = jnp.dot(left, contrast_w[:, span], preferred_element_type=f32)
            store(span, (part + pool_part[taken, span]).astype(bf16))

    def to_partner(span, part):
        out_stage[:, span] = part

    def to_self(span, part):
        out_ref[:, span] = part

    projected(other, to_partner)
    out_copy.start()
    projected(tp, to_self)
    out_copy.wait()

    pair_first.wait_send()
    for ch in range(chunks):
        swap(ch).wait_send()
        pair_copy(1, ch).wait_send()

        @pl.when(crosses)
        def _(ch=ch):
            own_up(ch).wait_send()
            low_up(ch).wait_send()

        @pl.when(relays)
        def _(ch=ch):
            for step in range(2, 4):
                pair_copy(step, ch).wait_send()
                for slot in range(4):

                    @pl.when(jnp.logical_not(far_stays(slot // 2, slot % 2)))
                    def _(step=step, slot=slot):
                        far_copy(step, ch, slot // 2, slot % 2).wait_send()

                @pl.when(own_goal)
                def _(step=step):
                    far_pass(step, member, ch).wait_send()

        @pl.when(in_upper)
        def _(ch=ch):
            for step in range(2, 4):
                for source in range(members):

                    @pl.when(far_passes(source))
                    def _(step=step, source=source):
                        far_pass(step, source, ch).wait_send()

    def drain(step):
        for j in range(2):

            @pl.when(jnp.logical_not(own_stays(step, j)))
            def _(j=j):
                kv_copy(step, j).wait_send()

            @pl.when(jnp.logical_not(query_stays(step, j)))
            def _(j=j):
                query_copy(step, j).wait_send()

        @pl.when(own_forwards(step))
        def _():
            forward_copy(step, member).wait_send()

        for source in range(members):

            @pl.when(passes_on(step, source))
            def _(source=source):
                forward_copy(step, source).wait_send()

    drain(0)
    drain(1)

    for i in range(members):

        @pl.when(jnp.logical_not(contrast_stays(i)))
        def _(i=i):
            contrast_copy(i).wait_send()

    @pl.when(sp + 1 < sp_count)
    def _():
        rim_copy.wait_send()


def kernel_scratch(members, half, model, width, pool_cols):
    bf16 = jnp.bfloat16
    rows = 2 * half
    dma = pltpu.SemaphoreType.DMA
    return [
        pltpu.VMEM((model, members * width), bf16),
        pltpu.VMEM((model, members * width), bf16),
        pltpu.VMEM((model, members * width), bf16),
        pltpu.VMEM((model, pool_cols), bf16),
        pltpu.VMEM((members * width, model), bf16),
        pltpu.VMEM((pool_cols, model), bf16),
        pltpu.VMEM((4, 2, half, model), bf16),
        pltpu.VMEM((4, members, rows, 2 * width), bf16),
        pltpu.VMEM((2, 2, rows, 2 * width), bf16),
        pltpu.VMEM((2, 4, rows, 2 * width), bf16),
        pltpu.VMEM((members, rows, width), bf16),
        pltpu.VMEM((2, 2, rows, width), bf16),
        pltpu.VMEM((2, members, rows, 128), jnp.float32),
        pltpu.VMEM((2, members, rows, 128), jnp.float32),
        pltpu.VMEM((2, members, rows, width), jnp.float32),
        pltpu.VMEM((members, rows, width), bf16),
        pltpu.VMEM((members, rows, width), bf16),
        pltpu.VMEM((reach_back + 1, pool_cols), bf16),
        pltpu.VMEM((reach_back + 1, pool_cols), bf16),
        pltpu.VMEM((rows, model), jnp.float32),
        pltpu.VMEM((half, model), bf16),
        dma((6,)),
        dma,
        dma((4, 2)),
        dma((4, 2)),
        dma((4, 2)),
        dma((4, 2)),
        dma((2, 2)),
        dma((2, members)),
        dma((2, members)),
        dma((2, 4, 2)),
        dma((2, members, 2)),
        dma((2, members, 2)),
        dma((2, 2)),
        dma((members,)),
        dma((members,)),
        dma((members,)),
        dma,
        dma,
        dma,
        dma,
    ]


vmem_most = 67043328


def scratch_bytes(scratch):
    return sum(
        math.prod(item.shape) * jnp.dtype(item.dtype).itemsize
        for item in scratch
        if getattr(item, "memory_space", None) == pltpu.VMEM
    )


def whole_layer(
    normed,
    query_weight,
    key_weight,
    value_weight,
    pool_in_weight,
    pool_weight,
    map_balance,
    head_gain,
    contrast_out_weight,
    pool_out_weight,
):
    sp_count = lax.axis_size("sp")
    width = head_gain.shape[0]
    members = query_weight.shape[1] // width
    half, model = normed.shape
    pool_cols = pool_in_weight.shape[1]
    groups_here = pool_weight.shape[0]
    scratch = kernel_scratch(max(members, 1), half, model, width, pool_cols)
    fits = (
        lax.axis_size("tp") == 2
        and members == 4
        and sp_count == 4 * members
        and groups_here % 4 == 0
        and scratch_bytes(scratch) < vmem_most * 3 // 4
    )
    if not fits:
        return per_device(
            normed,
            query_weight,
            key_weight,
            value_weight,
            pool_in_weight,
            pool_weight,
            map_balance,
            head_gain,
            contrast_out_weight,
            pool_out_weight,
        )
    vmem = pl.BlockSpec(memory_space=pltpu.VMEM)
    hbm = pl.BlockSpec(memory_space=pl.ANY)
    own_part, partner_part = pl.pallas_call(
        functools.partial(layer_kernel, sp_count, members),
        out_shape=[jax.ShapeDtypeStruct((half, model), jnp.bfloat16)] * 2,
        in_specs=[vmem, vmem, pl.BlockSpec(memory_space=pltpu.SMEM), vmem] + [hbm] * 6,
        out_specs=[vmem, vmem],
        scratch_shapes=scratch,
        compiler_params=pltpu.CompilerParams(
            collective_id=0, has_side_effects=True, vmem_limit_bytes=vmem_most
        ),
    )(
        normed,
        pool_weight,
        map_balance,
        head_gain.reshape(1, width),
        query_weight,
        key_weight,
        value_weight,
        pool_in_weight,
        contrast_out_weight,
        pool_out_weight,
    )
    return (own_part.astype(jnp.float32) + partner_part.astype(jnp.float32)).astype(jnp.bfloat16)


def solution(mesh):
    return jax.shard_map(
        whole_layer,
        mesh=mesh,
        in_specs=(
            P(("sp", "tp"), None),
            P(None, "tp"),
            P(None, "tp"),
            P(None, "tp"),
            P(None, "tp"),
            P("tp", None, None),
            P(),
            P(),
            P("tp", None),
            P("tp", None),
        ),
        out_specs=P(("sp", "tp"), None),
        check_vma=False,
    )
```

```python
import functools
import math

import jax
import jax.numpy as jnp
from jax import lax
from jax.experimental import pallas as pl
from jax.experimental.pallas import tpu as pltpu
from jax.sharding import PartitionSpec as P

reach_back = 15
norm_epsilon = 1e-06


def passed_along(block, axis, distance):
    devices = range(lax.axis_size(axis))
    route = [(i - distance, i) for i in devices if i - distance in devices]
    return lax.ppermute(block, axis, route)


def from_partner(block, axis, stride):
    count = lax.axis_size(axis)
    route = []
    for low in range(count):
        high = low | 1 << stride
        if high != low and high < count:
            route += [(low, high), (high, low)]
    return lax.ppermute(block, axis, route)


def shifted(array, axis, by):
    size = lax.axis_size(axis)
    return lax.ppermute(array, axis, [(i, (i + by) % size) for i in range(size)])


def as_sent(array):

    def short(part):
        return part.astype(jnp.bfloat16) if part.dtype == jnp.float32 else part

    return jax.tree.map(short, array)


def attend(running, queries, key_rows, value_rows, query_first, key_first, score_scale):
    key_count = key_rows.shape[0]
    key_block = math.gcd(key_count, 1024)
    unit_count = queries.shape[1]
    heads_here = value_rows.shape[1]
    per_head = unit_count // heads_here
    query_count = queries.shape[0]
    query_order = query_first + lax.iota(jnp.int32, query_count)

    def key_step(block_index, carried):
        block_start = block_index * key_block

        def block_work(current):
            row_peak, row_total, weighted = current
            scores = (
                jnp.einsum("qud,kud->uqk", queries, key_rows, preferred_element_type=jnp.float32)
                * score_scale
            )
            key_order = key_first + block_start + lax.iota(jnp.int32, key_block)
            scores = jnp.where(
                key_order[None, None, :] <= query_order[None, :, None], scores, -jnp.inf
            )
            new_peak = jnp.maximum(row_peak, jnp.max(scores, axis=2))
            shrink = jnp.exp(row_peak - new_peak)
            raised = jnp.exp(scores - new_peak[:, :, None])
            row_total = row_total * shrink + jnp.sum(raised, axis=2)
            map_weights = raised.astype(jnp.bfloat16).reshape(
                heads_here, per_head, query_count, key_block
            )
            update = jnp.einsum(
                "hmqk,khe->hmqe", map_weights, value_rows, preferred_element_type=jnp.float32
            )
            weighted = weighted * shrink[:, :, None] + update.reshape(unit_count, query_count, -1)
            return (new_peak, row_total, weighted)

        def keep_state(current):
            return current

        return lax.cond(
            key_first + block_start <= query_first + query_count - 1,
            block_work,
            keep_state,
            carried,
        )

    return lax.fori_loop(0, key_count // key_block, key_step, running)


def fresh_state(unit_count, row_count, value_width):
    return (
        jnp.full((unit_count, row_count), -1e30, jnp.float32),
        jnp.zeros((unit_count, row_count), jnp.float32),
        jnp.zeros((unit_count, row_count, value_width), jnp.float32),
    )


def finished(running):
    row_peak, row_total, weighted = running
    return (weighted / row_total[:, :, None]).astype(jnp.bfloat16)


def joined_state(first, second):
    first_peak, first_total, first_weighted = first
    second_peak, second_total, second_weighted = second
    new_peak = jnp.maximum(first_peak, second_peak)
    first_shrink = jnp.exp(first_peak - new_peak)
    second_shrink = jnp.exp(second_peak - new_peak)
    new_total = first_total * first_shrink + second_total * second_shrink
    new_weighted = (
        first_weighted * first_shrink[:, :, None] + second_weighted * second_shrink[:, :, None]
    )
    return (new_peak, new_total, new_weighted)


def per_device(
    normed,
    query_weight,
    key_weight,
    value_weight,
    pool_in_weight,
    pool_weight,
    map_balance,
    head_gain,
    contrast_out_weight,
    pool_out_weight,
):
    tp_index = lax.axis_index("tp")
    sp_count = lax.axis_size("sp")
    sp_index = lax.axis_index("sp")
    head_dim = head_gain.shape[0] // 2
    value_width = 2 * head_dim
    query_cols = query_weight.shape[1]
    value_cols = value_weight.shape[1]
    unit_count = query_cols // head_dim
    heads_here = unit_count // 2
    project_incoming = lax.all_gather(normed, "tp", axis=0, tiled=True)
    products = [
        jnp.dot(project_incoming, weight_part, preferred_element_type=jnp.float32)
        for weight_part in (query_weight, key_weight, value_weight, pool_in_weight)
    ]
    joined = jnp.concatenate(products, axis=1).astype(jnp.bfloat16)
    row_count = joined.shape[0]
    queries = joined[:, :query_cols].reshape(row_count, unit_count, head_dim)
    key_rows = joined[:, query_cols : 2 * query_cols].reshape(row_count, unit_count, head_dim)
    value_rows = joined[:, 2 * query_cols : 2 * query_cols + value_cols].reshape(
        row_count, heads_here, value_width
    )
    pool_input = joined[:, 2 * query_cols + value_cols :]
    pool_cols = pool_input.shape[1]
    upper_rim = passed_along(pool_input[row_count - reach_back :], "sp", 1)
    extended = jnp.concatenate([upper_rim, pool_input], axis=0).astype(jnp.float32)
    groups_here = pool_weight.shape[0]
    group_width = pool_weight.shape[1]
    group_index = tp_index * groups_here + lax.iota(jnp.int32, pool_cols) // group_width
    widths = jnp.left_shift(jnp.int32(2), group_index % 4)
    window_sum = jnp.zeros((row_count, pool_cols), jnp.float32)
    for offset in range(reach_back + 1):
        window_sum = window_sum + extended[
            reach_back - offset : reach_back - offset + row_count
        ] * (offset < widths)[None, :].astype(jnp.float32)
    position = sp_index * row_count + lax.iota(jnp.int32, row_count)
    counts = jnp.minimum(position[:, None] + 1, widths[None, :]).astype(jnp.float32)
    spread = (window_sum / counts - extended[reach_back:]).astype(jnp.bfloat16)
    mixed_groups = jnp.einsum(
        "tgc,gce->tge",
        spread.reshape(row_count, groups_here, group_width),
        pool_weight,
        preferred_element_type=jnp.float32,
    )
    pool_out = mixed_groups.reshape(row_count, pool_cols).astype(jnp.bfloat16)
    score_scale = head_dim ** (-0.5)
    level_count = sp_count.bit_length() - 1
    low_levels = level_count // 2
    band_size = 1 << low_levels
    band_count = sp_count // band_size
    member = sp_index % band_size
    band = sp_index // band_size
    band_queries = queries
    for bit in range(low_levels):
        received = from_partner(band_queries, "sp", bit)
        upper = member >> bit & 1 == 1
        band_queries = jnp.where(
            upper,
            jnp.concatenate([received, band_queries], axis=0),
            jnp.concatenate([band_queries, received], axis=0),
        )
    band_first = band * band_size * row_count
    running = fresh_state(unit_count, band_size * row_count, value_width)
    for step in range(band_count):
        if step == 0:
            key_piece, value_piece = (key_rows, value_rows)
        else:
            key_piece, value_piece = shifted((key_rows, value_rows), "sp", step * band_size)
        source = (sp_index - step * band_size) % sp_count
        running = attend(
            running,
            band_queries,
            key_piece,
            value_piece,
            band_first,
            source * row_count,
            score_scale,
        )
    for bit in range(low_levels - 1, -1, -1):
        half = running[0].shape[1] // 2
        upper = member >> bit & 1 == 1
        lower_part = jax.tree.map(lambda item: item[:, :half], running)
        upper_part = jax.tree.map(lambda item: item[:, half:], running)
        outgoing = jax.tree.map(
            lambda low, high: jnp.where(upper, low, high), lower_part, upper_part
        )
        kept = jax.tree.map(lambda low, high: jnp.where(upper, high, low), lower_part, upper_part)
        incoming = from_partner(
            (as_sent(outgoing[0]), as_sent(outgoing[1]), as_sent(outgoing[2])), "sp", bit
        )
        running = joined_state(kept, incoming)
    maps = finished(running)
    paired = maps.reshape(heads_here, 2, row_count, value_width)
    paired = lax.optimization_barrier(paired).astype(jnp.float32)
    head_first = tp_index * heads_here
    balance_here = lax.dynamic_slice_in_dim(map_balance, head_first, heads_here, 0)
    contrast = paired[:, 0] - balance_here[:, None, None] * paired[:, 1]
    mean_square = jnp.mean(contrast * contrast, axis=2, keepdims=True)
    contrast = contrast * lax.rsqrt(mean_square + norm_epsilon) * head_gain
    contrast_out = (
        contrast.astype(jnp.bfloat16)
        .transpose(1, 0, 2)
        .reshape(row_count, heads_here * value_width)
    )
    partial_value = jnp.dot(contrast_out, contrast_out_weight, preferred_element_type=jnp.float32)
    return lax.psum_scatter(
        (
            partial_value + jnp.dot(pool_out, pool_out_weight, preferred_element_type=jnp.float32)
        ).astype(jnp.bfloat16),
        "tp",
        scatter_dimension=0,
        tiled=True,
    )


MESH = pl.DeviceIdType.MESH


def layer_kernel(
    sp_count,
    members,
    x_ref,
    pool_weight,
    balance,
    gain,
    query_hbm,
    key_hbm,
    value_hbm,
    pool_in_hbm,
    contrast_hbm,
    pool_out_hbm,
    out_ref,
    out_recv,
    query_w,
    key_w,
    value_w,
    pool_in_w,
    contrast_w,
    pool_out_w,
    rows_in,
    kv,
    kv_stage,
    far_stage,
    queries,
    query_stage,
    peaks,
    totals,
    weighted,
    contrasts,
    contrast_stage,
    rim,
    rim_stage,
    pool_part,
    out_stage,
    weight_sem,
    local_sem,
    pair_send,
    pair_recv,
    relay_send,
    relay_recv,
    kv_send,
    kv_recv,
    forward_send,
    far_send,
    far_recv,
    far_forward,
    query_send,
    query_recv,
    contrast_send,
    contrast_recv,
    rim_send,
    rim_recv,
    out_send,
    out_recv_sem,
):
    f32 = jnp.float32
    bf16 = jnp.bfloat16
    sp = lax.axis_index("sp")
    tp = lax.axis_index("tp")
    other = 1 - tp
    plane = lax.div(sp, members)
    member = lax.rem(sp, members)
    upper = lax.div(plane, 2)
    side = lax.rem(plane, 2)
    across = lax.div(member, 2)
    along = lax.rem(member, 2)
    half_count = 2 * members
    half, model = x_ref.shape
    rows = 2 * half
    width = gain.shape[1]
    head_dim = width // 2
    chunks = 2
    piece = half // chunks
    in_lower = upper == 0
    in_upper = upper == 1
    crosses = plane == 1
    relays = plane == 2
    query_band = 2 * upper + tp
    bands_of = (plane, plane + 1 - 2 * side)

    loads = [
        pltpu.make_async_copy(src, dst, weight_sem.at[i])
        for i, (src, dst) in enumerate(
            (
                (key_hbm, key_w),
                (value_hbm, value_w),
                (query_hbm, query_w),
                (pool_in_hbm, pool_in_w),
                (pool_out_hbm, pool_out_w),
                (contrast_hbm, contrast_w),
            )
        )
    ]
    for load in loads:
        load.start()
    keep = pltpu.make_async_copy(x_ref, rows_in.at[0, tp], local_sem)
    keep.start()

    barrier = pltpu.get_barrier_semaphore()

    def greet(target):
        pl.semaphore_signal(barrier, inc=1, device_id=target, device_id_type=MESH)

    place = (side * members + member) * 2 + tp
    for d in range(1, 2 * half_count):
        goal = lax.rem(place + d, 2 * half_count)
        greet((upper * half_count + lax.div(goal, 2), lax.rem(goal, 2)))

    @pl.when(crosses)
    def _():
        greet((sp + members, tp))

    @pl.when(relays)
    def _():
        greet((sp - members, tp))

    @pl.when(sp == half_count - 1)
    def _():
        greet((sp + 1, tp))

    @pl.when(sp == half_count)
    def _():
        greet((sp - 1, tp))

    extra = jnp.where(jnp.logical_or(crosses, relays), 1, 0)
    extra = extra + jnp.where(jnp.logical_or(sp == half_count - 1, sp == half_count), 1, 0)
    pl.semaphore_wait(barrier, 2 * half_count - 1 + extra)

    def cut(ch):
        return pl.ds(ch * piece, piece)

    pair_first = pltpu.make_async_remote_copy(
        src_ref=x_ref,
        dst_ref=rows_in.at[0, tp],
        send_sem=pair_send.at[0, 0],
        recv_sem=pair_recv.at[0, 0],
        device_id=(sp, other),
        device_id_type=MESH,
    )

    def pair_copy(step, ch):
        return pltpu.make_async_remote_copy(
            src_ref=rows_in.at[step, tp, cut(ch)],
            dst_ref=rows_in.at[step, tp, cut(ch)],
            send_sem=pair_send.at[step, ch],
            recv_sem=pair_recv.at[step, ch],
            device_id=(sp, other),
            device_id_type=MESH,
        )

    def relay_copy(src, step, ch, target):
        return pltpu.make_async_remote_copy(
            src_ref=src.at[cut(ch)],
            dst_ref=rows_in.at[step, tp, cut(ch)],
            send_sem=relay_send.at[step, ch],
            recv_sem=relay_recv.at[step, ch],
            device_id=(target, tp),
            device_id_type=MESH,
        )

    def swap(ch):
        return relay_copy(x_ref, 1, ch, sp + members * (1 - 2 * side))

    def own_up(ch):
        return relay_copy(x_ref, 2, ch, sp + members)

    def low_up(ch):
        return relay_copy(rows_in.at[1, tp], 3, ch, sp + members)

    def top(step):
        return side == (1 if step == 0 else 0)

    def kv_copy(step, j):
        goal = 2 * tp + j
        first = jnp.where(top(step), 1, along)
        return pltpu.make_async_remote_copy(
            src_ref=kv_stage.at[step, j],
            dst_ref=kv.at[step, member],
            send_sem=kv_send.at[step, j],
            recv_sem=kv_recv.at[step, member],
            device_id=(plane * members + goal, first),
            device_id_type=MESH,
        )

    def forward_copy(step, source):
        return pltpu.make_async_remote_copy(
            src_ref=kv.at[step, source],
            dst_ref=kv.at[step, source],
            send_sem=forward_send.at[step, source],
            recv_sem=kv_recv.at[step, source],
            device_id=(sp, other),
            device_id_type=MESH,
        )

    def query_copy(step, j):
        core = jnp.where(top(step), 1, 0)
        return pltpu.make_async_remote_copy(
            src_ref=query_stage.at[step, j],
            dst_ref=queries.at[member],
            send_sem=query_send.at[step, j],
            recv_sem=query_recv.at[member],
            device_id=(plane * members + 2 * tp + j, core),
            device_id_type=MESH,
        )

    own_goal = across == tp

    def part(ch):
        return pl.ds(ch * half, half)

    def far_copy(step, ch, goal_side, j):
        slot = goal_side * 2 + j
        goal = (2 * upper + goal_side) * members + 2 * tp + j
        return pltpu.make_async_remote_copy(
            src_ref=far_stage.at[step - 2, slot, part(ch)],
            dst_ref=kv.at[step, member, part(ch)],
            send_sem=far_send.at[step - 2, slot, ch],
            recv_sem=far_recv.at[step - 2, member, ch],
            device_id=(goal, along),
            device_id_type=MESH,
        )

    def far_pass(step, source, ch):
        return pltpu.make_async_remote_copy(
            src_ref=kv.at[step, source, part(ch)],
            dst_ref=kv.at[step, source, part(ch)],
            send_sem=far_forward.at[step - 2, source, ch],
            recv_sem=far_recv.at[step - 2, source, ch],
            device_id=(sp, other),
            device_id_type=MESH,
        )

    def far_stays(goal_side, j):
        return jnp.logical_and(goal_side == side, jnp.logical_and(own_goal, j == along))

    def far_here(source):
        return jnp.logical_and(relays, source == member)

    def far_passes(source):
        return jnp.logical_and(source % 2 == tp, jnp.logical_not(far_here(source)))

    def far_awaits(source):
        return jnp.logical_not(jnp.logical_and(far_here(source), own_goal))

    def own_stays(step, j):
        return jnp.logical_and(own_goal, j == along)

    def query_stays(step, j):
        return jnp.logical_and(own_stays(step, j), jnp.where(top(step), 1, 0) == tp)

    def own_forwards(step):
        return jnp.logical_and(
            own_goal, jnp.logical_or(jnp.logical_not(top(step)), tp == 0)
        )

    def passes_on(step, source):
        mine = jnp.logical_and(source % 2 == tp, jnp.logical_not(top(step)))
        return jnp.logical_and(source != member, mine)

    def awaits(step, source):
        needed = jnp.logical_or(tp == 1, jnp.logical_not(top(step)))
        made_here = jnp.logical_and(source == member, own_goal)
        return jnp.logical_and(needed, jnp.logical_not(made_here))

    def contrast_stays(i):
        return jnp.logical_and(
            jnp.logical_and(query_band == plane, i == member), across == tp
        )

    head_here = 2 * side + along

    def contrast_copy(i):
        return pltpu.make_async_remote_copy(
            src_ref=contrast_stage.at[i],
            dst_ref=contrasts.at[head_here],
            send_sem=contrast_send.at[i],
            recv_sem=contrast_recv.at[head_here],
            device_id=(query_band * members + i, across),
            device_id_type=MESH,
        )

    def contrast_incoming(head):
        return pltpu.make_async_remote_copy(
            src_ref=contrast_stage.at[0],
            dst_ref=contrasts.at[head],
            send_sem=contrast_send.at[0],
            recv_sem=contrast_recv.at[head],
            device_id=(sp, other),
            device_id_type=MESH,
        )

    def contrast_local(head):
        same = jnp.logical_and(head // 2 == side, 2 * tp + head % 2 == member)
        return jnp.logical_and(same, side == tp)

    rim_copy = pltpu.make_async_remote_copy(
        src_ref=rim_stage,
        dst_ref=rim,
        send_sem=rim_send,
        recv_sem=rim_recv,
        device_id=(lax.rem(sp + 1, sp_count), tp),
        device_id_type=MESH,
    )
    out_copy = pltpu.make_async_remote_copy(
        src_ref=out_stage,
        dst_ref=out_recv,
        send_sem=out_send,
        recv_sem=out_recv_sem,
        device_id=(sp, other),
        device_id_type=MESH,
    )

    pair_first.start()
    for ch in range(chunks):
        swap(ch).start()

        @pl.when(crosses)
        def _(ch=ch):
            own_up(ch).start()

    peaks[...] = jnp.full(peaks.shape, -1e30, f32)
    totals[...] = jnp.zeros(totals.shape, f32)
    weighted[...] = jnp.zeros(weighted.shape, f32)

    def project(step):
        def one(t, carry):
            j = jnp.where(t == 0, 1 - along, along)
            columns = pl.ds(pl.multiple_of((2 * side + j) * width, width), width)
            x = rows_in[step].reshape(rows, model)
            mine = jnp.dot(x, query_w[:, columns], preferred_element_type=f32).astype(bf16)
            keys = jnp.dot(x, key_w[:, columns], preferred_element_type=f32).astype(bf16)
            values = jnp.dot(x, value_w[:, columns], preferred_element_type=f32).astype(bf16)
            kept = query_stays(step, j)
            stays = own_stays(step, j)

            @pl.when(jnp.logical_not(kept))
            def _():
                query_stage[step, j] = mine
                query_copy(step, j).start()

            @pl.when(kept)
            def _():
                queries[member] = mine

            @pl.when(jnp.logical_not(stays))
            def _():
                kv_stage[step, j, :, :width] = keys
                kv_stage[step, j, :, width:] = values
                kv_copy(step, j).start()

            @pl.when(stays)
            def _():
                kv[step, member, :, :width] = keys
                kv[step, member, :, width:] = values

                @pl.when(own_forwards(step))
                def _():
                    forward_copy(step, member).start()

            return carry

        lax.fori_loop(0, 2, one, 0)

    def project_far(step, ch):
        pair_copy(step, ch).wait_recv()

        def one(t, carry):
            goal_side = 1 - lax.div(t, 2)
            j = jnp.where(lax.rem(t, 2) == 0, 1 - along, along)
            columns = pl.ds(pl.multiple_of((2 * goal_side + j) * width, width), width)
            x = rows_in[step, :, cut(ch), :].reshape(half, model)
            keys = jnp.dot(x, key_w[:, columns], preferred_element_type=f32).astype(bf16)
            values = jnp.dot(x, value_w[:, columns], preferred_element_type=f32).astype(bf16)
            stays = far_stays(goal_side, j)

            @pl.when(jnp.logical_not(stays))
            def _():
                far_stage[step - 2, goal_side * 2 + j, part(ch), :width] = keys
                far_stage[step - 2, goal_side * 2 + j, part(ch), width:] = values
                far_copy(step, ch, goal_side, j).start()

            @pl.when(stays)
            def _():
                kv[step, member, part(ch), :width] = keys
                kv[step, member, part(ch), width:] = values
                far_pass(step, member, ch).start()

            return carry

        lax.fori_loop(0, 4, one, 0)

    def take_swap(ch):
        swap(ch).wait_recv()

        @pl.when(crosses)
        def _():
            low_up(ch).start()

        pair_copy(1, ch).start()

    def take_far(step, ch):
        (own_up(ch) if step == 2 else low_up(ch)).wait_recv()
        pair_copy(step, ch).start()

    def paired(step):
        for ch in range(chunks):
            pair_copy(step, ch).wait_recv()

    log_scale = head_dim ** (-0.5) * math.log2(math.e)

    def attend_block(step, i, seen, masked):
        for u in range(2):
            cols = slice(u * head_dim, (u + 1) * head_dim)
            keys = kv[step, :seen, :, cols].reshape(-1, head_dim)
            values = kv[step, :seen, :, width:].reshape(-1, width)
            scores = lax.dot_general(
                queries[i, :, cols], keys, (((1,), (1,)), ((), ())), preferred_element_type=f32
            )
            if masked:
                query_order = lax.broadcasted_iota(jnp.int32, scores.shape, 0) + (seen - 1) * rows
                key_order = lax.broadcasted_iota(jnp.int32, scores.shape, 1)
                scores = jnp.where(key_order <= query_order, scores, -jnp.inf)
            old = peaks[u, i][:, :1]
            peak = jnp.maximum(jnp.max(scores, axis=1, keepdims=True), old)
            shrink = jnp.exp2((old - peak) * log_scale)
            raised = jnp.exp2((scores - peak) * log_scale)
            total = jnp.sum(raised, axis=1, keepdims=True)
            update = jnp.dot(raised.astype(bf16), values, preferred_element_type=f32)
            total = total + totals[u, i][:, :1] * shrink
            update = update + weighted[u, i] * shrink
            peaks[u, i] = jnp.broadcast_to(peak, peaks.shape[2:])
            totals[u, i] = jnp.broadcast_to(total, totals.shape[2:])
            weighted[u, i] = update

    weight = balance[across * members + head_here]

    def finish(i):
        first = (weighted[0, i] / totals[0, i][:, :1]).astype(bf16).astype(f32)
        second = (weighted[1, i] / totals[1, i][:, :1]).astype(bf16).astype(f32)
        contrast = first - weight * second
        mean_square = jnp.mean(contrast * contrast, axis=1, keepdims=True)
        result = (contrast * lax.rsqrt(mean_square + norm_epsilon) * gain[...]).astype(bf16)
        stays = contrast_stays(i)

        @pl.when(jnp.logical_not(stays))
        def _():
            contrast_stage[i] = result
            contrast_copy(i).start()

        @pl.when(stays)
        def _():
            contrasts[head_here] = result

    def each_block(work):
        def one(t, carry):
            work(lax.rem(member + 1 + t, members))
            return carry

        lax.fori_loop(0, members, one, 0)

    def lands_here(step, source):
        return jnp.logical_and(
            source != member, jnp.where(top(step), 1, source % 2) == tp
        )

    def pass_on(step):
        for source in range(members):

            @pl.when(lands_here(step, source))
            def _(source=source):
                forward_copy(step, source).wait_recv()

            @pl.when(passes_on(step, source))
            def _(source=source):
                forward_copy(step, source).start()

    def arrive(step):
        for source in range(members):
            passed = jnp.logical_not(lands_here(step, source))

            @pl.when(jnp.logical_and(awaits(step, source), passed))
            def _(source=source):
                forward_copy(step, source).wait_recv()

    def attend(step):
        band = bands_of[step]

        @pl.when(band == query_band)
        def _():
            for i in range(members):
                attend_block(step, i, i + 1, True)

        @pl.when(band < query_band)
        def _():
            each_block(lambda i: attend_block(step, i, members, False))

    def far_pass_on(step, ch):
        for source in range(members):

            @pl.when(far_passes(source))
            def _(source=source):
                far_pass(step, source, ch).wait_recv()
                far_pass(step, source, ch).start()

    def far_arrive(step, ch):
        for source in range(members):
            passed = jnp.logical_not(far_passes(source))

            @pl.when(jnp.logical_and(far_awaits(source), passed))
            def _(source=source):
                far_pass(step, source, ch).wait_recv()

    keep.wait()
    loads[0].wait()
    loads[1].wait()
    loads[2].wait()
    pair_first.wait_recv()
    project(0)

    loads[3].wait()
    pool_input = jnp.dot(
        rows_in[0].reshape(rows, model), pool_in_w[...], preferred_element_type=f32
    ).astype(bf16)
    rim_stage[...] = pool_input[rows - rim.shape[0] :]

    @pl.when(sp + 1 < sp_count)
    def _():
        rim_copy.start()

    take_swap(0)

    @pl.when(relays)
    def _():
        take_far(2, 0)
        project_far(2, 0)

    take_swap(1)

    @pl.when(relays)
    def _():
        take_far(2, 1)

    paired(1)
    project(1)

    @pl.when(relays)
    def _():
        project_far(2, 1)
        take_far(3, 0)
        project_far(3, 0)

    @pl.when(sp > 0)
    def _():
        rim_copy.wait_recv()

    @pl.when(sp == 0)
    def _():
        rim[...] = jnp.zeros_like(rim)

    loads[4].wait()
    extended = jnp.concatenate([rim[...], pool_input], axis=0).astype(f32)
    group_width = pool_weight.shape[1]
    skirt = rim.shape[0]
    position = sp * rows + lax.broadcasted_iota(jnp.int32, (rows, group_width), 0)
    mixed = []
    for group in range(pool_weight.shape[0]):
        block = extended[:, group * group_width : (group + 1) * group_width]
        window = block
        reach = 1
        span = 2 ** (1 + group % 4)
        while reach < span:
            window = window + pltpu.roll(window, reach, 0)
            reach *= 2
        counts = jnp.minimum(position + 1, span).astype(f32)
        spread = (window[skirt:] / counts - block[skirt:]).astype(bf16)
        mixed.append(
            jnp.dot(spread, pool_weight[group], preferred_element_type=f32).astype(bf16)
        )
    pool_out = jnp.concatenate(mixed, axis=1)
    chunk = math.gcd(model, 512)
    for start in range(0, model, chunk):
        pool_part[:, start : start + chunk] = jnp.dot(
            pool_out, pool_out_w[:, start : start + chunk], preferred_element_type=f32
        )

    def query_incoming(source):
        return pltpu.make_async_remote_copy(
            src_ref=query_stage.at[0, 0],
            dst_ref=queries.at[source],
            send_sem=query_send.at[0, 0],
            recv_sem=query_recv.at[source],
            device_id=(sp, other),
            device_id_type=MESH,
        )

    def take_queries():
        for source in range(members):

            @pl.when(jnp.logical_not(jnp.logical_and(source == member, own_goal)))
            def _(source=source):
                query_incoming(source).wait_recv()

    pass_on(0)
    take_queries()
    arrive(0)
    attend(0)

    @pl.when(relays)
    def _():
        take_far(3, 1)
        project_far(3, 1)

    @pl.when(in_upper)
    def _():
        far_pass_on(2, 0)
        far_pass_on(2, 1)
        far_arrive(2, 0)
        far_arrive(2, 1)
        each_block(lambda i: attend_block(2, i, members, False))

    pass_on(1)

    @pl.when(in_upper)
    def _():
        far_pass_on(3, 0)

    arrive(1)
    attend(1)

    @pl.when(in_lower)
    def _():
        each_block(finish)

    @pl.when(in_upper)
    def _():
        far_pass_on(3, 1)
        far_arrive(3, 0)
        far_arrive(3, 1)

        def last(i):
            attend_block(3, i, members, False)
            finish(i)

        each_block(last)

    loads[5].wait()
    for head in range(members):

        @pl.when(jnp.logical_not(contrast_local(head)))
        def _(head=head):
            contrast_incoming(head).wait_recv()

    def projected(taken_side, store):
        taken = pl.ds(pl.multiple_of(taken_side * half, half), half)
        left = jnp.concatenate([contrasts[h, taken, :] for h in range(members)], axis=1)
        for start in range(0, model, chunk):
            span = slice(start, start + chunk)
            part = jnp.dot(left, contrast_w[:, span], preferred_element_type=f32)
            store(span, (part + pool_part[taken, span]).astype(bf16))

    def to_partner(span, part):
        out_stage[:, span] = part

    def to_self(span, part):
        out_ref[:, span] = part

    projected(other, to_partner)
    out_copy.start()
    projected(tp, to_self)
    out_copy.wait()

    pair_first.wait_send()
    for ch in range(chunks):
        swap(ch).wait_send()
        pair_copy(1, ch).wait_send()

        @pl.when(crosses)
        def _(ch=ch):
            own_up(ch).wait_send()
            low_up(ch).wait_send()

        @pl.when(relays)
        def _(ch=ch):
            for step in range(2, 4):
                pair_copy(step, ch).wait_send()
                for slot in range(4):

                    @pl.when(jnp.logical_not(far_stays(slot // 2, slot % 2)))
                    def _(step=step, slot=slot):
                        far_copy(step, ch, slot // 2, slot % 2).wait_send()

                @pl.when(own_goal)
                def _(step=step):
                    far_pass(step, member, ch).wait_send()

        @pl.when(in_upper)
        def _(ch=ch):
            for step in range(2, 4):
                for source in range(members):

                    @pl.when(far_passes(source))
                    def _(step=step, source=source):
                        far_pass(step, source, ch).wait_send()

    def drain(step):
        for j in range(2):

            @pl.when(jnp.logical_not(own_stays(step, j)))
            def _(j=j):
                kv_copy(step, j).wait_send()

            @pl.when(jnp.logical_not(query_stays(step, j)))
            def _(j=j):
                query_copy(step, j).wait_send()

        @pl.when(own_forwards(step))
        def _():
            forward_copy(step, member).wait_send()

        for source in range(members):

            @pl.when(passes_on(step, source))
            def _(source=source):
                forward_copy(step, source).wait_send()

    drain(0)
    drain(1)

    for i in range(members):

        @pl.when(jnp.logical_not(contrast_stays(i)))
        def _(i=i):
            contrast_copy(i).wait_send()

    @pl.when(sp + 1 < sp_count)
    def _():
        rim_copy.wait_send()


def kernel_scratch(members, half, model, width, pool_cols):
    bf16 = jnp.bfloat16
    rows = 2 * half
    dma = pltpu.SemaphoreType.DMA
    return [
        pltpu.VMEM((model, members * width), bf16),
        pltpu.VMEM((model, members * width), bf16),
        pltpu.VMEM((model, members * width), bf16),
        pltpu.VMEM((model, pool_cols), bf16),
        pltpu.VMEM((members * width, model), bf16),
        pltpu.VMEM((pool_cols, model), bf16),
        pltpu.VMEM((4, 2, half, model), bf16),
        pltpu.VMEM((4, members, rows, 2 * width), bf16),
        pltpu.VMEM((2, 2, rows, 2 * width), bf16),
        pltpu.VMEM((2, 4, rows, 2 * width), bf16),
        pltpu.VMEM((members, rows, width), bf16),
        pltpu.VMEM((2, 2, rows, width), bf16),
        pltpu.VMEM((2, members, rows, 128), jnp.float32),
        pltpu.VMEM((2, members, rows, 128), jnp.float32),
        pltpu.VMEM((2, members, rows, width), jnp.float32),
        pltpu.VMEM((members, rows, width), bf16),
        pltpu.VMEM((members, rows, width), bf16),
        pltpu.VMEM((reach_back + 1, pool_cols), bf16),
        pltpu.VMEM((reach_back + 1, pool_cols), bf16),
        pltpu.VMEM((rows, model), jnp.float32),
        pltpu.VMEM((half, model), bf16),
        dma((6,)),
        dma,
        dma((4, 2)),
        dma((4, 2)),
        dma((4, 2)),
        dma((4, 2)),
        dma((2, 2)),
        dma((2, members)),
        dma((2, members)),
        dma((2, 4, 2)),
        dma((2, members, 2)),
        dma((2, members, 2)),
        dma((2, 2)),
        dma((members,)),
        dma((members,)),
        dma((members,)),
        dma,
        dma,
        dma,
        dma,
    ]


vmem_most = 67043328


def scratch_bytes(scratch):
    return sum(
        math.prod(item.shape) * jnp.dtype(item.dtype).itemsize
        for item in scratch
        if getattr(item, "memory_space", None) == pltpu.VMEM
    )


def whole_layer(
    normed,
    query_weight,
    key_weight,
    value_weight,
    pool_in_weight,
    pool_weight,
    map_balance,
    head_gain,
    contrast_out_weight,
    pool_out_weight,
):
    sp_count = lax.axis_size("sp")
    width = head_gain.shape[0]
    members = query_weight.shape[1] // width
    half, model = normed.shape
    pool_cols = pool_in_weight.shape[1]
    groups_here = pool_weight.shape[0]
    scratch = kernel_scratch(max(members, 1), half, model, width, pool_cols)
    fits = (
        lax.axis_size("tp") == 2
        and members == 4
        and sp_count == 4 * members
        and groups_here % 4 == 0
        and scratch_bytes(scratch) < vmem_most * 3 // 4
    )
    if not fits:
        return per_device(
            normed,
            query_weight,
            key_weight,
            value_weight,
            pool_in_weight,
            pool_weight,
            map_balance,
            head_gain,
            contrast_out_weight,
            pool_out_weight,
        )
    vmem = pl.BlockSpec(memory_space=pltpu.VMEM)
    hbm = pl.BlockSpec(memory_space=pl.ANY)
    own_part, partner_part = pl.pallas_call(
        functools.partial(layer_kernel, sp_count, members),
        out_shape=[jax.ShapeDtypeStruct((half, model), jnp.bfloat16)] * 2,
        in_specs=[vmem, vmem, pl.BlockSpec(memory_space=pltpu.SMEM), vmem] + [hbm] * 6,
        out_specs=[vmem, vmem],
        scratch_shapes=scratch,
        compiler_params=pltpu.CompilerParams(
            collective_id=0, has_side_effects=True, vmem_limit_bytes=vmem_most
        ),
    )(
        normed,
        pool_weight,
        map_balance,
        head_gain.reshape(1, width),
        query_weight,
        key_weight,
        value_weight,
        pool_in_weight,
        contrast_out_weight,
        pool_out_weight,
    )
    return (own_part.astype(jnp.float32) + partner_part.astype(jnp.float32)).astype(jnp.bfloat16)


def solution(mesh):
    return jax.shard_map(
        whole_layer,
        mesh=mesh,
        in_specs=(
            P(("sp", "tp"), None),
            P(None, "tp"),
            P(None, "tp"),
            P(None, "tp"),
            P(None, "tp"),
            P("tp", None, None),
            P(),
            P(),
            P("tp", None),
            P("tp", None),
        ),
        out_specs=P(("sp", "tp"), None),
        check_vma=False,
    )
```

```python
import functools
import math

import jax
import jax.numpy as jnp
from jax import lax
from jax.experimental import pallas as pl
from jax.experimental.pallas import tpu as pltpu
from jax.sharding import PartitionSpec as P

reach_back = 15
norm_epsilon = 1e-06


def passed_along(block, axis, distance):
    devices = range(lax.axis_size(axis))
    route = [(i - distance, i) for i in devices if i - distance in devices]
    return lax.ppermute(block, axis, route)


def from_partner(block, axis, stride):
    count = lax.axis_size(axis)
    route = []
    for low in range(count):
        high = low | 1 << stride
        if high != low and high < count:
            route += [(low, high), (high, low)]
    return lax.ppermute(block, axis, route)


def shifted(array, axis, by):
    size = lax.axis_size(axis)
    return lax.ppermute(array, axis, [(i, (i + by) % size) for i in range(size)])


def as_sent(array):

    def short(part):
        return part.astype(jnp.bfloat16) if part.dtype == jnp.float32 else part

    return jax.tree.map(short, array)


def attend(running, queries, key_rows, value_rows, query_first, key_first, score_scale):
    key_count = key_rows.shape[0]
    key_block = math.gcd(key_count, 1024)
    unit_count = queries.shape[1]
    heads_here = value_rows.shape[1]
    per_head = unit_count // heads_here
    query_count = queries.shape[0]
    query_order = query_first + lax.iota(jnp.int32, query_count)

    def key_step(block_index, carried):
        block_start = block_index * key_block

        def block_work(current):
            row_peak, row_total, weighted = current
            scores = (
                jnp.einsum("qud,kud->uqk", queries, key_rows, preferred_element_type=jnp.float32)
                * score_scale
            )
            key_order = key_first + block_start + lax.iota(jnp.int32, key_block)
            scores = jnp.where(
                key_order[None, None, :] <= query_order[None, :, None], scores, -jnp.inf
            )
            new_peak = jnp.maximum(row_peak, jnp.max(scores, axis=2))
            shrink = jnp.exp(row_peak - new_peak)
            raised = jnp.exp(scores - new_peak[:, :, None])
            row_total = row_total * shrink + jnp.sum(raised, axis=2)
            map_weights = raised.astype(jnp.bfloat16).reshape(
                heads_here, per_head, query_count, key_block
            )
            update = jnp.einsum(
                "hmqk,khe->hmqe", map_weights, value_rows, preferred_element_type=jnp.float32
            )
            weighted = weighted * shrink[:, :, None] + update.reshape(unit_count, query_count, -1)
            return (new_peak, row_total, weighted)

        def keep_state(current):
            return current

        return lax.cond(
            key_first + block_start <= query_first + query_count - 1,
            block_work,
            keep_state,
            carried,
        )

    return lax.fori_loop(0, key_count // key_block, key_step, running)


def fresh_state(unit_count, row_count, value_width):
    return (
        jnp.full((unit_count, row_count), -1e30, jnp.float32),
        jnp.zeros((unit_count, row_count), jnp.float32),
        jnp.zeros((unit_count, row_count, value_width), jnp.float32),
    )


def finished(running):
    row_peak, row_total, weighted = running
    return (weighted / row_total[:, :, None]).astype(jnp.bfloat16)


def joined_state(first, second):
    first_peak, first_total, first_weighted = first
    second_peak, second_total, second_weighted = second
    new_peak = jnp.maximum(first_peak, second_peak)
    first_shrink = jnp.exp(first_peak - new_peak)
    second_shrink = jnp.exp(second_peak - new_peak)
    new_total = first_total * first_shrink + second_total * second_shrink
    new_weighted = (
        first_weighted * first_shrink[:, :, None] + second_weighted * second_shrink[:, :, None]
    )
    return (new_peak, new_total, new_weighted)


def per_device(
    normed,
    query_weight,
    key_weight,
    value_weight,
    pool_in_weight,
    pool_weight,
    map_balance,
    head_gain,
    contrast_out_weight,
    pool_out_weight,
):
    tp_index = lax.axis_index("tp")
    sp_count = lax.axis_size("sp")
    sp_index = lax.axis_index("sp")
    head_dim = head_gain.shape[0] // 2
    value_width = 2 * head_dim
    query_cols = query_weight.shape[1]
    value_cols = value_weight.shape[1]
    unit_count = query_cols // head_dim
    heads_here = unit_count // 2
    project_incoming = lax.all_gather(normed, "tp", axis=0, tiled=True)
    products = [
        jnp.dot(project_incoming, weight_part, preferred_element_type=jnp.float32)
        for weight_part in (query_weight, key_weight, value_weight, pool_in_weight)
    ]
    joined = jnp.concatenate(products, axis=1).astype(jnp.bfloat16)
    row_count = joined.shape[0]
    queries = joined[:, :query_cols].reshape(row_count, unit_count, head_dim)
    key_rows = joined[:, query_cols : 2 * query_cols].reshape(row_count, unit_count, head_dim)
    value_rows = joined[:, 2 * query_cols : 2 * query_cols + value_cols].reshape(
        row_count, heads_here, value_width
    )
    pool_input = joined[:, 2 * query_cols + value_cols :]
    pool_cols = pool_input.shape[1]
    upper_rim = passed_along(pool_input[row_count - reach_back :], "sp", 1)
    extended = jnp.concatenate([upper_rim, pool_input], axis=0).astype(jnp.float32)
    groups_here = pool_weight.shape[0]
    group_width = pool_weight.shape[1]
    group_index = tp_index * groups_here + lax.iota(jnp.int32, pool_cols) // group_width
    widths = jnp.left_shift(jnp.int32(2), group_index % 4)
    window_sum = jnp.zeros((row_count, pool_cols), jnp.float32)
    for offset in range(reach_back + 1):
        window_sum = window_sum + extended[
            reach_back - offset : reach_back - offset + row_count
        ] * (offset < widths)[None, :].astype(jnp.float32)
    position = sp_index * row_count + lax.iota(jnp.int32, row_count)
    counts = jnp.minimum(position[:, None] + 1, widths[None, :]).astype(jnp.float32)
    spread = (window_sum / counts - extended[reach_back:]).astype(jnp.bfloat16)
    mixed_groups = jnp.einsum(
        "tgc,gce->tge",
        spread.reshape(row_count, groups_here, group_width),
        pool_weight,
        preferred_element_type=jnp.float32,
    )
    pool_out = mixed_groups.reshape(row_count, pool_cols).astype(jnp.bfloat16)
    score_scale = head_dim ** (-0.5)
    level_count = sp_count.bit_length() - 1
    low_levels = level_count // 2
    band_size = 1 << low_levels
    band_count = sp_count // band_size
    member = sp_index % band_size
    band = sp_index // band_size
    band_queries = queries
    for bit in range(low_levels):
        received = from_partner(band_queries, "sp", bit)
        upper = member >> bit & 1 == 1
        band_queries = jnp.where(
            upper,
            jnp.concatenate([received, band_queries], axis=0),
            jnp.concatenate([band_queries, received], axis=0),
        )
    band_first = band * band_size * row_count
    running = fresh_state(unit_count, band_size * row_count, value_width)
    for step in range(band_count):
        if step == 0:
            key_piece, value_piece = (key_rows, value_rows)
        else:
            key_piece, value_piece = shifted((key_rows, value_rows), "sp", step * band_size)
        source = (sp_index - step * band_size) % sp_count
        running = attend(
            running,
            band_queries,
            key_piece,
            value_piece,
            band_first,
            source * row_count,
            score_scale,
        )
    for bit in range(low_levels - 1, -1, -1):
        half = running[0].shape[1] // 2
        upper = member >> bit & 1 == 1
        lower_part = jax.tree.map(lambda item: item[:, :half], running)
        upper_part = jax.tree.map(lambda item: item[:, half:], running)
        outgoing = jax.tree.map(
            lambda low, high: jnp.where(upper, low, high), lower_part, upper_part
        )
        kept = jax.tree.map(lambda low, high: jnp.where(upper, high, low), lower_part, upper_part)
        incoming = from_partner(
            (as_sent(outgoing[0]), as_sent(outgoing[1]), as_sent(outgoing[2])), "sp", bit
        )
        running = joined_state(kept, incoming)
    maps = finished(running)
    paired = maps.reshape(heads_here, 2, row_count, value_width)
    paired = lax.optimization_barrier(paired).astype(jnp.float32)
    head_first = tp_index * heads_here
    balance_here = lax.dynamic_slice_in_dim(map_balance, head_first, heads_here, 0)
    contrast = paired[:, 0] - balance_here[:, None, None] * paired[:, 1]
    mean_square = jnp.mean(contrast * contrast, axis=2, keepdims=True)
    contrast = contrast * lax.rsqrt(mean_square + norm_epsilon) * head_gain
    contrast_out = (
        contrast.astype(jnp.bfloat16)
        .transpose(1, 0, 2)
        .reshape(row_count, heads_here * value_width)
    )
    partial_value = jnp.dot(contrast_out, contrast_out_weight, preferred_element_type=jnp.float32)
    return lax.psum_scatter(
        (
            partial_value + jnp.dot(pool_out, pool_out_weight, preferred_element_type=jnp.float32)
        ).astype(jnp.bfloat16),
        "tp",
        scatter_dimension=0,
        tiled=True,
    )


MESH = pl.DeviceIdType.MESH


def layer_kernel(
    sp_count,
    members,
    x_ref,
    pool_weight,
    balance,
    gain,
    query_hbm,
    key_hbm,
    value_hbm,
    pool_in_hbm,
    contrast_hbm,
    pool_out_hbm,
    out_ref,
    out_recv,
    query_w,
    key_w,
    value_w,
    pool_in_w,
    contrast_w,
    pool_out_w,
    rows_in,
    kv,
    kv_stage,
    far_stage,
    queries,
    query_stage,
    peaks,
    totals,
    weighted,
    contrasts,
    contrast_stage,
    rim,
    rim_stage,
    pool_part,
    out_stage,
    weight_sem,
    local_sem,
    pair_send,
    pair_recv,
    relay_send,
    relay_recv,
    kv_send,
    kv_recv,
    forward_send,
    far_send,
    far_recv,
    far_forward,
    query_send,
    query_recv,
    contrast_send,
    contrast_recv,
    rim_send,
    rim_recv,
    out_send,
    out_recv_sem,
):
    f32 = jnp.float32
    bf16 = jnp.bfloat16
    sp = lax.axis_index("sp")
    tp = lax.axis_index("tp")
    other = 1 - tp
    plane = lax.div(sp, members)
    member = lax.rem(sp, members)
    upper = lax.div(plane, 2)
    side = lax.rem(plane, 2)
    across = lax.div(member, 2)
    along = lax.rem(member, 2)
    half_count = 2 * members
    half, model = x_ref.shape
    rows = 2 * half
    width = gain.shape[1]
    head_dim = width // 2
    chunk = math.gcd(model, 512)
    chunks = 2
    piece = half // chunks
    in_lower = upper == 0
    in_upper = upper == 1
    crosses = plane == 1
    relays = plane == 2
    query_band = 2 * upper + tp
    bands_of = (plane, plane + 1 - 2 * side)

    loads = [
        pltpu.make_async_copy(src, dst, weight_sem.at[i])
        for i, (src, dst) in enumerate(
            (
                (key_hbm, key_w),
                (value_hbm, value_w),
                (query_hbm, query_w),
                (pool_in_hbm, pool_in_w),
                (pool_out_hbm, pool_out_w),
                (contrast_hbm, contrast_w),
            )
        )
    ]
    for load in loads:
        load.start()
    keep = pltpu.make_async_copy(x_ref, rows_in.at[0, tp], local_sem)
    keep.start()

    barrier = pltpu.get_barrier_semaphore()

    def greet(target):
        pl.semaphore_signal(barrier, inc=1, device_id=target, device_id_type=MESH)

    place = (side * members + member) * 2 + tp
    for d in range(1, 2 * half_count):
        goal = lax.rem(place + d, 2 * half_count)
        greet((upper * half_count + lax.div(goal, 2), lax.rem(goal, 2)))

    @pl.when(crosses)
    def _():
        greet((sp + members, tp))

    @pl.when(relays)
    def _():
        greet((sp - members, tp))

    @pl.when(sp == half_count - 1)
    def _():
        greet((sp + 1, tp))

    @pl.when(sp == half_count)
    def _():
        greet((sp - 1, tp))

    extra = jnp.where(jnp.logical_or(crosses, relays), 1, 0)
    extra = extra + jnp.where(jnp.logical_or(sp == half_count - 1, sp == half_count), 1, 0)
    pl.semaphore_wait(barrier, 2 * half_count - 1 + extra)

    def cut(ch):
        return pl.ds(ch * piece, piece)

    pair_first = pltpu.make_async_remote_copy(
        src_ref=x_ref,
        dst_ref=rows_in.at[0, tp],
        send_sem=pair_send.at[0, 0],
        recv_sem=pair_recv.at[0, 0],
        device_id=(sp, other),
        device_id_type=MESH,
    )

    def pair_copy(step, ch):
        return pltpu.make_async_remote_copy(
            src_ref=rows_in.at[step, tp, cut(ch)],
            dst_ref=rows_in.at[step, tp, cut(ch)],
            send_sem=pair_send.at[step, ch],
            recv_sem=pair_recv.at[step, ch],
            device_id=(sp, other),
            device_id_type=MESH,
        )

    def relay_copy(src, step, ch, target):
        return pltpu.make_async_remote_copy(
            src_ref=src.at[cut(ch)],
            dst_ref=rows_in.at[step, tp, cut(ch)],
            send_sem=relay_send.at[step, ch],
            recv_sem=relay_recv.at[step, ch],
            device_id=(target, tp),
            device_id_type=MESH,
        )

    def swap(ch):
        return relay_copy(x_ref, 1, ch, sp + members * (1 - 2 * side))

    def own_up(ch):
        return relay_copy(x_ref, 2, ch, sp + members)

    def low_up(ch):
        return relay_copy(rows_in.at[1, tp], 3, ch, sp + members)

    def top(step):
        return side == (1 if step == 0 else 0)

    def kv_copy(step, j, ch):
        goal = 2 * tp + j
        first = jnp.where(top(step), 1, along)
        return pltpu.make_async_remote_copy(
            src_ref=kv_stage.at[step, j, :, cut(ch)],
            dst_ref=kv.at[step, member, :, cut(ch)],
            send_sem=kv_send.at[step, j, ch],
            recv_sem=kv_recv.at[step, member, ch],
            device_id=(plane * members + goal, first),
            device_id_type=MESH,
        )

    def forward_copy(step, source, ch):
        return pltpu.make_async_remote_copy(
            src_ref=kv.at[step, source, :, cut(ch)],
            dst_ref=kv.at[step, source, :, cut(ch)],
            send_sem=forward_send.at[step, source, ch],
            recv_sem=kv_recv.at[step, source, ch],
            device_id=(sp, other),
            device_id_type=MESH,
        )

    def query_copy(step, j, ch):
        core = jnp.where(top(step), 1, 0)
        return pltpu.make_async_remote_copy(
            src_ref=query_stage.at[step, j, :, cut(ch)],
            dst_ref=queries.at[member, :, cut(ch)],
            send_sem=query_send.at[step, j, ch],
            recv_sem=query_recv.at[member, ch],
            device_id=(plane * members + 2 * tp + j, core),
            device_id_type=MESH,
        )

    own_goal = across == tp

    def far_copy(step, ch, goal_side, j):
        slot = goal_side * 2 + j
        goal = (2 * upper + goal_side) * members + 2 * tp + j
        return pltpu.make_async_remote_copy(
            src_ref=far_stage.at[step - 2, slot, ch],
            dst_ref=kv.at[step, member, ch],
            send_sem=far_send.at[step - 2, slot, ch],
            recv_sem=far_recv.at[step - 2, member, ch],
            device_id=(goal, along),
            device_id_type=MESH,
        )

    def far_pass(step, source, ch):
        return pltpu.make_async_remote_copy(
            src_ref=kv.at[step, source, ch],
            dst_ref=kv.at[step, source, ch],
            send_sem=far_forward.at[step - 2, source, ch],
            recv_sem=far_recv.at[step - 2, source, ch],
            device_id=(sp, other),
            device_id_type=MESH,
        )

    def far_stays(goal_side, j):
        return jnp.logical_and(goal_side == side, jnp.logical_and(own_goal, j == along))

    def far_here(source):
        return jnp.logical_and(relays, source == member)

    def far_passes(source):
        return jnp.logical_and(source % 2 == tp, jnp.logical_not(far_here(source)))

    def far_awaits(source):
        return jnp.logical_not(jnp.logical_and(far_here(source), own_goal))

    def own_stays(step, j):
        return jnp.logical_and(own_goal, j == along)

    def query_stays(step, j):
        return jnp.logical_and(own_stays(step, j), jnp.where(top(step), 1, 0) == tp)

    def own_forwards(step):
        return jnp.logical_and(
            own_goal, jnp.logical_or(jnp.logical_not(top(step)), tp == 0)
        )

    def passes_on(step, source):
        mine = jnp.logical_and(source % 2 == tp, jnp.logical_not(top(step)))
        return jnp.logical_and(source != member, mine)

    def awaits(step, source):
        needed = jnp.logical_or(tp == 1, jnp.logical_not(top(step)))
        made_here = jnp.logical_and(source == member, own_goal)
        return jnp.logical_and(needed, jnp.logical_not(made_here))

    def contrast_stays(i):
        return jnp.logical_and(
            jnp.logical_and(query_band == plane, i == member), across == tp
        )

    head_here = 2 * side + along

    def contrast_copy(i):
        return pltpu.make_async_remote_copy(
            src_ref=contrast_stage.at[i],
            dst_ref=contrasts.at[head_here],
            send_sem=contrast_send.at[i],
            recv_sem=contrast_recv.at[head_here],
            device_id=(query_band * members + i, across),
            device_id_type=MESH,
        )

    def contrast_incoming(head):
        return pltpu.make_async_remote_copy(
            src_ref=contrast_stage.at[0],
            dst_ref=contrasts.at[head],
            send_sem=contrast_send.at[0],
            recv_sem=contrast_recv.at[head],
            device_id=(sp, other),
            device_id_type=MESH,
        )

    def contrast_local(head):
        same = jnp.logical_and(head // 2 == side, 2 * tp + head % 2 == member)
        return jnp.logical_and(same, side == tp)

    rim_copy = pltpu.make_async_remote_copy(
        src_ref=rim_stage,
        dst_ref=rim,
        send_sem=rim_send,
        recv_sem=rim_recv,
        device_id=(lax.rem(sp + 1, sp_count), tp),
        device_id_type=MESH,
    )

    def out_copy(start):
        span = slice(start, start + chunk)
        return pltpu.make_async_remote_copy(
            src_ref=out_stage.at[:, span],
            dst_ref=out_recv.at[:, span],
            send_sem=out_send.at[start // chunk],
            recv_sem=out_recv_sem.at[start // chunk],
            device_id=(sp, other),
            device_id_type=MESH,
        )


    pair_first.start()
    for ch in range(chunks):
        swap(ch).start()

        @pl.when(crosses)
        def _(ch=ch):
            own_up(ch).start()

    peaks[...] = jnp.full(peaks.shape, -1e30, f32)
    totals[...] = jnp.zeros(totals.shape, f32)
    weighted[...] = jnp.zeros(weighted.shape, f32)

    def project(step, pieces):
        here = cut(pieces[0]) if len(pieces) == 1 else slice(None)

        def one(t, carry):
            j = jnp.where(t == 0, 1 - along, along)
            columns = pl.ds(pl.multiple_of((2 * side + j) * width, width), width)
            x = rows_in[step, :, here, :].reshape(-1, model)

            def through(held):
                dot = jnp.dot(x, held[:, columns], preferred_element_type=f32)
                return dot.astype(bf16).reshape(2, -1, width)

            mine = through(query_w)
            keys = through(key_w)
            values = through(value_w)
            kept = query_stays(step, j)
            stays = own_stays(step, j)

            @pl.when(jnp.logical_not(kept))
            def _():
                query_stage[step, j, :, here] = mine
                for ch in pieces:
                    query_copy(step, j, ch).start()

            @pl.when(kept)
            def _():
                queries[member, :, here] = mine

            @pl.when(jnp.logical_not(stays))
            def _():
                kv_stage[step, j, :, here, :width] = keys
                kv_stage[step, j, :, here, width:] = values
                for ch in pieces:
                    kv_copy(step, j, ch).start()

            @pl.when(stays)
            def _():
                kv[step, member, :, here, :width] = keys
                kv[step, member, :, here, width:] = values

                @pl.when(own_forwards(step))
                def _():
                    for ch in pieces:
                        forward_copy(step, member, ch).start()

            return carry

        lax.fori_loop(0, 2, one, 0)

    def project_far(step, ch):
        pair_copy(step, ch).wait_recv()

        def one(t, carry):
            goal_side = 1 - lax.div(t, 2)
            j = jnp.where(lax.rem(t, 2) == 0, 1 - along, along)
            columns = pl.ds(pl.multiple_of((2 * goal_side + j) * width, width), width)
            x = rows_in[step, :, cut(ch), :].reshape(half, model)
            keys = jnp.dot(x, key_w[:, columns], preferred_element_type=f32).astype(bf16)
            values = jnp.dot(x, value_w[:, columns], preferred_element_type=f32).astype(bf16)
            stays = far_stays(goal_side, j)

            @pl.when(jnp.logical_not(stays))
            def _():
                far_stage[step - 2, goal_side * 2 + j, ch, :, :width] = keys
                far_stage[step - 2, goal_side * 2 + j, ch, :, width:] = values
                far_copy(step, ch, goal_side, j).start()

            @pl.when(stays)
            def _():
                kv[step, member, ch, :, :width] = keys
                kv[step, member, ch, :, width:] = values
                far_pass(step, member, ch).start()

            return carry

        lax.fori_loop(0, 4, one, 0)

    def take_swap(ch):
        swap(ch).wait_recv()

        @pl.when(crosses)
        def _():
            low_up(ch).start()

        pair_copy(1, ch).start()

    def take_far(step, ch):
        (own_up(ch) if step == 2 else low_up(ch)).wait_recv()
        pair_copy(step, ch).start()

    def project_swap(ch):
        pair_copy(1, ch).wait_recv()
        project(1, (ch,))

    log_scale = head_dim ** (-0.5) * math.log2(math.e)

    def attend_block(step, i, seen, masked):
        for u in range(2):
            cols = slice(u * head_dim, (u + 1) * head_dim)
            keys = kv[step, :seen, :, :, cols].reshape(-1, head_dim)
            values = kv[step, :seen, :, :, width:].reshape(-1, width)
            scores = lax.dot_general(
                queries[i, :, :, cols].reshape(rows, head_dim), keys, (((1,), (1,)), ((), ())), preferred_element_type=f32
            )
            if masked:
                query_order = lax.broadcasted_iota(jnp.int32, scores.shape, 0) + (seen - 1) * rows
                key_order = lax.broadcasted_iota(jnp.int32, scores.shape, 1)
                scores = jnp.where(key_order <= query_order, scores, -jnp.inf)
            old = peaks[u, i][:, :1]
            peak = jnp.maximum(jnp.max(scores, axis=1, keepdims=True), old)
            shrink = jnp.exp2((old - peak) * log_scale)
            raised = jnp.exp2((scores - peak) * log_scale)
            total = jnp.sum(raised, axis=1, keepdims=True)
            update = jnp.dot(raised.astype(bf16), values, preferred_element_type=f32)
            total = total + totals[u, i][:, :1] * shrink
            update = update + weighted[u, i] * shrink
            peaks[u, i] = jnp.broadcast_to(peak, peaks.shape[2:])
            totals[u, i] = jnp.broadcast_to(total, totals.shape[2:])
            weighted[u, i] = update

    weight = balance[across * members + head_here]

    def finished_block(i):
        first = (weighted[0, i] / totals[0, i][:, :1]).astype(bf16).astype(f32)
        second = (weighted[1, i] / totals[1, i][:, :1]).astype(bf16).astype(f32)
        contrast = first - weight * second
        mean_square = jnp.mean(contrast * contrast, axis=1, keepdims=True)
        return (contrast * lax.rsqrt(mean_square + norm_epsilon) * gain[...]).astype(bf16)

    def send_block(i, result):
        stays = contrast_stays(i)

        @pl.when(jnp.logical_not(stays))
        def _():
            contrast_stage[i] = result
            contrast_copy(i).start()

        @pl.when(stays)
        def _():
            contrasts[head_here] = result

    def turn(t):
        return lax.rem(member + 1 + t, members)

    def block_pairs(work):
        def one(t, carry):
            work(turn(2 * t), turn(2 * t + 1))
            return carry

        lax.fori_loop(0, members // 2, one, 0)

    def finish_pair(i, k):
        results = finished_block(i), finished_block(k)
        send_block(i, results[0])
        send_block(k, results[1])

    def lands_here(step, source):
        return jnp.logical_and(
            source != member, jnp.where(top(step), 1, source % 2) == tp
        )

    def pass_on(step):
        for ch in range(chunks):
            for source in range(members):

                @pl.when(lands_here(step, source))
                def _(source=source, ch=ch):
                    forward_copy(step, source, ch).wait_recv()

                @pl.when(passes_on(step, source))
                def _(source=source, ch=ch):
                    forward_copy(step, source, ch).start()

    def arrive(step):
        for ch in range(chunks):
            for source in range(members):
                passed = jnp.logical_not(lands_here(step, source))

                @pl.when(jnp.logical_and(awaits(step, source), passed))
                def _(source=source, ch=ch):
                    forward_copy(step, source, ch).wait_recv()

    def attend(step):
        band = bands_of[step]

        def between():
            if step == 0:

                @pl.when(relays)
                def _():
                    take_far(3, 1)

        @pl.when(band == query_band)
        def _():
            for i in range(members):
                if i == members // 2:
                    between()
                attend_block(step, i, i + 1, True)

        @pl.when(band < query_band)
        def _():
            def one(t, carry):
                attend_block(step, turn(2 * t), members, False)
                attend_block(step, turn(2 * t + 1), members, False)

                @pl.when(t == 0)
                def _():
                    between()

                return carry

            lax.fori_loop(0, members // 2, one, 0)

    def far_pass_on(step, ch):
        for source in range(members):

            @pl.when(far_passes(source))
            def _(source=source):
                far_pass(step, source, ch).wait_recv()
                far_pass(step, source, ch).start()

    def far_arrive(step, ch):
        for source in range(members):
            passed = jnp.logical_not(far_passes(source))

            @pl.when(jnp.logical_and(far_awaits(source), passed))
            def _(source=source):
                far_pass(step, source, ch).wait_recv()

    keep.wait()
    loads[0].wait()
    loads[1].wait()
    loads[2].wait()
    pair_first.wait_recv()
    project(0, tuple(range(chunks)))

    loads[3].wait()
    pool_input = jnp.dot(
        rows_in[0].reshape(rows, model), pool_in_w[...], preferred_element_type=f32
    ).astype(bf16)
    rim_stage[...] = pool_input[rows - rim.shape[0] :]

    @pl.when(sp + 1 < sp_count)
    def _():
        rim_copy.start()

    take_swap(0)

    @pl.when(relays)
    def _():
        take_far(2, 0)

    project_swap(0)

    @pl.when(relays)
    def _():
        project_far(2, 0)

    take_swap(1)

    @pl.when(relays)
    def _():
        take_far(2, 1)

    project_swap(1)

    @pl.when(relays)
    def _():
        project_far(2, 1)
        take_far(3, 0)

    pass_on(0)

    @pl.when(relays)
    def _():
        project_far(3, 0)

    def query_incoming(source, ch):
        return pltpu.make_async_remote_copy(
            src_ref=query_stage.at[0, 0, :, cut(ch)],
            dst_ref=queries.at[source, :, cut(ch)],
            send_sem=query_send.at[0, 0, ch],
            recv_sem=query_recv.at[source, ch],
            device_id=(sp, other),
            device_id_type=MESH,
        )

    def take_queries():
        for source in range(members):

            @pl.when(jnp.logical_not(jnp.logical_and(source == member, own_goal)))
            def _(source=source):
                for ch in range(chunks):
                    query_incoming(source, ch).wait_recv()

    idle_first = jnp.logical_and(in_upper, jnp.logical_and(side == 1, tp == 0))

    @pl.when(idle_first)
    def _():
        far_pass_on(2, 0)
        far_pass_on(2, 1)

    take_queries()
    arrive(0)
    attend(0)

    @pl.when(relays)
    def _():
        project_far(3, 1)

    def far_pair(i, k):
        attend_block(2, i, members, False)
        attend_block(2, k, members, False)

    @pl.when(in_upper)
    def _():
        @pl.when(jnp.logical_not(idle_first))
        def _():
            far_pass_on(2, 0)
            far_pass_on(2, 1)

        far_arrive(2, 0)
        far_arrive(2, 1)
        block_pairs(far_pair)

    pass_on(1)

    @pl.when(in_upper)
    def _():
        far_pass_on(3, 0)

    arrive(1)
    attend(1)

    @pl.when(in_lower)
    def _():
        block_pairs(finish_pair)

    @pl.when(in_upper)
    def _():
        far_pass_on(3, 1)
        far_arrive(3, 0)
        far_arrive(3, 1)

        def last_pair(i, k):
            attend_block(3, i, members, False)
            attend_block(3, k, members, False)
            finish_pair(i, k)

        block_pairs(last_pair)

    @pl.when(sp > 0)
    def _():
        rim_copy.wait_recv()

    @pl.when(sp == 0)
    def _():
        rim[...] = jnp.zeros_like(rim)

    loads[4].wait()
    extended = jnp.concatenate([rim[...], pool_input], axis=0).astype(f32)
    group_width = pool_weight.shape[1]
    skirt = rim.shape[0]
    position = sp * rows + lax.broadcasted_iota(jnp.int32, (rows, group_width), 0)
    mixed = []
    for group in range(pool_weight.shape[0]):
        block = extended[:, group * group_width : (group + 1) * group_width]
        window = block
        reach = 1
        span = 2 ** (1 + group % 4)
        while reach < span:
            window = window + pltpu.roll(window, reach, 0)
            reach *= 2
        counts = jnp.minimum(position + 1, span).astype(f32)
        spread = (window[skirt:] / counts - block[skirt:]).astype(bf16)
        mixed.append(
            jnp.dot(spread, pool_weight[group], preferred_element_type=f32).astype(bf16)
        )
    pool_out = jnp.concatenate(mixed, axis=1)
    for start in range(0, model, chunk):
        pool_part[:, start : start + chunk] = jnp.dot(
            pool_out, pool_out_w[:, start : start + chunk], preferred_element_type=f32
        )

    loads[5].wait()
    for head in range(members):

        @pl.when(jnp.logical_not(contrast_local(head)))
        def _(head=head):
            contrast_incoming(head).wait_recv()

    def projected(taken_side, store):
        taken = pl.ds(pl.multiple_of(taken_side * half, half), half)
        left = jnp.concatenate([contrasts[h, taken, :] for h in range(members)], axis=1)
        for start in range(0, model, chunk):
            span = slice(start, start + chunk)
            part = jnp.dot(left, contrast_w[:, span], preferred_element_type=f32)
            store(span, (part + pool_part[taken, span]).astype(bf16))

    def to_partner(span, part):
        out_stage[:, span] = part
        out_copy(span.start).start()

    def to_self(span, part):
        out_ref[:, span] = part

    projected(other, to_partner)
    projected(tp, to_self)
    for start in range(0, model, chunk):
        out_copy(start).wait()

    pair_first.wait_send()
    for ch in range(chunks):
        swap(ch).wait_send()
        pair_copy(1, ch).wait_send()

        @pl.when(crosses)
        def _(ch=ch):
            own_up(ch).wait_send()
            low_up(ch).wait_send()

        @pl.when(relays)
        def _(ch=ch):
            for step in range(2, 4):
                pair_copy(step, ch).wait_send()
                for slot in range(4):

                    @pl.when(jnp.logical_not(far_stays(slot // 2, slot % 2)))
                    def _(step=step, slot=slot):
                        far_copy(step, ch, slot // 2, slot % 2).wait_send()

                @pl.when(own_goal)
                def _(step=step):
                    far_pass(step, member, ch).wait_send()

        @pl.when(in_upper)
        def _(ch=ch):
            for step in range(2, 4):
                for source in range(members):

                    @pl.when(far_passes(source))
                    def _(step=step, source=source):
                        far_pass(step, source, ch).wait_send()

    def drain(step, ch):
        for j in range(2):

            @pl.when(jnp.logical_not(own_stays(step, j)))
            def _(j=j):
                kv_copy(step, j, ch).wait_send()

            @pl.when(jnp.logical_not(query_stays(step, j)))
            def _(j=j):
                query_copy(step, j, ch).wait_send()

        @pl.when(own_forwards(step))
        def _():
            forward_copy(step, member, ch).wait_send()

        for source in range(members):

            @pl.when(passes_on(step, source))
            def _(source=source):
                forward_copy(step, source, ch).wait_send()

    for ch in range(chunks):
        drain(0, ch)
        drain(1, ch)

    for i in range(members):

        @pl.when(jnp.logical_not(contrast_stays(i)))
        def _(i=i):
            contrast_copy(i).wait_send()

    @pl.when(sp + 1 < sp_count)
    def _():
        rim_copy.wait_send()


def kernel_scratch(members, half, model, width, pool_cols):
    bf16 = jnp.bfloat16
    rows = 2 * half
    dma = pltpu.SemaphoreType.DMA
    return [
        pltpu.VMEM((model, members * width), bf16),
        pltpu.VMEM((model, members * width), bf16),
        pltpu.VMEM((model, members * width), bf16),
        pltpu.VMEM((model, pool_cols), bf16),
        pltpu.VMEM((members * width, model), bf16),
        pltpu.VMEM((pool_cols, model), bf16),
        pltpu.VMEM((4, 2, half, model), bf16),
        pltpu.VMEM((4, members, 2, half, 2 * width), bf16),
        pltpu.VMEM((2, 2, 2, half, 2 * width), bf16),
        pltpu.VMEM((2, 4, 2, half, 2 * width), bf16),
        pltpu.VMEM((members, 2, half, width), bf16),
        pltpu.VMEM((2, 2, 2, half, width), bf16),
        pltpu.VMEM((2, members, rows, 128), jnp.float32),
        pltpu.VMEM((2, members, rows, 128), jnp.float32),
        pltpu.VMEM((2, members, rows, width), jnp.float32),
        pltpu.VMEM((members, rows, width), bf16),
        pltpu.VMEM((members, rows, width), bf16),
        pltpu.VMEM((reach_back + 1, pool_cols), bf16),
        pltpu.VMEM((reach_back + 1, pool_cols), bf16),
        pltpu.VMEM((rows, model), jnp.float32),
        pltpu.VMEM((half, model), bf16),
        dma((6,)),
        dma,
        dma((4, 2)),
        dma((4, 2)),
        dma((4, 2)),
        dma((4, 2)),
        dma((2, 2, 2)),
        dma((2, members, 2)),
        dma((2, members, 2)),
        dma((2, 4, 2)),
        dma((2, members, 2)),
        dma((2, members, 2)),
        dma((2, 2, 2)),
        dma((members, 2)),
        dma((members,)),
        dma((members,)),
        dma,
        dma,
        dma((model // math.gcd(model, 512),)),
        dma((model // math.gcd(model, 512),)),
    ]


vmem_most = 67043328


def scratch_bytes(scratch):
    return sum(
        math.prod(item.shape) * jnp.dtype(item.dtype).itemsize
        for item in scratch
        if getattr(item, "memory_space", None) == pltpu.VMEM
    )


def whole_layer(
    normed,
    query_weight,
    key_weight,
    value_weight,
    pool_in_weight,
    pool_weight,
    map_balance,
    head_gain,
    contrast_out_weight,
    pool_out_weight,
):
    sp_count = lax.axis_size("sp")
    width = head_gain.shape[0]
    members = query_weight.shape[1] // width
    half, model = normed.shape
    pool_cols = pool_in_weight.shape[1]
    groups_here = pool_weight.shape[0]
    scratch = kernel_scratch(max(members, 1), half, model, width, pool_cols)
    fits = (
        lax.axis_size("tp") == 2
        and members == 4
        and sp_count == 4 * members
        and groups_here % 4 == 0
        and scratch_bytes(scratch) < vmem_most * 3 // 4
    )
    if not fits:
        return per_device(
            normed,
            query_weight,
            key_weight,
            value_weight,
            pool_in_weight,
            pool_weight,
            map_balance,
            head_gain,
            contrast_out_weight,
            pool_out_weight,
        )
    vmem = pl.BlockSpec(memory_space=pltpu.VMEM)
    hbm = pl.BlockSpec(memory_space=pl.ANY)
    own_part, partner_part = pl.pallas_call(
        functools.partial(layer_kernel, sp_count, members),
        out_shape=[jax.ShapeDtypeStruct((half, model), jnp.bfloat16)] * 2,
        in_specs=[vmem, vmem, pl.BlockSpec(memory_space=pltpu.SMEM), vmem] + [hbm] * 6,
        out_specs=[vmem, vmem],
        scratch_shapes=scratch,
        compiler_params=pltpu.CompilerParams(
            collective_id=0, has_side_effects=True, vmem_limit_bytes=vmem_most
        ),
    )(
        normed,
        pool_weight,
        map_balance,
        head_gain.reshape(1, width),
        query_weight,
        key_weight,
        value_weight,
        pool_in_weight,
        contrast_out_weight,
        pool_out_weight,
    )
    return (own_part.astype(jnp.float32) + partner_part.astype(jnp.float32)).astype(jnp.bfloat16)


def solution(mesh):
    return jax.shard_map(
        whole_layer,
        mesh=mesh,
        in_specs=(
            P(("sp", "tp"), None),
            P(None, "tp"),
            P(None, "tp"),
            P(None, "tp"),
            P(None, "tp"),
            P("tp", None, None),
            P(),
            P(),
            P("tp", None),
            P("tp", None),
        ),
        out_specs=P(("sp", "tp"), None),
        check_vma=False,
    )
```

```python
import functools
import math

import jax
import jax.numpy as jnp
from jax import lax
from jax.experimental import pallas as pl
from jax.experimental.pallas import tpu as pltpu
from jax.sharding import PartitionSpec as P

reach_back = 15
norm_epsilon = 1e-06


def passed_along(block, axis, distance):
    devices = range(lax.axis_size(axis))
    route = [(i - distance, i) for i in devices if i - distance in devices]
    return lax.ppermute(block, axis, route)


def from_partner(block, axis, stride):
    count = lax.axis_size(axis)
    route = []
    for low in range(count):
        high = low | 1 << stride
        if high != low and high < count:
            route += [(low, high), (high, low)]
    return lax.ppermute(block, axis, route)


def shifted(array, axis, by):
    size = lax.axis_size(axis)
    return lax.ppermute(array, axis, [(i, (i + by) % size) for i in range(size)])


def as_sent(array):

    def short(part):
        return part.astype(jnp.bfloat16) if part.dtype == jnp.float32 else part

    return jax.tree.map(short, array)


def attend(running, queries, key_rows, value_rows, query_first, key_first, score_scale):
    key_count = key_rows.shape[0]
    key_block = math.gcd(key_count, 1024)
    unit_count = queries.shape[1]
    heads_here = value_rows.shape[1]
    per_head = unit_count // heads_here
    query_count = queries.shape[0]
    query_order = query_first + lax.iota(jnp.int32, query_count)

    def key_step(block_index, carried):
        block_start = block_index * key_block

        def block_work(current):
            row_peak, row_total, weighted = current
            scores = (
                jnp.einsum("qud,kud->uqk", queries, key_rows, preferred_element_type=jnp.float32)
                * score_scale
            )
            key_order = key_first + block_start + lax.iota(jnp.int32, key_block)
            scores = jnp.where(
                key_order[None, None, :] <= query_order[None, :, None], scores, -jnp.inf
            )
            new_peak = jnp.maximum(row_peak, jnp.max(scores, axis=2))
            shrink = jnp.exp(row_peak - new_peak)
            raised = jnp.exp(scores - new_peak[:, :, None])
            row_total = row_total * shrink + jnp.sum(raised, axis=2)
            map_weights = raised.astype(jnp.bfloat16).reshape(
                heads_here, per_head, query_count, key_block
            )
            update = jnp.einsum(
                "hmqk,khe->hmqe", map_weights, value_rows, preferred_element_type=jnp.float32
            )
            weighted = weighted * shrink[:, :, None] + update.reshape(unit_count, query_count, -1)
            return (new_peak, row_total, weighted)

        def keep_state(current):
            return current

        return lax.cond(
            key_first + block_start <= query_first + query_count - 1,
            block_work,
            keep_state,
            carried,
        )

    return lax.fori_loop(0, key_count // key_block, key_step, running)


def fresh_state(unit_count, row_count, value_width):
    return (
        jnp.full((unit_count, row_count), -1e30, jnp.float32),
        jnp.zeros((unit_count, row_count), jnp.float32),
        jnp.zeros((unit_count, row_count, value_width), jnp.float32),
    )


def finished(running):
    row_peak, row_total, weighted = running
    return (weighted / row_total[:, :, None]).astype(jnp.bfloat16)


def joined_state(first, second):
    first_peak, first_total, first_weighted = first
    second_peak, second_total, second_weighted = second
    new_peak = jnp.maximum(first_peak, second_peak)
    first_shrink = jnp.exp(first_peak - new_peak)
    second_shrink = jnp.exp(second_peak - new_peak)
    new_total = first_total * first_shrink + second_total * second_shrink
    new_weighted = (
        first_weighted * first_shrink[:, :, None] + second_weighted * second_shrink[:, :, None]
    )
    return (new_peak, new_total, new_weighted)


def per_device(
    normed,
    query_weight,
    key_weight,
    value_weight,
    pool_in_weight,
    pool_weight,
    map_balance,
    head_gain,
    contrast_out_weight,
    pool_out_weight,
):
    tp_index = lax.axis_index("tp")
    sp_count = lax.axis_size("sp")
    sp_index = lax.axis_index("sp")
    head_dim = head_gain.shape[0] // 2
    value_width = 2 * head_dim
    query_cols = query_weight.shape[1]
    value_cols = value_weight.shape[1]
    unit_count = query_cols // head_dim
    heads_here = unit_count // 2
    project_incoming = lax.all_gather(normed, "tp", axis=0, tiled=True)
    products = [
        jnp.dot(project_incoming, weight_part, preferred_element_type=jnp.float32)
        for weight_part in (query_weight, key_weight, value_weight, pool_in_weight)
    ]
    joined = jnp.concatenate(products, axis=1).astype(jnp.bfloat16)
    row_count = joined.shape[0]
    queries = joined[:, :query_cols].reshape(row_count, unit_count, head_dim)
    key_rows = joined[:, query_cols : 2 * query_cols].reshape(row_count, unit_count, head_dim)
    value_rows = joined[:, 2 * query_cols : 2 * query_cols + value_cols].reshape(
        row_count, heads_here, value_width
    )
    pool_input = joined[:, 2 * query_cols + value_cols :]
    pool_cols = pool_input.shape[1]
    upper_rim = passed_along(pool_input[row_count - reach_back :], "sp", 1)
    extended = jnp.concatenate([upper_rim, pool_input], axis=0).astype(jnp.float32)
    groups_here = pool_weight.shape[0]
    group_width = pool_weight.shape[1]
    group_index = tp_index * groups_here + lax.iota(jnp.int32, pool_cols) // group_width
    widths = jnp.left_shift(jnp.int32(2), group_index % 4)
    window_sum = jnp.zeros((row_count, pool_cols), jnp.float32)
    for offset in range(reach_back + 1):
        window_sum = window_sum + extended[
            reach_back - offset : reach_back - offset + row_count
        ] * (offset < widths)[None, :].astype(jnp.float32)
    position = sp_index * row_count + lax.iota(jnp.int32, row_count)
    counts = jnp.minimum(position[:, None] + 1, widths[None, :]).astype(jnp.float32)
    spread = (window_sum / counts - extended[reach_back:]).astype(jnp.bfloat16)
    mixed_groups = jnp.einsum(
        "tgc,gce->tge",
        spread.reshape(row_count, groups_here, group_width),
        pool_weight,
        preferred_element_type=jnp.float32,
    )
    pool_out = mixed_groups.reshape(row_count, pool_cols).astype(jnp.bfloat16)
    score_scale = head_dim ** (-0.5)
    level_count = sp_count.bit_length() - 1
    low_levels = level_count // 2
    band_size = 1 << low_levels
    band_count = sp_count // band_size
    member = sp_index % band_size
    band = sp_index // band_size
    band_queries = queries
    for bit in range(low_levels):
        received = from_partner(band_queries, "sp", bit)
        upper = member >> bit & 1 == 1
        band_queries = jnp.where(
            upper,
            jnp.concatenate([received, band_queries], axis=0),
            jnp.concatenate([band_queries, received], axis=0),
        )
    band_first = band * band_size * row_count
    running = fresh_state(unit_count, band_size * row_count, value_width)
    for step in range(band_count):
        if step == 0:
            key_piece, value_piece = (key_rows, value_rows)
        else:
            key_piece, value_piece = shifted((key_rows, value_rows), "sp", step * band_size)
        source = (sp_index - step * band_size) % sp_count
        running = attend(
            running,
            band_queries,
            key_piece,
            value_piece,
            band_first,
            source * row_count,
            score_scale,
        )
    for bit in range(low_levels - 1, -1, -1):
        half = running[0].shape[1] // 2
        upper = member >> bit & 1 == 1
        lower_part = jax.tree.map(lambda item: item[:, :half], running)
        upper_part = jax.tree.map(lambda item: item[:, half:], running)
        outgoing = jax.tree.map(
            lambda low, high: jnp.where(upper, low, high), lower_part, upper_part
        )
        kept = jax.tree.map(lambda low, high: jnp.where(upper, high, low), lower_part, upper_part)
        incoming = from_partner(
            (as_sent(outgoing[0]), as_sent(outgoing[1]), as_sent(outgoing[2])), "sp", bit
        )
        running = joined_state(kept, incoming)
    maps = finished(running)
    paired = maps.reshape(heads_here, 2, row_count, value_width)
    paired = lax.optimization_barrier(paired).astype(jnp.float32)
    head_first = tp_index * heads_here
    balance_here = lax.dynamic_slice_in_dim(map_balance, head_first, heads_here, 0)
    contrast = paired[:, 0] - balance_here[:, None, None] * paired[:, 1]
    mean_square = jnp.mean(contrast * contrast, axis=2, keepdims=True)
    contrast = contrast * lax.rsqrt(mean_square + norm_epsilon) * head_gain
    contrast_out = (
        contrast.astype(jnp.bfloat16)
        .transpose(1, 0, 2)
        .reshape(row_count, heads_here * value_width)
    )
    partial_value = jnp.dot(contrast_out, contrast_out_weight, preferred_element_type=jnp.float32)
    return lax.psum_scatter(
        (
            partial_value + jnp.dot(pool_out, pool_out_weight, preferred_element_type=jnp.float32)
        ).astype(jnp.bfloat16),
        "tp",
        scatter_dimension=0,
        tiled=True,
    )


MESH = pl.DeviceIdType.MESH


def layer_kernel(
    sp_count,
    members,
    x_hbm,
    pool_weight_hbm,
    balance_hbm,
    gain_hbm,
    query_hbm,
    key_hbm,
    value_hbm,
    pool_in_hbm,
    contrast_hbm,
    pool_out_hbm,
    out_ref,
    out_recv,
    pool_weight,
    balance,
    gain,
    query_w,
    key_w,
    value_w,
    pool_in_w,
    contrast_w,
    pool_out_w,
    rows_in,
    kv,
    kv_stage,
    far_stage,
    queries,
    query_stage,
    peaks,
    totals,
    weighted,
    contrasts,
    contrast_stage,
    rim,
    rim_stage,
    pool_part,
    out_stage,
    weight_sem,
    local_sem,
    pair_send,
    pair_recv,
    relay_send,
    relay_recv,
    kv_send,
    kv_recv,
    forward_send,
    far_send,
    far_recv,
    far_forward,
    query_send,
    query_recv,
    contrast_send,
    contrast_recv,
    rim_send,
    rim_recv,
    out_send,
    out_recv_sem,
):
    f32 = jnp.float32
    bf16 = jnp.bfloat16
    sp = lax.axis_index("sp")
    tp = lax.axis_index("tp")
    other = 1 - tp
    plane = lax.div(sp, members)
    member = lax.rem(sp, members)
    upper = lax.div(plane, 2)
    side = lax.rem(plane, 2)
    across = lax.div(member, 2)
    along = lax.rem(member, 2)
    half_count = 2 * members
    half, model = x_hbm.shape
    rows = 2 * half
    width = gain.shape[1]
    head_dim = width // 2
    chunk = math.gcd(model, 512)
    chunks = 2
    piece = half // chunks
    in_lower = upper == 0
    in_upper = upper == 1
    crosses = plane == 1
    relays = plane == 2
    query_band = 2 * upper + tp
    bands_of = (plane, plane + 1 - 2 * side)

    keep = pltpu.make_async_copy(x_hbm, rows_in.at[0, tp], local_sem)
    keep.start()
    x_ref = rows_in.at[0, tp]

    loads = [
        pltpu.make_async_copy(src, dst, weight_sem.at[i])
        for i, (src, dst) in enumerate(
            (
                (query_hbm, query_w),
                (key_hbm, key_w),
                (value_hbm, value_w),
                (pool_in_hbm, pool_in_w),
                (pool_out_hbm, pool_out_w),
                (contrast_hbm, contrast_w),
                (pool_weight_hbm, pool_weight),
                (balance_hbm, balance),
                (gain_hbm, gain),
            )
        )
    ]

    barrier = pltpu.get_barrier_semaphore()

    def greet(target):
        pl.semaphore_signal(barrier, inc=1, device_id=target, device_id_type=MESH)

    place = (side * members + member) * 2 + tp
    for d in range(1, 2 * half_count):
        goal = lax.rem(place + d, 2 * half_count)
        greet((upper * half_count + lax.div(goal, 2), lax.rem(goal, 2)))

    @pl.when(crosses)
    def _():
        greet((sp + members, tp))

    @pl.when(relays)
    def _():
        greet((sp - members, tp))

    @pl.when(sp == half_count - 1)
    def _():
        greet((sp + 1, tp))

    @pl.when(sp == half_count)
    def _():
        greet((sp - 1, tp))

    for load in loads:
        load.start()

    extra = jnp.where(jnp.logical_or(crosses, relays), 1, 0)
    extra = extra + jnp.where(jnp.logical_or(sp == half_count - 1, sp == half_count), 1, 0)
    pl.semaphore_wait(barrier, 2 * half_count - 1 + extra)

    def cut(ch):
        return pl.ds(ch * piece, piece)

    pair_first = pltpu.make_async_remote_copy(
        src_ref=x_ref,
        dst_ref=rows_in.at[0, tp],
        send_sem=pair_send.at[0, 0],
        recv_sem=pair_recv.at[0, 0],
        device_id=(sp, other),
        device_id_type=MESH,
    )

    def pair_copy(step, ch):
        return pltpu.make_async_remote_copy(
            src_ref=rows_in.at[step, tp, cut(ch)],
            dst_ref=rows_in.at[step, tp, cut(ch)],
            send_sem=pair_send.at[step, ch],
            recv_sem=pair_recv.at[step, ch],
            device_id=(sp, other),
            device_id_type=MESH,
        )

    def relay_copy(src, step, ch, target):
        return pltpu.make_async_remote_copy(
            src_ref=src.at[cut(ch)],
            dst_ref=rows_in.at[step, tp, cut(ch)],
            send_sem=relay_send.at[step, ch],
            recv_sem=relay_recv.at[step, ch],
            device_id=(target, tp),
            device_id_type=MESH,
        )

    def swap(ch):
        return relay_copy(x_ref, 1, ch, sp + members * (1 - 2 * side))

    def own_up(ch):
        return relay_copy(x_ref, 2, ch, sp + members)

    def low_up(ch):
        return relay_copy(rows_in.at[1, tp], 3, ch, sp + members)

    def top(step):
        return side == (1 if step == 0 else 0)

    def kv_copy(step, j, ch):
        goal = 2 * tp + j
        first = jnp.where(top(step), 1, along)
        return pltpu.make_async_remote_copy(
            src_ref=kv_stage.at[step, j, :, cut(ch)],
            dst_ref=kv.at[step, member, :, cut(ch)],
            send_sem=kv_send.at[step, j, ch],
            recv_sem=kv_recv.at[step, member, ch],
            device_id=(plane * members + goal, first),
            device_id_type=MESH,
        )

    def forward_copy(step, source, ch):
        return pltpu.make_async_remote_copy(
            src_ref=kv.at[step, source, :, cut(ch)],
            dst_ref=kv.at[step, source, :, cut(ch)],
            send_sem=forward_send.at[step, source, ch],
            recv_sem=kv_recv.at[step, source, ch],
            device_id=(sp, other),
            device_id_type=MESH,
        )

    def query_copy(step, j, ch):
        core = jnp.where(top(step), 1, 0)
        return pltpu.make_async_remote_copy(
            src_ref=query_stage.at[step, j, :, cut(ch)],
            dst_ref=queries.at[member, :, cut(ch)],
            send_sem=query_send.at[step, j, ch],
            recv_sem=query_recv.at[member, ch],
            device_id=(plane * members + 2 * tp + j, core),
            device_id_type=MESH,
        )

    own_goal = across == tp

    def far_copy(step, ch, goal_side, j):
        slot = goal_side * 2 + j
        goal = (2 * upper + goal_side) * members + 2 * tp + j
        return pltpu.make_async_remote_copy(
            src_ref=far_stage.at[step - 2, slot, ch],
            dst_ref=kv.at[step, member, ch],
            send_sem=far_send.at[step - 2, slot, ch],
            recv_sem=far_recv.at[step - 2, member, ch],
            device_id=(goal, along),
            device_id_type=MESH,
        )

    def far_pass(step, source, ch):
        return pltpu.make_async_remote_copy(
            src_ref=kv.at[step, source, ch],
            dst_ref=kv.at[step, source, ch],
            send_sem=far_forward.at[step - 2, source, ch],
            recv_sem=far_recv.at[step - 2, source, ch],
            device_id=(sp, other),
            device_id_type=MESH,
        )

    def far_stays(goal_side, j):
        return jnp.logical_and(goal_side == side, jnp.logical_and(own_goal, j == along))

    def far_here(source):
        return jnp.logical_and(relays, source == member)

    def far_passes(source):
        return jnp.logical_and(source % 2 == tp, jnp.logical_not(far_here(source)))

    def far_awaits(source):
        return jnp.logical_not(jnp.logical_and(far_here(source), own_goal))

    def own_stays(step, j):
        return jnp.logical_and(own_goal, j == along)

    def query_stays(step, j):
        return jnp.logical_and(own_stays(step, j), jnp.where(top(step), 1, 0) == tp)

    def own_forwards(step):
        return jnp.logical_and(
            own_goal, jnp.logical_or(jnp.logical_not(top(step)), tp == 0)
        )

    def passes_on(step, source):
        mine = jnp.logical_and(source % 2 == tp, jnp.logical_not(top(step)))
        return jnp.logical_and(source != member, mine)

    def awaits(step, source):
        needed = jnp.logical_or(tp == 1, jnp.logical_not(top(step)))
        made_here = jnp.logical_and(source == member, own_goal)
        return jnp.logical_and(needed, jnp.logical_not(made_here))

    def contrast_stays(i):
        return jnp.logical_and(
            jnp.logical_and(query_band == plane, i == member), across == tp
        )

    head_here = 2 * side + along

    def contrast_copy(i):
        return pltpu.make_async_remote_copy(
            src_ref=contrast_stage.at[i],
            dst_ref=contrasts.at[head_here],
            send_sem=contrast_send.at[i],
            recv_sem=contrast_recv.at[head_here],
            device_id=(query_band * members + i, across),
            device_id_type=MESH,
        )

    def contrast_incoming(head):
        return pltpu.make_async_remote_copy(
            src_ref=contrast_stage.at[0],
            dst_ref=contrasts.at[head],
            send_sem=contrast_send.at[0],
            recv_sem=contrast_recv.at[head],
            device_id=(sp, other),
            device_id_type=MESH,
        )

    def contrast_local(head):
        same = jnp.logical_and(head // 2 == side, 2 * tp + head % 2 == member)
        return jnp.logical_and(same, side == tp)

    rim_copy = pltpu.make_async_remote_copy(
        src_ref=rim_stage,
        dst_ref=rim,
        send_sem=rim_send,
        recv_sem=rim_recv,
        device_id=(lax.rem(sp + 1, sp_count), tp),
        device_id_type=MESH,
    )

    def out_copy(start):
        span = slice(start, start + chunk)
        return pltpu.make_async_remote_copy(
            src_ref=out_stage.at[:, span],
            dst_ref=out_recv.at[:, span],
            send_sem=out_send.at[start // chunk],
            recv_sem=out_recv_sem.at[start // chunk],
            device_id=(sp, other),
            device_id_type=MESH,
        )


    keep.wait()
    pair_first.start()
    for ch in range(chunks):
        swap(ch).start()

        @pl.when(crosses)
        def _(ch=ch):
            own_up(ch).start()

    peaks[...] = jnp.full(peaks.shape, -1e30, f32)
    totals[...] = jnp.zeros(totals.shape, f32)
    weighted[...] = jnp.zeros(weighted.shape, f32)

    def project(step, pieces):
        here = cut(pieces[0]) if len(pieces) == 1 else slice(None)

        def one(t, carry):
            j = jnp.where(t == 0, 1 - along, along)
            columns = pl.ds(pl.multiple_of((2 * side + j) * width, width), width)
            x = rows_in[step, :, here, :].reshape(-1, model)

            def through(held):
                dot = jnp.dot(x, held[:, columns], preferred_element_type=f32)
                return dot.astype(bf16).reshape(2, -1, width)

            mine = through(query_w)
            keys = through(key_w)
            values = through(value_w)
            kept = query_stays(step, j)
            stays = own_stays(step, j)

            @pl.when(jnp.logical_not(kept))
            def _():
                query_stage[step, j, :, here] = mine
                for ch in pieces:
                    query_copy(step, j, ch).start()

            @pl.when(kept)
            def _():
                queries[member, :, here] = mine

            @pl.when(jnp.logical_not(stays))
            def _():
                kv_stage[step, j, :, here, :width] = keys
                kv_stage[step, j, :, here, width:] = values
                for ch in pieces:
                    kv_copy(step, j, ch).start()

            @pl.when(stays)
            def _():
                kv[step, member, :, here, :width] = keys
                kv[step, member, :, here, width:] = values

                @pl.when(own_forwards(step))
                def _():
                    for ch in pieces:
                        forward_copy(step, member, ch).start()

            return carry

        lax.fori_loop(0, 2, one, 0)

    def project_far(step, ch):
        pair_copy(step, ch).wait_recv()

        def one(t, carry):
            goal_side = 1 - lax.div(t, 2)
            j = jnp.where(lax.rem(t, 2) == 0, 1 - along, along)
            columns = pl.ds(pl.multiple_of((2 * goal_side + j) * width, width), width)
            x = rows_in[step, :, cut(ch), :].reshape(half, model)
            keys = jnp.dot(x, key_w[:, columns], preferred_element_type=f32).astype(bf16)
            values = jnp.dot(x, value_w[:, columns], preferred_element_type=f32).astype(bf16)
            stays = far_stays(goal_side, j)

            @pl.when(jnp.logical_not(stays))
            def _():
                far_stage[step - 2, goal_side * 2 + j, ch, :, :width] = keys
                far_stage[step - 2, goal_side * 2 + j, ch, :, width:] = values
                far_copy(step, ch, goal_side, j).start()

            @pl.when(stays)
            def _():
                kv[step, member, ch, :, :width] = keys
                kv[step, member, ch, :, width:] = values
                far_pass(step, member, ch).start()

            return carry

        lax.fori_loop(0, 4, one, 0)

    def take_swap(ch):
        swap(ch).wait_recv()

        @pl.when(crosses)
        def _():
            low_up(ch).start()

        pair_copy(1, ch).start()

    def take_far(step, ch):
        (own_up(ch) if step == 2 else low_up(ch)).wait_recv()
        pair_copy(step, ch).start()

    def project_swap(ch):
        pair_copy(1, ch).wait_recv()
        project(1, (ch,))

    log_scale = head_dim ** (-0.5) * math.log2(math.e)

    def attend_block(step, i, seen, masked):
        for u in range(2):
            cols = slice(u * head_dim, (u + 1) * head_dim)
            keys = kv[step, :seen, :, :, cols].reshape(-1, head_dim)
            values = kv[step, :seen, :, :, width:].reshape(-1, width)
            scores = lax.dot_general(
                queries[i, :, :, cols].reshape(rows, head_dim), keys, (((1,), (1,)), ((), ())), preferred_element_type=f32
            )
            if masked:
                query_order = lax.broadcasted_iota(jnp.int32, scores.shape, 0) + (seen - 1) * rows
                key_order = lax.broadcasted_iota(jnp.int32, scores.shape, 1)
                scores = jnp.where(key_order <= query_order, scores, -jnp.inf)
            old = peaks[u, i][:, :1]
            peak = jnp.maximum(jnp.max(scores, axis=1, keepdims=True), old)
            shrink = jnp.exp2((old - peak) * log_scale)
            raised = jnp.exp2((scores - peak) * log_scale)
            total = jnp.sum(raised, axis=1, keepdims=True)
            update = jnp.dot(raised.astype(bf16), values, preferred_element_type=f32)
            total = total + totals[u, i][:, :1] * shrink
            update = update + weighted[u, i] * shrink
            peaks[u, i] = jnp.broadcast_to(peak, peaks.shape[2:])
            totals[u, i] = jnp.broadcast_to(total, totals.shape[2:])
            weighted[u, i] = update

    def finished_block(i):
        first = (weighted[0, i] * (1.0 / totals[0, i][:, :1])).astype(bf16).astype(f32)
        second = (weighted[1, i] * (1.0 / totals[1, i][:, :1])).astype(bf16).astype(f32)
        contrast = first - balance[across * members + head_here] * second
        mean_square = jnp.mean(contrast * contrast, axis=1, keepdims=True)
        return (contrast * lax.rsqrt(mean_square + norm_epsilon) * gain[...]).astype(bf16)

    def send_block(i, result):
        stays = contrast_stays(i)

        @pl.when(jnp.logical_not(stays))
        def _():
            contrast_stage[i] = result
            contrast_copy(i).start()

        @pl.when(stays)
        def _():
            contrasts[head_here] = result

    def turn(t):
        return lax.rem(member + 1 + t, members)

    def block_pairs(work):
        def one(t, carry):
            work(turn(2 * t), turn(2 * t + 1))
            return carry

        lax.fori_loop(0, members // 2, one, 0)

    def finish_pair(i, k):
        results = finished_block(i), finished_block(k)
        send_block(i, results[0])
        send_block(k, results[1])

    def lands_here(step, source):
        return jnp.logical_and(
            source != member, jnp.where(top(step), 1, source % 2) == tp
        )

    def pass_on(step):
        for ch in range(chunks):
            for source in range(members):

                @pl.when(lands_here(step, source))
                def _(source=source, ch=ch):
                    forward_copy(step, source, ch).wait_recv()

                @pl.when(passes_on(step, source))
                def _(source=source, ch=ch):
                    forward_copy(step, source, ch).start()

    def arrive(step):
        for ch in range(chunks):
            for source in range(members):
                passed = jnp.logical_not(lands_here(step, source))

                @pl.when(jnp.logical_and(awaits(step, source), passed))
                def _(source=source, ch=ch):
                    forward_copy(step, source, ch).wait_recv()

    def attend(step, between):
        band = bands_of[step]

        @pl.when(band == query_band)
        def _():
            for i in range(members):
                if i == members // 2:
                    between()
                attend_block(step, i, i + 1, True)

        @pl.when(band < query_band)
        def _():
            def one(t, carry):
                attend_block(step, turn(2 * t), members, False)
                attend_block(step, turn(2 * t + 1), members, False)

                @pl.when(t == 0)
                def _():
                    between()

                return carry

            lax.fori_loop(0, members // 2, one, 0)

        @pl.when(band > query_band)
        def _():
            between()

    def far_pass_on(step, ch):
        for source in range(members):

            @pl.when(far_passes(source))
            def _(source=source):
                far_pass(step, source, ch).wait_recv()
                far_pass(step, source, ch).start()

    def far_arrive(step, ch):
        for source in range(members):
            passed = jnp.logical_not(far_passes(source))

            @pl.when(jnp.logical_and(far_awaits(source), passed))
            def _(source=source):
                far_pass(step, source, ch).wait_recv()

    loads[0].wait()
    loads[1].wait()
    loads[2].wait()
    pair_first.wait_recv()
    project(0, tuple(range(chunks)))

    loads[3].wait()
    pool_input = jnp.dot(
        rows_in[0].reshape(rows, model), pool_in_w[...], preferred_element_type=f32
    ).astype(bf16)
    rim_stage[...] = pool_input[rows - rim.shape[0] :]

    @pl.when(sp + 1 < sp_count)
    def _():
        rim_copy.start()

    take_swap(0)

    @pl.when(relays)
    def _():
        take_far(2, 0)

    project_swap(0)

    @pl.when(relays)
    def _():
        project_far(2, 0)

    take_swap(1)

    @pl.when(relays)
    def _():
        take_far(2, 1)

    project_swap(1)

    @pl.when(relays)
    def _():
        project_far(2, 1)
        take_far(3, 0)

    pass_on(0)

    @pl.when(relays)
    def _():
        project_far(3, 0)

    def query_incoming(source, ch):
        return pltpu.make_async_remote_copy(
            src_ref=query_stage.at[0, 0, :, cut(ch)],
            dst_ref=queries.at[source, :, cut(ch)],
            send_sem=query_send.at[0, 0, ch],
            recv_sem=query_recv.at[source, ch],
            device_id=(sp, other),
            device_id_type=MESH,
        )

    def take_queries():
        for source in range(members):

            @pl.when(jnp.logical_not(jnp.logical_and(source == member, own_goal)))
            def _(source=source):
                for ch in range(chunks):
                    query_incoming(source, ch).wait_recv()

    idle_first = jnp.logical_and(in_upper, jnp.logical_and(side == 1, tp == 0))

    @pl.when(idle_first)
    def _():
        far_pass_on(2, 0)
        far_pass_on(2, 1)

    take_queries()
    arrive(0)

    def last_rows():
        @pl.when(relays)
        def _():
            take_far(3, 1)

    attend(0, last_rows)

    @pl.when(relays)
    def _():
        project_far(3, 1)

    def last_passes():
        @pl.when(jnp.logical_and(in_upper, side == 1))
        def _():
            far_pass_on(3, 1)

    def attend_swapped():
        pass_on(1)

        @pl.when(jnp.logical_and(in_upper, side == 1))
        def _():
            far_pass_on(3, 0)

        arrive(1)
        attend(1, last_passes)

    @pl.when(in_upper)
    def _():
        @pl.when(jnp.logical_not(idle_first))
        def _():
            far_pass_on(2, 0)
            far_pass_on(2, 1)

        @pl.when(relays)
        def _():
            attend_swapped()
            far_pass_on(3, 0)

        far_arrive(2, 0)
        far_arrive(2, 1)

        def one(t, carry):
            attend_block(2, turn(2 * t), members, False)
            attend_block(2, turn(2 * t + 1), members, False)

            @pl.when(jnp.logical_and(t == 0, jnp.logical_and(relays, tp == 1)))
            def _():
                far_pass_on(3, 1)

            return carry

        lax.fori_loop(0, members // 2, one, 0)

    @pl.when(jnp.logical_not(relays))
    def _():
        attend_swapped()

    for load in loads[6:]:
        load.wait()

    @pl.when(in_lower)
    def _():
        block_pairs(finish_pair)

    @pl.when(in_upper)
    def _():
        @pl.when(jnp.logical_and(relays, tp == 0))
        def _():
            far_pass_on(3, 1)

        far_arrive(3, 0)
        far_arrive(3, 1)

        def last_pair(i, k):
            attend_block(3, i, members, False)
            attend_block(3, k, members, False)
            finish_pair(i, k)

        block_pairs(last_pair)

    @pl.when(sp > 0)
    def _():
        rim_copy.wait_recv()

    @pl.when(sp == 0)
    def _():
        rim[...] = jnp.zeros_like(rim)

    loads[4].wait()
    extended = jnp.concatenate([rim[...], pool_input], axis=0).astype(f32)
    group_width = pool_weight.shape[1]
    skirt = rim.shape[0]
    position = sp * rows + lax.broadcasted_iota(jnp.int32, (rows, group_width), 0)
    mixed = []
    for group in range(pool_weight.shape[0]):
        block = extended[:, group * group_width : (group + 1) * group_width]
        window = block
        reach = 1
        span = 2 ** (1 + group % 4)
        while reach < span:
            window = window + pltpu.roll(window, reach, 0)
            reach *= 2
        counts = jnp.minimum(position + 1, span).astype(f32)
        spread = (window[skirt:] / counts - block[skirt:]).astype(bf16)
        mixed.append(
            jnp.dot(spread, pool_weight[group], preferred_element_type=f32).astype(bf16)
        )
    pool_out = jnp.concatenate(mixed, axis=1)
    for start in range(0, model, chunk):
        pool_part[:, start : start + chunk] = jnp.dot(
            pool_out, pool_out_w[:, start : start + chunk], preferred_element_type=f32
        )

    loads[5].wait()
    for head in range(members):

        @pl.when(jnp.logical_not(contrast_local(head)))
        def _(head=head):
            contrast_incoming(head).wait_recv()

    def projected(taken_side, store):
        taken = pl.ds(pl.multiple_of(taken_side * half, half), half)
        left = jnp.concatenate([contrasts[h, taken, :] for h in range(members)], axis=1)
        for start in range(0, model, chunk):
            span = slice(start, start + chunk)
            part = jnp.dot(left, contrast_w[:, span], preferred_element_type=f32)
            store(span, (part + pool_part[taken, span]).astype(bf16))

    def to_partner(span, part):
        out_stage[:, span] = part
        out_copy(span.start).start()

    def to_self(span, part):
        out_ref[:, span] = part

    projected(other, to_partner)
    projected(tp, to_self)
    for start in range(0, model, chunk):
        out_copy(start).wait()

    pair_first.wait_send()
    for ch in range(chunks):
        swap(ch).wait_send()
        pair_copy(1, ch).wait_send()

        @pl.when(crosses)
        def _(ch=ch):
            own_up(ch).wait_send()
            low_up(ch).wait_send()

        @pl.when(relays)
        def _(ch=ch):
            for step in range(2, 4):
                pair_copy(step, ch).wait_send()
                for slot in range(4):

                    @pl.when(jnp.logical_not(far_stays(slot // 2, slot % 2)))
                    def _(step=step, slot=slot):
                        far_copy(step, ch, slot // 2, slot % 2).wait_send()

                @pl.when(own_goal)
                def _(step=step):
                    far_pass(step, member, ch).wait_send()

        @pl.when(in_upper)
        def _(ch=ch):
            for step in range(2, 4):
                for source in range(members):

                    @pl.when(far_passes(source))
                    def _(step=step, source=source):
                        far_pass(step, source, ch).wait_send()

    def drain(step, ch):
        for j in range(2):

            @pl.when(jnp.logical_not(own_stays(step, j)))
            def _(j=j):
                kv_copy(step, j, ch).wait_send()

            @pl.when(jnp.logical_not(query_stays(step, j)))
            def _(j=j):
                query_copy(step, j, ch).wait_send()

        @pl.when(own_forwards(step))
        def _():
            forward_copy(step, member, ch).wait_send()

        for source in range(members):

            @pl.when(passes_on(step, source))
            def _(source=source):
                forward_copy(step, source, ch).wait_send()

    for ch in range(chunks):
        drain(0, ch)
        drain(1, ch)

    for i in range(members):

        @pl.when(jnp.logical_not(contrast_stays(i)))
        def _(i=i):
            contrast_copy(i).wait_send()

    @pl.when(sp + 1 < sp_count)
    def _():
        rim_copy.wait_send()


def kernel_scratch(members, half, model, width, pool_cols, heads, groups_here):
    bf16 = jnp.bfloat16
    rows = 2 * half
    group_width = pool_cols // groups_here
    dma = pltpu.SemaphoreType.DMA
    return [
        pltpu.VMEM((groups_here, group_width, group_width), bf16),
        pltpu.SMEM((heads,), jnp.float32),
        pltpu.VMEM((1, width), jnp.float32),
        pltpu.VMEM((model, members * width), bf16),
        pltpu.VMEM((model, members * width), bf16),
        pltpu.VMEM((model, members * width), bf16),
        pltpu.VMEM((model, pool_cols), bf16),
        pltpu.VMEM((members * width, model), bf16),
        pltpu.VMEM((pool_cols, model), bf16),
        pltpu.VMEM((4, 2, half, model), bf16),
        pltpu.VMEM((4, members, 2, half, 2 * width), bf16),
        pltpu.VMEM((2, 2, 2, half, 2 * width), bf16),
        pltpu.VMEM((2, 4, 2, half, 2 * width), bf16),
        pltpu.VMEM((members, 2, half, width), bf16),
        pltpu.VMEM((2, 2, 2, half, width), bf16),
        pltpu.VMEM((2, members, rows, 128), jnp.float32),
        pltpu.VMEM((2, members, rows, 128), jnp.float32),
        pltpu.VMEM((2, members, rows, width), jnp.float32),
        pltpu.VMEM((members, rows, width), bf16),
        pltpu.VMEM((members, rows, width), bf16),
        pltpu.VMEM((reach_back + 1, pool_cols), bf16),
        pltpu.VMEM((reach_back + 1, pool_cols), bf16),
        pltpu.VMEM((rows, model), jnp.float32),
        pltpu.VMEM((half, model), bf16),
        dma((9,)),
        dma,
        dma((4, 2)),
        dma((4, 2)),
        dma((4, 2)),
        dma((4, 2)),
        dma((2, 2, 2)),
        dma((2, members, 2)),
        dma((2, members, 2)),
        dma((2, 4, 2)),
        dma((2, members, 2)),
        dma((2, members, 2)),
        dma((2, 2, 2)),
        dma((members, 2)),
        dma((members,)),
        dma((members,)),
        dma,
        dma,
        dma((model // math.gcd(model, 512),)),
        dma((model // math.gcd(model, 512),)),
    ]


vmem_most = 67043328
kernel_grant = 54 * 2**20


def scratch_bytes(scratch):
    return sum(
        math.prod(item.shape) * jnp.dtype(item.dtype).itemsize
        for item in scratch
        if getattr(item, "memory_space", None) == pltpu.VMEM
    )


def whole_layer(
    normed,
    query_weight,
    key_weight,
    value_weight,
    pool_in_weight,
    pool_weight,
    map_balance,
    head_gain,
    contrast_out_weight,
    pool_out_weight,
):
    sp_count = lax.axis_size("sp")
    width = head_gain.shape[0]
    members = query_weight.shape[1] // width
    half, model = normed.shape
    pool_cols = pool_in_weight.shape[1]
    groups_here = pool_weight.shape[0]
    heads = map_balance.shape[0]
    scratch = kernel_scratch(
        max(members, 1), half, model, width, pool_cols, heads, groups_here
    )
    fits = (
        lax.axis_size("tp") == 2
        and members == 4
        and sp_count == 4 * members
        and groups_here % 4 == 0
        and scratch_bytes(scratch) < vmem_most * 3 // 4
    )
    if not fits:
        return per_device(
            normed,
            query_weight,
            key_weight,
            value_weight,
            pool_in_weight,
            pool_weight,
            map_balance,
            head_gain,
            contrast_out_weight,
            pool_out_weight,
        )
    vmem = pl.BlockSpec(memory_space=pltpu.VMEM)
    hbm = pl.BlockSpec(memory_space=pltpu.HBM)
    own_part, partner_part = pl.pallas_call(
        functools.partial(layer_kernel, sp_count, members),
        out_shape=[pltpu.VMEM((half, model), jnp.bfloat16)] * 2,
        in_specs=[hbm] * 10,
        out_specs=[vmem, vmem],
        scratch_shapes=scratch,
        compiler_params=pltpu.CompilerParams(
            collective_id=0, has_side_effects=True, vmem_limit_bytes=kernel_grant
        ),
    )(
        normed,
        pool_weight,
        map_balance,
        head_gain.reshape(1, width),
        query_weight,
        key_weight,
        value_weight,
        pool_in_weight,
        contrast_out_weight,
        pool_out_weight,
    )
    return (own_part.astype(jnp.float32) + partner_part.astype(jnp.float32)).astype(jnp.bfloat16)


def solution(mesh):
    return jax.shard_map(
        whole_layer,
        mesh=mesh,
        in_specs=(
            P(("sp", "tp"), None),
            P(None, "tp"),
            P(None, "tp"),
            P(None, "tp"),
            P(None, "tp"),
            P("tp", None, None),
            P(),
            P(),
            P("tp", None),
            P("tp", None),
        ),
        out_specs=P(("sp", "tp"), None),
        check_vma=False,
    )
```

```python
import functools
import math

import jax
import jax.numpy as jnp
from jax import lax
from jax.experimental import pallas as pl
from jax.experimental.pallas import tpu as pltpu
from jax.sharding import PartitionSpec as P

reach_back = 15
norm_epsilon = 1e-06


def passed_along(block, axis, distance):
    devices = range(lax.axis_size(axis))
    route = [(i - distance, i) for i in devices if i - distance in devices]
    return lax.ppermute(block, axis, route)


def from_partner(block, axis, stride):
    count = lax.axis_size(axis)
    route = []
    for low in range(count):
        high = low | 1 << stride
        if high != low and high < count:
            route += [(low, high), (high, low)]
    return lax.ppermute(block, axis, route)


def shifted(array, axis, by):
    size = lax.axis_size(axis)
    return lax.ppermute(array, axis, [(i, (i + by) % size) for i in range(size)])


def as_sent(array):

    def short(part):
        return part.astype(jnp.bfloat16) if part.dtype == jnp.float32 else part

    return jax.tree.map(short, array)


def attend(running, queries, key_rows, value_rows, query_first, key_first, score_scale):
    key_count = key_rows.shape[0]
    key_block = math.gcd(key_count, 1024)
    unit_count = queries.shape[1]
    heads_here = value_rows.shape[1]
    per_head = unit_count // heads_here
    query_count = queries.shape[0]
    query_order = query_first + lax.iota(jnp.int32, query_count)

    def key_step(block_index, carried):
        block_start = block_index * key_block

        def block_work(current):
            row_peak, row_total, weighted = current
            scores = (
                jnp.einsum("qud,kud->uqk", queries, key_rows, preferred_element_type=jnp.float32)
                * score_scale
            )
            key_order = key_first + block_start + lax.iota(jnp.int32, key_block)
            scores = jnp.where(
                key_order[None, None, :] <= query_order[None, :, None], scores, -jnp.inf
            )
            new_peak = jnp.maximum(row_peak, jnp.max(scores, axis=2))
            shrink = jnp.exp(row_peak - new_peak)
            raised = jnp.exp(scores - new_peak[:, :, None])
            row_total = row_total * shrink + jnp.sum(raised, axis=2)
            map_weights = raised.astype(jnp.bfloat16).reshape(
                heads_here, per_head, query_count, key_block
            )
            update = jnp.einsum(
                "hmqk,khe->hmqe", map_weights, value_rows, preferred_element_type=jnp.float32
            )
            weighted = weighted * shrink[:, :, None] + update.reshape(unit_count, query_count, -1)
            return (new_peak, row_total, weighted)

        def keep_state(current):
            return current

        return lax.cond(
            key_first + block_start <= query_first + query_count - 1,
            block_work,
            keep_state,
            carried,
        )

    return lax.fori_loop(0, key_count // key_block, key_step, running)


def fresh_state(unit_count, row_count, value_width):
    return (
        jnp.full((unit_count, row_count), -1e30, jnp.float32),
        jnp.zeros((unit_count, row_count), jnp.float32),
        jnp.zeros((unit_count, row_count, value_width), jnp.float32),
    )


def finished(running):
    row_peak, row_total, weighted = running
    return (weighted / row_total[:, :, None]).astype(jnp.bfloat16)


def joined_state(first, second):
    first_peak, first_total, first_weighted = first
    second_peak, second_total, second_weighted = second
    new_peak = jnp.maximum(first_peak, second_peak)
    first_shrink = jnp.exp(first_peak - new_peak)
    second_shrink = jnp.exp(second_peak - new_peak)
    new_total = first_total * first_shrink + second_total * second_shrink
    new_weighted = (
        first_weighted * first_shrink[:, :, None] + second_weighted * second_shrink[:, :, None]
    )
    return (new_peak, new_total, new_weighted)


def per_device(
    normed,
    query_weight,
    key_weight,
    value_weight,
    pool_in_weight,
    pool_weight,
    map_balance,
    head_gain,
    contrast_out_weight,
    pool_out_weight,
):
    tp_index = lax.axis_index("tp")
    sp_count = lax.axis_size("sp")
    sp_index = lax.axis_index("sp")
    head_dim = head_gain.shape[0] // 2
    value_width = 2 * head_dim
    query_cols = query_weight.shape[1]
    value_cols = value_weight.shape[1]
    unit_count = query_cols // head_dim
    heads_here = unit_count // 2
    project_incoming = lax.all_gather(normed, "tp", axis=0, tiled=True)
    products = [
        jnp.dot(project_incoming, weight_part, preferred_element_type=jnp.float32)
        for weight_part in (query_weight, key_weight, value_weight, pool_in_weight)
    ]
    joined = jnp.concatenate(products, axis=1).astype(jnp.bfloat16)
    row_count = joined.shape[0]
    queries = joined[:, :query_cols].reshape(row_count, unit_count, head_dim)
    key_rows = joined[:, query_cols : 2 * query_cols].reshape(row_count, unit_count, head_dim)
    value_rows = joined[:, 2 * query_cols : 2 * query_cols + value_cols].reshape(
        row_count, heads_here, value_width
    )
    pool_input = joined[:, 2 * query_cols + value_cols :]
    pool_cols = pool_input.shape[1]
    upper_rim = passed_along(pool_input[row_count - reach_back :], "sp", 1)
    extended = jnp.concatenate([upper_rim, pool_input], axis=0).astype(jnp.float32)
    groups_here = pool_weight.shape[0]
    group_width = pool_weight.shape[1]
    group_index = tp_index * groups_here + lax.iota(jnp.int32, pool_cols) // group_width
    widths = jnp.left_shift(jnp.int32(2), group_index % 4)
    window_sum = jnp.zeros((row_count, pool_cols), jnp.float32)
    for offset in range(reach_back + 1):
        window_sum = window_sum + extended[
            reach_back - offset : reach_back - offset + row_count
        ] * (offset < widths)[None, :].astype(jnp.float32)
    position = sp_index * row_count + lax.iota(jnp.int32, row_count)
    counts = jnp.minimum(position[:, None] + 1, widths[None, :]).astype(jnp.float32)
    spread = (window_sum / counts - extended[reach_back:]).astype(jnp.bfloat16)
    mixed_groups = jnp.einsum(
        "tgc,gce->tge",
        spread.reshape(row_count, groups_here, group_width),
        pool_weight,
        preferred_element_type=jnp.float32,
    )
    pool_out = mixed_groups.reshape(row_count, pool_cols).astype(jnp.bfloat16)
    score_scale = head_dim ** (-0.5)
    level_count = sp_count.bit_length() - 1
    low_levels = level_count // 2
    band_size = 1 << low_levels
    band_count = sp_count // band_size
    member = sp_index % band_size
    band = sp_index // band_size
    band_queries = queries
    for bit in range(low_levels):
        received = from_partner(band_queries, "sp", bit)
        upper = member >> bit & 1 == 1
        band_queries = jnp.where(
            upper,
            jnp.concatenate([received, band_queries], axis=0),
            jnp.concatenate([band_queries, received], axis=0),
        )
    band_first = band * band_size * row_count
    running = fresh_state(unit_count, band_size * row_count, value_width)
    for step in range(band_count):
        if step == 0:
            key_piece, value_piece = (key_rows, value_rows)
        else:
            key_piece, value_piece = shifted((key_rows, value_rows), "sp", step * band_size)
        source = (sp_index - step * band_size) % sp_count
        running = attend(
            running,
            band_queries,
            key_piece,
            value_piece,
            band_first,
            source * row_count,
            score_scale,
        )
    for bit in range(low_levels - 1, -1, -1):
        half = running[0].shape[1] // 2
        upper = member >> bit & 1 == 1
        lower_part = jax.tree.map(lambda item: item[:, :half], running)
        upper_part = jax.tree.map(lambda item: item[:, half:], running)
        outgoing = jax.tree.map(
            lambda low, high: jnp.where(upper, low, high), lower_part, upper_part
        )
        kept = jax.tree.map(lambda low, high: jnp.where(upper, high, low), lower_part, upper_part)
        incoming = from_partner(
            (as_sent(outgoing[0]), as_sent(outgoing[1]), as_sent(outgoing[2])), "sp", bit
        )
        running = joined_state(kept, incoming)
    maps = finished(running)
    paired = maps.reshape(heads_here, 2, row_count, value_width)
    paired = lax.optimization_barrier(paired).astype(jnp.float32)
    head_first = tp_index * heads_here
    balance_here = lax.dynamic_slice_in_dim(map_balance, head_first, heads_here, 0)
    contrast = paired[:, 0] - balance_here[:, None, None] * paired[:, 1]
    mean_square = jnp.mean(contrast * contrast, axis=2, keepdims=True)
    contrast = contrast * lax.rsqrt(mean_square + norm_epsilon) * head_gain
    contrast_out = (
        contrast.astype(jnp.bfloat16)
        .transpose(1, 0, 2)
        .reshape(row_count, heads_here * value_width)
    )
    partial_value = jnp.dot(contrast_out, contrast_out_weight, preferred_element_type=jnp.float32)
    return lax.psum_scatter(
        (
            partial_value + jnp.dot(pool_out, pool_out_weight, preferred_element_type=jnp.float32)
        ).astype(jnp.bfloat16),
        "tp",
        scatter_dimension=0,
        tiled=True,
    )


MESH = pl.DeviceIdType.MESH


def layer_kernel(
    sp_count,
    members,
    x_hbm,
    pool_weight_hbm,
    balance_hbm,
    gain_hbm,
    query_hbm,
    key_hbm,
    value_hbm,
    pool_in_hbm,
    contrast_hbm,
    pool_out_hbm,
    out_ref,
    out_recv,
    pool_weight,
    balance,
    gain,
    query_w,
    key_w,
    value_w,
    pool_in_w,
    contrast_w,
    pool_out_w,
    rows_in,
    kv,
    kv_stage,
    far_stage,
    queries,
    query_stage,
    peaks,
    totals,
    weighted,
    contrasts,
    contrast_stage,
    rim,
    rim_stage,
    pool_part,
    out_stage,
    weight_sem,
    local_sem,
    pair_send,
    pair_recv,
    relay_send,
    relay_recv,
    kv_send,
    kv_recv,
    forward_send,
    far_send,
    far_recv,
    far_forward,
    query_send,
    query_recv,
    contrast_send,
    contrast_recv,
    rim_send,
    rim_recv,
    out_send,
    out_recv_sem,
):
    f32 = jnp.float32
    bf16 = jnp.bfloat16
    sp = lax.axis_index("sp")
    tp = lax.axis_index("tp")
    other = 1 - tp
    plane = lax.div(sp, members)
    member = lax.rem(sp, members)
    upper = lax.div(plane, 2)
    side = lax.rem(plane, 2)
    across = lax.div(member, 2)
    along = lax.rem(member, 2)
    half_count = 2 * members
    half, model = x_hbm.shape
    rows = 2 * half
    width = gain.shape[1]
    head_dim = width // 2
    chunk = math.gcd(model, 512)
    chunks = 2
    piece = half // chunks
    in_lower = upper == 0
    in_upper = upper == 1
    crosses = plane == 1
    relays = plane == 2
    query_band = 2 * upper + tp
    bands_of = (plane, plane + 1 - 2 * side)

    keep = pltpu.make_async_copy(x_hbm, rows_in.at[0, tp], local_sem)
    keep.start()
    x_ref = rows_in.at[0, tp]

    near = pl.ds(pl.multiple_of(side * 2 * width, 2 * width), 2 * width)
    far = pl.ds(pl.multiple_of((1 - side) * 2 * width, 2 * width), 2 * width)
    far_loads = [
        pltpu.make_async_copy(src.at[:, far], dst.at[:, far], weight_sem.at[9 + i])
        for i, (src, dst) in enumerate(((key_hbm, key_w), (value_hbm, value_w)))
    ]
    loads = [
        pltpu.make_async_copy(src, dst, weight_sem.at[i])
        for i, (src, dst) in enumerate(
            (
                (query_hbm.at[:, near], query_w.at[:, near]),
                (key_hbm.at[:, near], key_w.at[:, near]),
                (value_hbm.at[:, near], value_w.at[:, near]),
                (pool_in_hbm, pool_in_w),
                (pool_out_hbm, pool_out_w),
                (contrast_hbm, contrast_w),
                (pool_weight_hbm, pool_weight),
                (balance_hbm, balance),
                (gain_hbm, gain),
            )
        )
    ]

    barrier = pltpu.get_barrier_semaphore()

    def greet(target):
        pl.semaphore_signal(barrier, inc=1, device_id=target, device_id_type=MESH)

    place = (side * members + member) * 2 + tp
    for d in range(1, 2 * half_count):
        goal = lax.rem(place + d, 2 * half_count)
        greet((upper * half_count + lax.div(goal, 2), lax.rem(goal, 2)))

    @pl.when(crosses)
    def _():
        greet((sp + members, tp))

    @pl.when(relays)
    def _():
        greet((sp - members, tp))

    @pl.when(sp == half_count - 1)
    def _():
        greet((sp + 1, tp))

    @pl.when(sp == half_count)
    def _():
        greet((sp - 1, tp))

    for load in loads[:3]:
        load.start()

    @pl.when(relays)
    def _():
        for load in far_loads:
            load.start()

    for load in loads[3:]:
        load.start()

    extra = jnp.where(jnp.logical_or(crosses, relays), 1, 0)
    extra = extra + jnp.where(jnp.logical_or(sp == half_count - 1, sp == half_count), 1, 0)
    pl.semaphore_wait(barrier, 2 * half_count - 1 + extra)

    def cut(ch):
        return pl.ds(ch * piece, piece)

    pair_first = pltpu.make_async_remote_copy(
        src_ref=x_ref,
        dst_ref=rows_in.at[0, tp],
        send_sem=pair_send.at[0, 0],
        recv_sem=pair_recv.at[0, 0],
        device_id=(sp, other),
        device_id_type=MESH,
    )

    def pair_copy(step, ch):
        return pltpu.make_async_remote_copy(
            src_ref=rows_in.at[step, tp, cut(ch)],
            dst_ref=rows_in.at[step, tp, cut(ch)],
            send_sem=pair_send.at[step, ch],
            recv_sem=pair_recv.at[step, ch],
            device_id=(sp, other),
            device_id_type=MESH,
        )

    def relay_copy(src, step, ch, target):
        return pltpu.make_async_remote_copy(
            src_ref=src.at[cut(ch)],
            dst_ref=rows_in.at[step, tp, cut(ch)],
            send_sem=relay_send.at[step, ch],
            recv_sem=relay_recv.at[step, ch],
            device_id=(target, tp),
            device_id_type=MESH,
        )

    def swap(ch):
        return relay_copy(x_ref, 1, ch, sp + members * (1 - 2 * side))

    def own_up(ch):
        return relay_copy(x_ref, 2, ch, sp + members)

    def low_up(ch):
        return relay_copy(rows_in.at[1, tp], 3, ch, sp + members)

    def top(step):
        return side == (1 if step == 0 else 0)

    def kv_copy(step, j, ch):
        goal = 2 * tp + j
        first = jnp.where(top(step), 1, along)
        return pltpu.make_async_remote_copy(
            src_ref=kv_stage.at[step, j, :, cut(ch)],
            dst_ref=kv.at[step, member, :, cut(ch)],
            send_sem=kv_send.at[step, j, ch],
            recv_sem=kv_recv.at[step, member, ch],
            device_id=(plane * members + goal, first),
            device_id_type=MESH,
        )

    def forward_copy(step, source, ch):
        return pltpu.make_async_remote_copy(
            src_ref=kv.at[step, source, :, cut(ch)],
            dst_ref=kv.at[step, source, :, cut(ch)],
            send_sem=forward_send.at[step, source, ch],
            recv_sem=kv_recv.at[step, source, ch],
            device_id=(sp, other),
            device_id_type=MESH,
        )

    def query_copy(step, j, ch):
        core = jnp.where(top(step), 1, 0)
        return pltpu.make_async_remote_copy(
            src_ref=query_stage.at[step, j, :, cut(ch)],
            dst_ref=queries.at[member, :, cut(ch)],
            send_sem=query_send.at[step, j, ch],
            recv_sem=query_recv.at[member, ch],
            device_id=(plane * members + 2 * tp + j, core),
            device_id_type=MESH,
        )

    own_goal = across == tp

    def far_copy(step, ch, goal_side, j):
        slot = goal_side * 2 + j
        goal = (2 * upper + goal_side) * members + 2 * tp + j
        return pltpu.make_async_remote_copy(
            src_ref=far_stage.at[step - 2, slot, ch],
            dst_ref=kv.at[step, member, ch],
            send_sem=far_send.at[step - 2, slot, ch],
            recv_sem=far_recv.at[step - 2, member, ch],
            device_id=(goal, along),
            device_id_type=MESH,
        )

    def far_pass(step, source, ch):
        return pltpu.make_async_remote_copy(
            src_ref=kv.at[step, source, ch],
            dst_ref=kv.at[step, source, ch],
            send_sem=far_forward.at[step - 2, source, ch],
            recv_sem=far_recv.at[step - 2, source, ch],
            device_id=(sp, other),
            device_id_type=MESH,
        )

    def far_stays(goal_side, j):
        return jnp.logical_and(goal_side == side, jnp.logical_and(own_goal, j == along))

    def far_here(source):
        return jnp.logical_and(relays, source == member)

    def far_passes(source):
        return jnp.logical_and(source % 2 == tp, jnp.logical_not(far_here(source)))

    def far_awaits(source):
        return jnp.logical_not(jnp.logical_and(far_here(source), own_goal))

    def own_stays(step, j):
        return jnp.logical_and(own_goal, j == along)

    def query_stays(step, j):
        return jnp.logical_and(own_stays(step, j), jnp.where(top(step), 1, 0) == tp)

    def own_forwards(step):
        return jnp.logical_and(
            own_goal, jnp.logical_or(jnp.logical_not(top(step)), tp == 0)
        )

    def passes_on(step, source):
        mine = jnp.logical_and(source % 2 == tp, jnp.logical_not(top(step)))
        return jnp.logical_and(source != member, mine)

    def awaits(step, source):
        needed = jnp.logical_or(tp == 1, jnp.logical_not(top(step)))
        made_here = jnp.logical_and(source == member, own_goal)
        return jnp.logical_and(needed, jnp.logical_not(made_here))

    def contrast_stays(i):
        return jnp.logical_and(
            jnp.logical_and(query_band == plane, i == member), across == tp
        )

    head_here = 2 * side + along

    def contrast_copy(i):
        return pltpu.make_async_remote_copy(
            src_ref=contrast_stage.at[i],
            dst_ref=contrasts.at[head_here],
            send_sem=contrast_send.at[i],
            recv_sem=contrast_recv.at[head_here],
            device_id=(query_band * members + i, across),
            device_id_type=MESH,
        )

    def contrast_incoming(head):
        return pltpu.make_async_remote_copy(
            src_ref=contrast_stage.at[0],
            dst_ref=contrasts.at[head],
            send_sem=contrast_send.at[0],
            recv_sem=contrast_recv.at[head],
            device_id=(sp, other),
            device_id_type=MESH,
        )

    def contrast_local(head):
        same = jnp.logical_and(head // 2 == side, 2 * tp + head % 2 == member)
        return jnp.logical_and(same, side == tp)

    rim_copy = pltpu.make_async_remote_copy(
        src_ref=rim_stage,
        dst_ref=rim,
        send_sem=rim_send,
        recv_sem=rim_recv,
        device_id=(lax.rem(sp + 1, sp_count), tp),
        device_id_type=MESH,
    )

    def out_copy(start):
        span = slice(start, start + chunk)
        return pltpu.make_async_remote_copy(
            src_ref=out_stage.at[:, span],
            dst_ref=out_recv.at[:, span],
            send_sem=out_send.at[start // chunk],
            recv_sem=out_recv_sem.at[start // chunk],
            device_id=(sp, other),
            device_id_type=MESH,
        )


    keep.wait()
    pair_first.start()
    for ch in range(chunks):
        swap(ch).start()

        @pl.when(crosses)
        def _(ch=ch):
            own_up(ch).start()

    peaks[...] = jnp.full(peaks.shape, -1e30, f32)
    totals[...] = jnp.zeros(totals.shape, f32)
    weighted[...] = jnp.zeros(weighted.shape, f32)

    def project(step, pieces):
        here = cut(pieces[0]) if len(pieces) == 1 else slice(None)

        def one(t, carry):
            j = jnp.where(t == 0, 1 - along, along)
            columns = pl.ds(pl.multiple_of((2 * side + j) * width, width), width)
            x = rows_in[step, :, here, :].reshape(-1, model)

            def through(held):
                dot = jnp.dot(x, held[:, columns], preferred_element_type=f32)
                return dot.astype(bf16).reshape(2, -1, width)

            mine = through(query_w)
            keys = through(key_w)
            values = through(value_w)
            kept = query_stays(step, j)
            stays = own_stays(step, j)

            @pl.when(jnp.logical_not(kept))
            def _():
                query_stage[step, j, :, here] = mine
                for ch in pieces:
                    query_copy(step, j, ch).start()

            @pl.when(kept)
            def _():
                queries[member, :, here] = mine

            @pl.when(jnp.logical_not(stays))
            def _():
                kv_stage[step, j, :, here, :width] = keys
                kv_stage[step, j, :, here, width:] = values
                for ch in pieces:
                    kv_copy(step, j, ch).start()

            @pl.when(stays)
            def _():
                kv[step, member, :, here, :width] = keys
                kv[step, member, :, here, width:] = values

                @pl.when(own_forwards(step))
                def _():
                    for ch in pieces:
                        forward_copy(step, member, ch).start()

            return carry

        lax.fori_loop(0, 2, one, 0)

    def project_far(step, ch):
        pair_copy(step, ch).wait_recv()

        def one(t, carry):
            goal_side = 1 - lax.div(t, 2)
            j = jnp.where(lax.rem(t, 2) == 0, 1 - along, along)
            columns = pl.ds(pl.multiple_of((2 * goal_side + j) * width, width), width)
            x = rows_in[step, :, cut(ch), :].reshape(half, model)
            keys = jnp.dot(x, key_w[:, columns], preferred_element_type=f32).astype(bf16)
            values = jnp.dot(x, value_w[:, columns], preferred_element_type=f32).astype(bf16)
            stays = far_stays(goal_side, j)

            @pl.when(jnp.logical_not(stays))
            def _():
                far_stage[step - 2, goal_side * 2 + j, ch, :, :width] = keys
                far_stage[step - 2, goal_side * 2 + j, ch, :, width:] = values
                far_copy(step, ch, goal_side, j).start()

            @pl.when(stays)
            def _():
                kv[step, member, ch, :, :width] = keys
                kv[step, member, ch, :, width:] = values
                far_pass(step, member, ch).start()

            return carry

        lax.fori_loop(0, 4, one, 0)

    def take_swap(ch):
        swap(ch).wait_recv()

        @pl.when(crosses)
        def _():
            low_up(ch).start()

        pair_copy(1, ch).start()

    def take_far(step, ch):
        (own_up(ch) if step == 2 else low_up(ch)).wait_recv()
        pair_copy(step, ch).start()

    def project_swap(ch):
        pair_copy(1, ch).wait_recv()
        project(1, (ch,))

    log_scale = head_dim ** (-0.5) * math.log2(math.e)

    def attend_block(step, i, seen, masked):
        for u in range(2):
            cols = slice(u * head_dim, (u + 1) * head_dim)
            keys = kv[step, :seen, :, :, cols].reshape(-1, head_dim)
            values = kv[step, :seen, :, :, width:].reshape(-1, width)
            scores = lax.dot_general(
                queries[i, :, :, cols].reshape(rows, head_dim), keys, (((1,), (1,)), ((), ())), preferred_element_type=f32
            )
            if masked:
                query_order = lax.broadcasted_iota(jnp.int32, scores.shape, 0) + (seen - 1) * rows
                key_order = lax.broadcasted_iota(jnp.int32, scores.shape, 1)
                scores = jnp.where(key_order <= query_order, scores, -jnp.inf)
            old = peaks[u, i][:, :1]
            peak = jnp.maximum(jnp.max(scores, axis=1, keepdims=True), old)
            shrink = jnp.exp2((old - peak) * log_scale)
            raised = jnp.exp2((scores - peak) * log_scale)
            total = jnp.sum(raised, axis=1, keepdims=True)
            update = jnp.dot(raised.astype(bf16), values, preferred_element_type=f32)
            total = total + totals[u, i][:, :1] * shrink
            update = update + weighted[u, i] * shrink
            peaks[u, i] = jnp.broadcast_to(peak, peaks.shape[2:])
            totals[u, i] = jnp.broadcast_to(total, totals.shape[2:])
            weighted[u, i] = update

    def finished_block(i):
        first = (weighted[0, i] * (1.0 / totals[0, i][:, :1])).astype(bf16).astype(f32)
        second = (weighted[1, i] * (1.0 / totals[1, i][:, :1])).astype(bf16).astype(f32)
        contrast = first - balance[across * members + head_here] * second
        mean_square = jnp.mean(contrast * contrast, axis=1, keepdims=True)
        return (contrast * lax.rsqrt(mean_square + norm_epsilon) * gain[...]).astype(bf16)

    def send_block(i, result):
        stays = contrast_stays(i)

        @pl.when(jnp.logical_not(stays))
        def _():
            contrast_stage[i] = result
            contrast_copy(i).start()

        @pl.when(stays)
        def _():
            contrasts[head_here] = result

    def turn(t):
        return lax.rem(member + 1 + t, members)

    def block_pairs(work):
        def one(t, carry):
            work(turn(2 * t), turn(2 * t + 1))
            return carry

        lax.fori_loop(0, members // 2, one, 0)

    def finish_pair(i, k):
        results = finished_block(i), finished_block(k)
        send_block(i, results[0])
        send_block(k, results[1])

    def lands_here(step, source):
        return jnp.logical_and(
            source != member, jnp.where(top(step), 1, source % 2) == tp
        )

    def pass_on(step):
        for ch in range(chunks):
            for source in range(members):

                @pl.when(lands_here(step, source))
                def _(source=source, ch=ch):
                    forward_copy(step, source, ch).wait_recv()

                @pl.when(passes_on(step, source))
                def _(source=source, ch=ch):
                    forward_copy(step, source, ch).start()

    def arrive(step):
        for ch in range(chunks):
            for source in range(members):
                passed = jnp.logical_not(lands_here(step, source))

                @pl.when(jnp.logical_and(awaits(step, source), passed))
                def _(source=source, ch=ch):
                    forward_copy(step, source, ch).wait_recv()

    def attend(step, between):
        band = bands_of[step]

        @pl.when(band == query_band)
        def _():
            for i in range(members):
                if i == members // 2:
                    between()
                attend_block(step, i, i + 1, True)

        @pl.when(band < query_band)
        def _():
            def one(t, carry):
                attend_block(step, turn(2 * t), members, False)
                attend_block(step, turn(2 * t + 1), members, False)

                @pl.when(t == 0)
                def _():
                    between()

                return carry

            lax.fori_loop(0, members // 2, one, 0)

        @pl.when(band > query_band)
        def _():
            between()

    def far_pass_on(step, ch):
        for source in range(members):

            @pl.when(far_passes(source))
            def _(source=source):
                far_pass(step, source, ch).wait_recv()
                far_pass(step, source, ch).start()

    def far_arrive(step, ch):
        for source in range(members):
            passed = jnp.logical_not(far_passes(source))

            @pl.when(jnp.logical_and(far_awaits(source), passed))
            def _(source=source):
                far_pass(step, source, ch).wait_recv()

    loads[0].wait()
    loads[1].wait()
    loads[2].wait()
    pair_first.wait_recv()
    project(0, tuple(range(chunks)))

    loads[3].wait()
    pool_input = jnp.dot(
        rows_in[0].reshape(rows, model), pool_in_w[...], preferred_element_type=f32
    ).astype(bf16)
    rim_stage[...] = pool_input[rows - rim.shape[0] :]

    @pl.when(sp + 1 < sp_count)
    def _():
        rim_copy.start()

    take_swap(0)

    @pl.when(relays)
    def _():
        take_far(2, 0)

    project_swap(0)

    @pl.when(relays)
    def _():
        for load in far_loads:
            load.wait()
        project_far(2, 0)

    take_swap(1)

    @pl.when(relays)
    def _():
        take_far(2, 1)

    project_swap(1)

    @pl.when(relays)
    def _():
        project_far(2, 1)
        take_far(3, 0)

    pass_on(0)

    @pl.when(relays)
    def _():
        project_far(3, 0)

    def query_incoming(source, ch):
        return pltpu.make_async_remote_copy(
            src_ref=query_stage.at[0, 0, :, cut(ch)],
            dst_ref=queries.at[source, :, cut(ch)],
            send_sem=query_send.at[0, 0, ch],
            recv_sem=query_recv.at[source, ch],
            device_id=(sp, other),
            device_id_type=MESH,
        )

    def take_queries():
        for source in range(members):

            @pl.when(jnp.logical_not(jnp.logical_and(source == member, own_goal)))
            def _(source=source):
                for ch in range(chunks):
                    query_incoming(source, ch).wait_recv()

    idle_first = jnp.logical_and(in_upper, jnp.logical_and(side == 1, tp == 0))

    @pl.when(idle_first)
    def _():
        far_pass_on(2, 0)
        far_pass_on(2, 1)

    @pl.when(jnp.logical_and(relays, tp == 1))
    def _():
        take_far(3, 1)
        project_far(3, 1)

    take_queries()
    arrive(0)

    def last_rows():
        @pl.when(jnp.logical_and(relays, tp == 0))
        def _():
            take_far(3, 1)

    attend(0, last_rows)

    @pl.when(jnp.logical_and(relays, tp == 0))
    def _():
        project_far(3, 1)

    def last_passes():
        @pl.when(jnp.logical_and(in_upper, side == 1))
        def _():
            far_pass_on(3, 1)

    def attend_swapped():
        pass_on(1)

        @pl.when(jnp.logical_and(in_upper, side == 1))
        def _():
            far_pass_on(3, 0)

        arrive(1)
        attend(1, last_passes)

    @pl.when(in_upper)
    def _():
        @pl.when(jnp.logical_not(idle_first))
        def _():
            far_pass_on(2, 0)
            far_pass_on(2, 1)

        @pl.when(relays)
        def _():
            attend_swapped()
            far_pass_on(3, 0)

        far_arrive(2, 0)
        far_arrive(2, 1)

        def one(t, carry):
            attend_block(2, turn(2 * t), members, False)
            attend_block(2, turn(2 * t + 1), members, False)

            @pl.when(jnp.logical_and(t == 0, jnp.logical_and(relays, tp == 1)))
            def _():
                far_pass_on(3, 1)

            return carry

        lax.fori_loop(0, members // 2, one, 0)

    @pl.when(jnp.logical_not(relays))
    def _():
        attend_swapped()

    for load in loads[6:]:
        load.wait()

    @pl.when(in_lower)
    def _():
        block_pairs(finish_pair)

    @pl.when(in_upper)
    def _():
        @pl.when(jnp.logical_and(relays, tp == 0))
        def _():
            far_pass_on(3, 1)

        far_arrive(3, 0)
        far_arrive(3, 1)

        def last_pair(i, k):
            attend_block(3, i, members, False)
            attend_block(3, k, members, False)
            finish_pair(i, k)

        block_pairs(last_pair)

    @pl.when(sp > 0)
    def _():
        rim_copy.wait_recv()

    @pl.when(sp == 0)
    def _():
        rim[...] = jnp.zeros_like(rim)

    loads[4].wait()
    extended = jnp.concatenate([rim[...], pool_input], axis=0).astype(f32)
    group_width = pool_weight.shape[1]
    skirt = rim.shape[0]
    position = sp * rows + lax.broadcasted_iota(jnp.int32, (rows, group_width), 0)
    mixed = []
    for group in range(pool_weight.shape[0]):
        block = extended[:, group * group_width : (group + 1) * group_width]
        window = block
        reach = 1
        span = 2 ** (1 + group % 4)
        while reach < span:
            window = window + pltpu.roll(window, reach, 0)
            reach *= 2
        counts = jnp.minimum(position + 1, span).astype(f32)
        spread = (window[skirt:] / counts - block[skirt:]).astype(bf16)
        mixed.append(
            jnp.dot(spread, pool_weight[group], preferred_element_type=f32).astype(bf16)
        )
    pool_out = jnp.concatenate(mixed, axis=1)
    for start in range(0, model, chunk):
        pool_part[:, start : start + chunk] = jnp.dot(
            pool_out, pool_out_w[:, start : start + chunk], preferred_element_type=f32
        )

    pair_first.wait_send()
    for ch in range(chunks):
        swap(ch).wait_send()
        pair_copy(1, ch).wait_send()

        @pl.when(crosses)
        def _(ch=ch):
            own_up(ch).wait_send()
            low_up(ch).wait_send()

        @pl.when(relays)
        def _(ch=ch):
            for step in range(2, 4):
                pair_copy(step, ch).wait_send()
                for slot in range(4):

                    @pl.when(jnp.logical_not(far_stays(slot // 2, slot % 2)))
                    def _(step=step, slot=slot):
                        far_copy(step, ch, slot // 2, slot % 2).wait_send()

                @pl.when(own_goal)
                def _(step=step):
                    far_pass(step, member, ch).wait_send()

        @pl.when(in_upper)
        def _(ch=ch):
            for step in range(2, 4):
                for source in range(members):

                    @pl.when(far_passes(source))
                    def _(step=step, source=source):
                        far_pass(step, source, ch).wait_send()

    def drain(step, ch):
        for j in range(2):

            @pl.when(jnp.logical_not(own_stays(step, j)))
            def _(j=j):
                kv_copy(step, j, ch).wait_send()

            @pl.when(jnp.logical_not(query_stays(step, j)))
            def _(j=j):
                query_copy(step, j, ch).wait_send()

        @pl.when(own_forwards(step))
        def _():
            forward_copy(step, member, ch).wait_send()

        for source in range(members):

            @pl.when(passes_on(step, source))
            def _(source=source):
                forward_copy(step, source, ch).wait_send()

    for ch in range(chunks):
        drain(0, ch)
        drain(1, ch)

    @pl.when(sp + 1 < sp_count)
    def _():
        rim_copy.wait_send()

    loads[5].wait()
    for head in range(members):

        @pl.when(jnp.logical_not(contrast_local(head)))
        def _(head=head):
            contrast_incoming(head).wait_recv()

    left = jnp.concatenate([contrasts[h] for h in range(members)], axis=1)
    for start in range(0, model, chunk):
        span = slice(start, start + chunk)
        part = jnp.dot(left, contrast_w[:, span], preferred_element_type=f32)
        part = part + pool_part[:, span]
        low, high = part[:half], part[half:]
        out_stage[:, span] = jnp.where(tp == 0, high, low).astype(bf16)
        out_copy(start).start()
        out_ref[:, span] = jnp.where(tp == 0, low, high).astype(bf16)

    for start in range(0, model, chunk):
        out_copy(start).wait()

    for i in range(members):

        @pl.when(jnp.logical_not(contrast_stays(i)))
        def _(i=i):
            contrast_copy(i).wait_send()


def kernel_scratch(members, half, model, width, pool_cols, heads, groups_here):
    bf16 = jnp.bfloat16
    rows = 2 * half
    group_width = pool_cols // groups_here
    dma = pltpu.SemaphoreType.DMA
    return [
        pltpu.VMEM((groups_here, group_width, group_width), bf16),
        pltpu.SMEM((heads,), jnp.float32),
        pltpu.VMEM((1, width), jnp.float32),
        pltpu.VMEM((model, members * width), bf16),
        pltpu.VMEM((model, members * width), bf16),
        pltpu.VMEM((model, members * width), bf16),
        pltpu.VMEM((model, pool_cols), bf16),
        pltpu.VMEM((members * width, model), bf16),
        pltpu.VMEM((pool_cols, model), bf16),
        pltpu.VMEM((4, 2, half, model), bf16),
        pltpu.VMEM((4, members, 2, half, 2 * width), bf16),
        pltpu.VMEM((2, 2, 2, half, 2 * width), bf16),
        pltpu.VMEM((2, 4, 2, half, 2 * width), bf16),
        pltpu.VMEM((members, 2, half, width), bf16),
        pltpu.VMEM((2, 2, 2, half, width), bf16),
        pltpu.VMEM((2, members, rows, 128), jnp.float32),
        pltpu.VMEM((2, members, rows, 128), jnp.float32),
        pltpu.VMEM((2, members, rows, width), jnp.float32),
        pltpu.VMEM((members, rows, width), bf16),
        pltpu.VMEM((members, rows, width), bf16),
        pltpu.VMEM((reach_back + 1, pool_cols), bf16),
        pltpu.VMEM((reach_back + 1, pool_cols), bf16),
        pltpu.VMEM((rows, model), jnp.float32),
        pltpu.VMEM((half, model), bf16),
        dma((11,)),
        dma,
        dma((4, 2)),
        dma((4, 2)),
        dma((4, 2)),
        dma((4, 2)),
        dma((2, 2, 2)),
        dma((2, members, 2)),
        dma((2, members, 2)),
        dma((2, 4, 2)),
        dma((2, members, 2)),
        dma((2, members, 2)),
        dma((2, 2, 2)),
        dma((members, 2)),
        dma((members,)),
        dma((members,)),
        dma,
        dma,
        dma((model // math.gcd(model, 512),)),
        dma((model // math.gcd(model, 512),)),
    ]


vmem_most = 67043328
kernel_grant = 54 * 2**20


def scratch_bytes(scratch):
    return sum(
        math.prod(item.shape) * jnp.dtype(item.dtype).itemsize
        for item in scratch
        if getattr(item, "memory_space", None) == pltpu.VMEM
    )


def whole_layer(
    normed,
    query_weight,
    key_weight,
    value_weight,
    pool_in_weight,
    pool_weight,
    map_balance,
    head_gain,
    contrast_out_weight,
    pool_out_weight,
):
    sp_count = lax.axis_size("sp")
    width = head_gain.shape[0]
    members = query_weight.shape[1] // width
    half, model = normed.shape
    pool_cols = pool_in_weight.shape[1]
    groups_here = pool_weight.shape[0]
    heads = map_balance.shape[0]
    scratch = kernel_scratch(
        max(members, 1), half, model, width, pool_cols, heads, groups_here
    )
    fits = (
        lax.axis_size("tp") == 2
        and members == 4
        and sp_count == 4 * members
        and groups_here % 4 == 0
        and scratch_bytes(scratch) < vmem_most * 3 // 4
    )
    if not fits:
        return per_device(
            normed,
            query_weight,
            key_weight,
            value_weight,
            pool_in_weight,
            pool_weight,
            map_balance,
            head_gain,
            contrast_out_weight,
            pool_out_weight,
        )
    vmem = pl.BlockSpec(memory_space=pltpu.VMEM)
    hbm = pl.BlockSpec(memory_space=pltpu.HBM)
    own_part, partner_part = pl.pallas_call(
        functools.partial(layer_kernel, sp_count, members),
        out_shape=[pltpu.VMEM((half, model), jnp.bfloat16)] * 2,
        in_specs=[hbm] * 10,
        out_specs=[vmem, vmem],
        scratch_shapes=scratch,
        compiler_params=pltpu.CompilerParams(
            collective_id=0, has_side_effects=True, vmem_limit_bytes=kernel_grant
        ),
    )(
        normed,
        pool_weight,
        map_balance,
        head_gain.reshape(1, width),
        query_weight,
        key_weight,
        value_weight,
        pool_in_weight,
        contrast_out_weight,
        pool_out_weight,
    )
    return (own_part.astype(jnp.float32) + partner_part.astype(jnp.float32)).astype(jnp.bfloat16)


def solution(mesh):
    return jax.shard_map(
        whole_layer,
        mesh=mesh,
        in_specs=(
            P(("sp", "tp"), None),
            P(None, "tp"),
            P(None, "tp"),
            P(None, "tp"),
            P(None, "tp"),
            P("tp", None, None),
            P(),
            P(),
            P("tp", None),
            P("tp", None),
        ),
        out_specs=P(("sp", "tp"), None),
        check_vma=False,
    )
```

```python
import functools
import math

import jax
import jax.numpy as jnp
from jax import lax
from jax.experimental import pallas as pl
from jax.experimental.pallas import tpu as pltpu
from jax.sharding import PartitionSpec as P

reach_back = 15
norm_epsilon = 1e-06


def passed_along(block, axis, distance):
    devices = range(lax.axis_size(axis))
    route = [(i - distance, i) for i in devices if i - distance in devices]
    return lax.ppermute(block, axis, route)


def from_partner(block, axis, stride):
    count = lax.axis_size(axis)
    route = []
    for low in range(count):
        high = low | 1 << stride
        if high != low and high < count:
            route += [(low, high), (high, low)]
    return lax.ppermute(block, axis, route)


def shifted(array, axis, by):
    size = lax.axis_size(axis)
    return lax.ppermute(array, axis, [(i, (i + by) % size) for i in range(size)])


def as_sent(array):

    def short(part):
        return part.astype(jnp.bfloat16) if part.dtype == jnp.float32 else part

    return jax.tree.map(short, array)


def attend(running, queries, key_rows, value_rows, query_first, key_first, score_scale):
    key_count = key_rows.shape[0]
    key_block = math.gcd(key_count, 1024)
    unit_count = queries.shape[1]
    heads_here = value_rows.shape[1]
    per_head = unit_count // heads_here
    query_count = queries.shape[0]
    query_order = query_first + lax.iota(jnp.int32, query_count)

    def key_step(block_index, carried):
        block_start = block_index * key_block

        def block_work(current):
            row_peak, row_total, weighted = current
            scores = (
                jnp.einsum("qud,kud->uqk", queries, key_rows, preferred_element_type=jnp.float32)
                * score_scale
            )
            key_order = key_first + block_start + lax.iota(jnp.int32, key_block)
            scores = jnp.where(
                key_order[None, None, :] <= query_order[None, :, None], scores, -jnp.inf
            )
            new_peak = jnp.maximum(row_peak, jnp.max(scores, axis=2))
            shrink = jnp.exp(row_peak - new_peak)
            raised = jnp.exp(scores - new_peak[:, :, None])
            row_total = row_total * shrink + jnp.sum(raised, axis=2)
            map_weights = raised.astype(jnp.bfloat16).reshape(
                heads_here, per_head, query_count, key_block
            )
            update = jnp.einsum(
                "hmqk,khe->hmqe", map_weights, value_rows, preferred_element_type=jnp.float32
            )
            weighted = weighted * shrink[:, :, None] + update.reshape(unit_count, query_count, -1)
            return (new_peak, row_total, weighted)

        def keep_state(current):
            return current

        return lax.cond(
            key_first + block_start <= query_first + query_count - 1,
            block_work,
            keep_state,
            carried,
        )

    return lax.fori_loop(0, key_count // key_block, key_step, running)


def fresh_state(unit_count, row_count, value_width):
    return (
        jnp.full((unit_count, row_count), -1e30, jnp.float32),
        jnp.zeros((unit_count, row_count), jnp.float32),
        jnp.zeros((unit_count, row_count, value_width), jnp.float32),
    )


def finished(running):
    row_peak, row_total, weighted = running
    return (weighted / row_total[:, :, None]).astype(jnp.bfloat16)


def joined_state(first, second):
    first_peak, first_total, first_weighted = first
    second_peak, second_total, second_weighted = second
    new_peak = jnp.maximum(first_peak, second_peak)
    first_shrink = jnp.exp(first_peak - new_peak)
    second_shrink = jnp.exp(second_peak - new_peak)
    new_total = first_total * first_shrink + second_total * second_shrink
    new_weighted = (
        first_weighted * first_shrink[:, :, None] + second_weighted * second_shrink[:, :, None]
    )
    return (new_peak, new_total, new_weighted)


def per_device(
    normed,
    query_weight,
    key_weight,
    value_weight,
    pool_in_weight,
    pool_weight,
    map_balance,
    head_gain,
    contrast_out_weight,
    pool_out_weight,
):
    tp_index = lax.axis_index("tp")
    sp_count = lax.axis_size("sp")
    sp_index = lax.axis_index("sp")
    head_dim = head_gain.shape[0] // 2
    value_width = 2 * head_dim
    query_cols = query_weight.shape[1]
    value_cols = value_weight.shape[1]
    unit_count = query_cols // head_dim
    heads_here = unit_count // 2
    project_incoming = lax.all_gather(normed, "tp", axis=0, tiled=True)
    products = [
        jnp.dot(project_incoming, weight_part, preferred_element_type=jnp.float32)
        for weight_part in (query_weight, key_weight, value_weight, pool_in_weight)
    ]
    joined = jnp.concatenate(products, axis=1).astype(jnp.bfloat16)
    row_count = joined.shape[0]
    queries = joined[:, :query_cols].reshape(row_count, unit_count, head_dim)
    key_rows = joined[:, query_cols : 2 * query_cols].reshape(row_count, unit_count, head_dim)
    value_rows = joined[:, 2 * query_cols : 2 * query_cols + value_cols].reshape(
        row_count, heads_here, value_width
    )
    pool_input = joined[:, 2 * query_cols + value_cols :]
    pool_cols = pool_input.shape[1]
    upper_rim = passed_along(pool_input[row_count - reach_back :], "sp", 1)
    extended = jnp.concatenate([upper_rim, pool_input], axis=0).astype(jnp.float32)
    groups_here = pool_weight.shape[0]
    group_width = pool_weight.shape[1]
    group_index = tp_index * groups_here + lax.iota(jnp.int32, pool_cols) // group_width
    widths = jnp.left_shift(jnp.int32(2), group_index % 4)
    window_sum = jnp.zeros((row_count, pool_cols), jnp.float32)
    for offset in range(reach_back + 1):
        window_sum = window_sum + extended[
            reach_back - offset : reach_back - offset + row_count
        ] * (offset < widths)[None, :].astype(jnp.float32)
    position = sp_index * row_count + lax.iota(jnp.int32, row_count)
    counts = jnp.minimum(position[:, None] + 1, widths[None, :]).astype(jnp.float32)
    spread = (window_sum / counts - extended[reach_back:]).astype(jnp.bfloat16)
    mixed_groups = jnp.einsum(
        "tgc,gce->tge",
        spread.reshape(row_count, groups_here, group_width),
        pool_weight,
        preferred_element_type=jnp.float32,
    )
    pool_out = mixed_groups.reshape(row_count, pool_cols).astype(jnp.bfloat16)
    score_scale = head_dim ** (-0.5)
    level_count = sp_count.bit_length() - 1
    low_levels = level_count // 2
    band_size = 1 << low_levels
    band_count = sp_count // band_size
    member = sp_index % band_size
    band = sp_index // band_size
    band_queries = queries
    for bit in range(low_levels):
        received = from_partner(band_queries, "sp", bit)
        upper = member >> bit & 1 == 1
        band_queries = jnp.where(
            upper,
            jnp.concatenate([received, band_queries], axis=0),
            jnp.concatenate([band_queries, received], axis=0),
        )
    band_first = band * band_size * row_count
    running = fresh_state(unit_count, band_size * row_count, value_width)
    for step in range(band_count):
        if step == 0:
            key_piece, value_piece = (key_rows, value_rows)
        else:
            key_piece, value_piece = shifted((key_rows, value_rows), "sp", step * band_size)
        source = (sp_index - step * band_size) % sp_count
        running = attend(
            running,
            band_queries,
            key_piece,
            value_piece,
            band_first,
            source * row_count,
            score_scale,
        )
    for bit in range(low_levels - 1, -1, -1):
        half = running[0].shape[1] // 2
        upper = member >> bit & 1 == 1
        lower_part = jax.tree.map(lambda item: item[:, :half], running)
        upper_part = jax.tree.map(lambda item: item[:, half:], running)
        outgoing = jax.tree.map(
            lambda low, high: jnp.where(upper, low, high), lower_part, upper_part
        )
        kept = jax.tree.map(lambda low, high: jnp.where(upper, high, low), lower_part, upper_part)
        incoming = from_partner(
            (as_sent(outgoing[0]), as_sent(outgoing[1]), as_sent(outgoing[2])), "sp", bit
        )
        running = joined_state(kept, incoming)
    maps = finished(running)
    paired = maps.reshape(heads_here, 2, row_count, value_width)
    paired = lax.optimization_barrier(paired).astype(jnp.float32)
    head_first = tp_index * heads_here
    balance_here = lax.dynamic_slice_in_dim(map_balance, head_first, heads_here, 0)
    contrast = paired[:, 0] - balance_here[:, None, None] * paired[:, 1]
    mean_square = jnp.mean(contrast * contrast, axis=2, keepdims=True)
    contrast = contrast * lax.rsqrt(mean_square + norm_epsilon) * head_gain
    contrast_out = (
        contrast.astype(jnp.bfloat16)
        .transpose(1, 0, 2)
        .reshape(row_count, heads_here * value_width)
    )
    partial_value = jnp.dot(contrast_out, contrast_out_weight, preferred_element_type=jnp.float32)
    return lax.psum_scatter(
        (
            partial_value + jnp.dot(pool_out, pool_out_weight, preferred_element_type=jnp.float32)
        ).astype(jnp.bfloat16),
        "tp",
        scatter_dimension=0,
        tiled=True,
    )


MESH = pl.DeviceIdType.MESH


def layer_kernel(
    sp_count,
    members,
    x_hbm,
    pool_weight_hbm,
    balance_hbm,
    gain_hbm,
    query_hbm,
    key_hbm,
    value_hbm,
    pool_in_hbm,
    contrast_hbm,
    pool_out_hbm,
    out_ref,
    out_recv,
    pool_weight,
    balance,
    gain,
    query_w,
    key_w,
    value_w,
    pool_in_w,
    contrast_w,
    pool_out_w,
    rows_in,
    kv,
    kv_stage,
    far_stage,
    queries,
    query_stage,
    peaks,
    totals,
    weighted,
    contrasts,
    contrast_stage,
    rim,
    rim_stage,
    pool_part,
    out_stage,
    weight_sem,
    local_sem,
    pair_send,
    pair_recv,
    relay_send,
    relay_recv,
    kv_send,
    kv_recv,
    forward_send,
    far_send,
    far_recv,
    far_forward,
    query_send,
    query_recv,
    contrast_send,
    contrast_recv,
    rim_send,
    rim_recv,
    out_send,
    out_recv_sem,
):
    f32 = jnp.float32
    bf16 = jnp.bfloat16
    sp = lax.axis_index("sp")
    tp = lax.axis_index("tp")
    other = 1 - tp
    plane = lax.div(sp, members)
    member = lax.rem(sp, members)
    upper = lax.div(plane, 2)
    side = lax.rem(plane, 2)
    across = lax.div(member, 2)
    along = lax.rem(member, 2)
    half_count = 2 * members
    half, model = x_hbm.shape
    rows = 2 * half
    width = gain.shape[1]
    head_dim = width // 2
    chunk = math.gcd(model, 512)
    chunks = 2
    piece = half // chunks
    in_lower = upper == 0
    in_upper = upper == 1
    crosses = plane == 1
    relays = plane == 2
    query_band = 2 * upper + tp
    bands_of = (plane, plane + 1 - 2 * side)

    keep = pltpu.make_async_copy(x_hbm, rows_in.at[0, tp], local_sem)
    keep.start()
    x_ref = rows_in.at[0, tp]

    near = pl.ds(pl.multiple_of(side * 2 * width, 2 * width), 2 * width)
    far = pl.ds(pl.multiple_of((1 - side) * 2 * width, 2 * width), 2 * width)
    far_loads = [
        pltpu.make_async_copy(src.at[:, far], dst.at[:, far], weight_sem.at[9 + i])
        for i, (src, dst) in enumerate(((key_hbm, key_w), (value_hbm, value_w)))
    ]
    loads = [
        pltpu.make_async_copy(src, dst, weight_sem.at[i])
        for i, (src, dst) in enumerate(
            (
                (query_hbm.at[:, near], query_w.at[:, near]),
                (key_hbm.at[:, near], key_w.at[:, near]),
                (value_hbm.at[:, near], value_w.at[:, near]),
                (pool_in_hbm, pool_in_w),
                (pool_out_hbm, pool_out_w),
                (contrast_hbm, contrast_w),
                (pool_weight_hbm, pool_weight),
                (balance_hbm, balance),
                (gain_hbm, gain),
            )
        )
    ]

    barrier = pltpu.get_barrier_semaphore()

    def greet(target):
        pl.semaphore_signal(barrier, inc=1, device_id=target, device_id_type=MESH)

    place = (side * members + member) * 2 + tp
    for d in range(1, 2 * half_count):
        goal = lax.rem(place + d, 2 * half_count)
        greet((upper * half_count + lax.div(goal, 2), lax.rem(goal, 2)))

    @pl.when(crosses)
    def _():
        greet((sp + members, tp))

    @pl.when(relays)
    def _():
        greet((sp - members, tp))

    @pl.when(sp == half_count - 1)
    def _():
        greet((sp + 1, tp))

    @pl.when(sp == half_count)
    def _():
        greet((sp - 1, tp))

    for load in loads[:3]:
        load.start()

    @pl.when(relays)
    def _():
        for load in far_loads:
            load.start()

    for load in loads[3:]:
        load.start()

    extra = jnp.where(jnp.logical_or(crosses, relays), 1, 0)
    extra = extra + jnp.where(jnp.logical_or(sp == half_count - 1, sp == half_count), 1, 0)
    pl.semaphore_wait(barrier, 2 * half_count - 1 + extra)

    def cut(ch):
        return pl.ds(ch * piece, piece)

    pair_first = pltpu.make_async_remote_copy(
        src_ref=x_ref,
        dst_ref=rows_in.at[0, tp],
        send_sem=pair_send.at[0, 0],
        recv_sem=pair_recv.at[0, 0],
        device_id=(sp, other),
        device_id_type=MESH,
    )

    def pair_copy(step, ch):
        return pltpu.make_async_remote_copy(
            src_ref=rows_in.at[step, tp, cut(ch)],
            dst_ref=rows_in.at[step, tp, cut(ch)],
            send_sem=pair_send.at[step, ch],
            recv_sem=pair_recv.at[step, ch],
            device_id=(sp, other),
            device_id_type=MESH,
        )

    def relay_copy(src, step, ch, target):
        return pltpu.make_async_remote_copy(
            src_ref=src.at[cut(ch)],
            dst_ref=rows_in.at[step, tp, cut(ch)],
            send_sem=relay_send.at[step, ch],
            recv_sem=relay_recv.at[step, ch],
            device_id=(target, tp),
            device_id_type=MESH,
        )

    def swap(ch):
        return relay_copy(x_ref, 1, ch, sp + members * (1 - 2 * side))

    def own_up(ch):
        return relay_copy(x_ref, 2, ch, sp + members)

    def low_up(ch):
        return relay_copy(rows_in.at[1, tp], 3, ch, sp + members)

    def top(step):
        return side == (1 if step == 0 else 0)

    def kv_copy(step, j, ch):
        goal = 2 * tp + j
        first = jnp.where(top(step), 1, along)
        return pltpu.make_async_remote_copy(
            src_ref=kv_stage.at[step, j, :, cut(ch)],
            dst_ref=kv.at[step, member, :, cut(ch)],
            send_sem=kv_send.at[step, j, ch],
            recv_sem=kv_recv.at[step, member, ch],
            device_id=(plane * members + goal, first),
            device_id_type=MESH,
        )

    def forward_copy(step, source, ch):
        return pltpu.make_async_remote_copy(
            src_ref=kv.at[step, source, :, cut(ch)],
            dst_ref=kv.at[step, source, :, cut(ch)],
            send_sem=forward_send.at[step, source, ch],
            recv_sem=kv_recv.at[step, source, ch],
            device_id=(sp, other),
            device_id_type=MESH,
        )

    def query_copy(step, j, ch):
        core = jnp.where(top(step), 1, 0)
        return pltpu.make_async_remote_copy(
            src_ref=query_stage.at[step, j, :, cut(ch)],
            dst_ref=queries.at[member, :, cut(ch)],
            send_sem=query_send.at[step, j, ch],
            recv_sem=query_recv.at[member, ch],
            device_id=(plane * members + 2 * tp + j, core),
            device_id_type=MESH,
        )

    own_goal = across == tp

    def far_copy(step, ch, goal_side, j):
        slot = goal_side * 2 + j
        goal = (2 * upper + goal_side) * members + 2 * tp + j
        return pltpu.make_async_remote_copy(
            src_ref=far_stage.at[step - 2, slot, ch],
            dst_ref=kv.at[step, member, ch],
            send_sem=far_send.at[step - 2, slot, ch],
            recv_sem=far_recv.at[step - 2, member, ch],
            device_id=(goal, along),
            device_id_type=MESH,
        )

    def far_pass(step, source, ch):
        return pltpu.make_async_remote_copy(
            src_ref=kv.at[step, source, ch],
            dst_ref=kv.at[step, source, ch],
            send_sem=far_forward.at[step - 2, source, ch],
            recv_sem=far_recv.at[step - 2, source, ch],
            device_id=(sp, other),
            device_id_type=MESH,
        )

    def far_stays(goal_side, j):
        return jnp.logical_and(goal_side == side, jnp.logical_and(own_goal, j == along))

    def far_here(source):
        return jnp.logical_and(relays, source == member)

    def far_passes(source):
        return jnp.logical_and(source % 2 == tp, jnp.logical_not(far_here(source)))

    def far_awaits(source):
        return jnp.logical_not(jnp.logical_and(far_here(source), own_goal))

    def own_stays(step, j):
        return jnp.logical_and(own_goal, j == along)

    def query_stays(step, j):
        return jnp.logical_and(own_stays(step, j), jnp.where(top(step), 1, 0) == tp)

    def own_forwards(step):
        return jnp.logical_and(
            own_goal, jnp.logical_or(jnp.logical_not(top(step)), tp == 0)
        )

    def passes_on(step, source):
        mine = jnp.logical_and(source % 2 == tp, jnp.logical_not(top(step)))
        return jnp.logical_and(source != member, mine)

    def awaits(step, source):
        needed = jnp.logical_or(tp == 1, jnp.logical_not(top(step)))
        made_here = jnp.logical_and(source == member, own_goal)
        return jnp.logical_and(needed, jnp.logical_not(made_here))

    def contrast_stays(i):
        return jnp.logical_and(
            jnp.logical_and(query_band == plane, i == member), across == tp
        )

    head_here = 2 * side + along

    def contrast_copy(i):
        return pltpu.make_async_remote_copy(
            src_ref=contrast_stage.at[i],
            dst_ref=contrasts.at[head_here],
            send_sem=contrast_send.at[i],
            recv_sem=contrast_recv.at[head_here],
            device_id=(query_band * members + i, across),
            device_id_type=MESH,
        )

    def contrast_incoming(head):
        return pltpu.make_async_remote_copy(
            src_ref=contrast_stage.at[0],
            dst_ref=contrasts.at[head],
            send_sem=contrast_send.at[0],
            recv_sem=contrast_recv.at[head],
            device_id=(sp, other),
            device_id_type=MESH,
        )

    def contrast_local(head):
        same = jnp.logical_and(head // 2 == side, 2 * tp + head % 2 == member)
        return jnp.logical_and(same, side == tp)

    rim_copy = pltpu.make_async_remote_copy(
        src_ref=rim_stage,
        dst_ref=rim,
        send_sem=rim_send,
        recv_sem=rim_recv,
        device_id=(lax.rem(sp + 1, sp_count), tp),
        device_id_type=MESH,
    )

    def out_copy(start):
        span = slice(start, start + chunk)
        return pltpu.make_async_remote_copy(
            src_ref=out_stage.at[:, span],
            dst_ref=out_recv.at[:, span],
            send_sem=out_send.at[start // chunk],
            recv_sem=out_recv_sem.at[start // chunk],
            device_id=(sp, other),
            device_id_type=MESH,
        )


    keep.wait()
    pair_first.start()
    for ch in range(chunks):
        swap(ch).start()

        @pl.when(crosses)
        def _(ch=ch):
            own_up(ch).start()

    peaks[...] = jnp.full(peaks.shape, -1e30, f32)
    totals[...] = jnp.zeros(totals.shape, f32)
    weighted[...] = jnp.zeros(weighted.shape, f32)

    def project(step, pieces):
        here = cut(pieces[0]) if len(pieces) == 1 else slice(None)

        def one(t, carry):
            j = jnp.where(t == 0, 1 - along, along)
            columns = pl.ds(pl.multiple_of((2 * side + j) * width, width), width)
            x = rows_in[step, :, here, :].reshape(-1, model)

            def through(held):
                dot = jnp.dot(x, held[:, columns], preferred_element_type=f32)
                return dot.astype(bf16).reshape(2, -1, width)

            mine = through(query_w)
            keys = through(key_w)
            values = through(value_w)
            kept = query_stays(step, j)
            stays = own_stays(step, j)

            @pl.when(jnp.logical_not(kept))
            def _():
                query_stage[step, j, :, here] = mine
                for ch in pieces:
                    query_copy(step, j, ch).start()

            @pl.when(kept)
            def _():
                queries[member, :, here] = mine

            @pl.when(jnp.logical_not(stays))
            def _():
                kv_stage[step, j, :, here, :width] = keys
                kv_stage[step, j, :, here, width:] = values
                for ch in pieces:
                    kv_copy(step, j, ch).start()

            @pl.when(stays)
            def _():
                kv[step, member, :, here, :width] = keys
                kv[step, member, :, here, width:] = values

                @pl.when(own_forwards(step))
                def _():
                    for ch in pieces:
                        forward_copy(step, member, ch).start()

            return carry

        lax.fori_loop(0, 2, one, 0)

    def project_far(step, ch):
        pair_copy(step, ch).wait_recv()

        def one(t, carry):
            goal_side = 1 - lax.div(t, 2)
            j = jnp.where(lax.rem(t, 2) == 0, 1 - along, along)
            columns = pl.ds(pl.multiple_of((2 * goal_side + j) * width, width), width)
            x = rows_in[step, :, cut(ch), :].reshape(half, model)
            keys = jnp.dot(x, key_w[:, columns], preferred_element_type=f32).astype(bf16)
            values = jnp.dot(x, value_w[:, columns], preferred_element_type=f32).astype(bf16)
            stays = far_stays(goal_side, j)

            @pl.when(jnp.logical_not(stays))
            def _():
                far_stage[step - 2, goal_side * 2 + j, ch, :, :width] = keys
                far_stage[step - 2, goal_side * 2 + j, ch, :, width:] = values
                far_copy(step, ch, goal_side, j).start()

            @pl.when(stays)
            def _():
                kv[step, member, ch, :, :width] = keys
                kv[step, member, ch, :, width:] = values
                far_pass(step, member, ch).start()

            return carry

        lax.fori_loop(0, 4, one, 0)

    def take_swap(ch):
        swap(ch).wait_recv()

        @pl.when(crosses)
        def _():
            low_up(ch).start()

        pair_copy(1, ch).start()

    def take_far(step, ch):
        (own_up(ch) if step == 2 else low_up(ch)).wait_recv()
        pair_copy(step, ch).start()

    def project_swap(ch):
        pair_copy(1, ch).wait_recv()
        project(1, (ch,))

    log_scale = head_dim ** (-0.5) * math.log2(math.e)

    def attend_block(step, i, seen, masked):
        for u in range(2):
            cols = slice(u * head_dim, (u + 1) * head_dim)
            keys = kv[step, :seen, :, :, cols].reshape(-1, head_dim)
            values = kv[step, :seen, :, :, width:].reshape(-1, width)
            scores = lax.dot_general(
                queries[i, :, :, cols].reshape(rows, head_dim), keys, (((1,), (1,)), ((), ())), preferred_element_type=f32
            )
            if masked:
                query_order = lax.broadcasted_iota(jnp.int32, scores.shape, 0) + (seen - 1) * rows
                key_order = lax.broadcasted_iota(jnp.int32, scores.shape, 1)
                scores = jnp.where(key_order <= query_order, scores, -jnp.inf)
            old = peaks[u, i][:, :1]
            peak = jnp.maximum(jnp.max(scores, axis=1, keepdims=True), old)
            shrink = jnp.exp2((old - peak) * log_scale)
            raised = jnp.exp2((scores - peak) * log_scale)
            total = jnp.sum(raised, axis=1, keepdims=True)
            update = jnp.dot(raised.astype(bf16), values, preferred_element_type=f32)
            total = total + totals[u, i][:, :1] * shrink
            update = update + weighted[u, i] * shrink
            peaks[u, i] = jnp.broadcast_to(peak, peaks.shape[2:])
            totals[u, i] = jnp.broadcast_to(total, totals.shape[2:])
            weighted[u, i] = update

    def finished_block(i):
        first = (weighted[0, i] * (1.0 / totals[0, i][:, :1])).astype(bf16).astype(f32)
        second = (weighted[1, i] * (1.0 / totals[1, i][:, :1])).astype(bf16).astype(f32)
        contrast = first - balance[across * members + head_here] * second
        mean_square = jnp.mean(contrast * contrast, axis=1, keepdims=True)
        return (contrast * lax.rsqrt(mean_square + norm_epsilon) * gain[...]).astype(bf16)

    def send_block(i, result):
        stays = contrast_stays(i)

        @pl.when(jnp.logical_not(stays))
        def _():
            contrast_stage[i] = result
            contrast_copy(i).start()

        @pl.when(stays)
        def _():
            contrasts[head_here] = result

    def turn(t):
        return lax.rem(member + 1 + t, members)

    def block_pairs(work):
        def one(t, carry):
            work(turn(2 * t), turn(2 * t + 1))
            return carry

        lax.fori_loop(0, members // 2, one, 0)

    def finish_pair(i, k):
        results = finished_block(i), finished_block(k)
        send_block(i, results[0])
        send_block(k, results[1])

    def lands_here(step, source):
        return jnp.logical_and(
            source != member, jnp.where(top(step), 1, source % 2) == tp
        )

    def pass_on(step):
        for ch in range(chunks):
            for source in range(members):

                @pl.when(lands_here(step, source))
                def _(source=source, ch=ch):
                    forward_copy(step, source, ch).wait_recv()

                @pl.when(passes_on(step, source))
                def _(source=source, ch=ch):
                    forward_copy(step, source, ch).start()

    def arrive(step):
        for ch in range(chunks):
            for source in range(members):
                passed = jnp.logical_not(lands_here(step, source))

                @pl.when(jnp.logical_and(awaits(step, source), passed))
                def _(source=source, ch=ch):
                    forward_copy(step, source, ch).wait_recv()

    def attend(step, between):
        band = bands_of[step]

        @pl.when(band == query_band)
        def _():
            for i in range(members):
                if i == members // 2:
                    between()
                attend_block(step, i, i + 1, True)

        @pl.when(band < query_band)
        def _():
            def one(t, carry):
                attend_block(step, turn(2 * t), members, False)
                attend_block(step, turn(2 * t + 1), members, False)

                @pl.when(t == 0)
                def _():
                    between()

                return carry

            lax.fori_loop(0, members // 2, one, 0)

        @pl.when(band > query_band)
        def _():
            between()

    def far_pass_on(step, ch):
        for source in range(members):

            @pl.when(far_passes(source))
            def _(source=source):
                far_pass(step, source, ch).wait_recv()
                far_pass(step, source, ch).start()

    def far_arrive(step, ch):
        for source in range(members):
            passed = jnp.logical_not(far_passes(source))

            @pl.when(jnp.logical_and(far_awaits(source), passed))
            def _(source=source):
                far_pass(step, source, ch).wait_recv()

    loads[0].wait()
    loads[1].wait()
    loads[2].wait()
    pair_first.wait_recv()
    project(0, tuple(range(chunks)))

    loads[3].wait()
    pool_input = jnp.dot(
        rows_in[0].reshape(rows, model), pool_in_w[...], preferred_element_type=f32
    ).astype(bf16)
    rim_stage[...] = pool_input[rows - rim.shape[0] :]

    @pl.when(sp + 1 < sp_count)
    def _():
        rim_copy.start()

    take_swap(0)

    @pl.when(relays)
    def _():
        take_far(2, 0)

    project_swap(0)

    @pl.when(relays)
    def _():
        for load in far_loads:
            load.wait()
        project_far(2, 0)

    take_swap(1)

    @pl.when(relays)
    def _():
        take_far(2, 1)

    project_swap(1)

    @pl.when(relays)
    def _():
        project_far(2, 1)
        take_far(3, 0)

    pass_on(0)

    @pl.when(relays)
    def _():
        project_far(3, 0)

    def query_incoming(source, ch):
        return pltpu.make_async_remote_copy(
            src_ref=query_stage.at[0, 0, :, cut(ch)],
            dst_ref=queries.at[source, :, cut(ch)],
            send_sem=query_send.at[0, 0, ch],
            recv_sem=query_recv.at[source, ch],
            device_id=(sp, other),
            device_id_type=MESH,
        )

    def take_queries():
        for source in range(members):

            @pl.when(jnp.logical_not(jnp.logical_and(source == member, own_goal)))
            def _(source=source):
                for ch in range(chunks):
                    query_incoming(source, ch).wait_recv()

    idle_first = jnp.logical_and(in_upper, jnp.logical_and(side == 1, tp == 0))

    @pl.when(idle_first)
    def _():
        far_pass_on(2, 0)
        far_pass_on(2, 1)

    @pl.when(jnp.logical_and(relays, tp == 1))
    def _():
        take_far(3, 1)

    take_queries()
    arrive(0)

    def last_rows():
        @pl.when(jnp.logical_and(relays, tp == 0))
        def _():
            take_far(3, 1)

        @pl.when(jnp.logical_and(relays, tp == 1))
        def _():
            project_far(3, 1)

    attend(0, last_rows)

    @pl.when(jnp.logical_and(relays, tp == 0))
    def _():
        project_far(3, 1)

    def last_passes():
        @pl.when(jnp.logical_and(in_upper, jnp.logical_and(side == 1, tp == 1)))
        def _():
            far_pass_on(3, 1)

    def attend_swapped():
        pass_on(1)

        @pl.when(jnp.logical_and(in_upper, side == 1))
        def _():
            far_pass_on(3, 0)

        arrive(1)
        attend(1, last_passes)

    @pl.when(in_upper)
    def _():
        @pl.when(jnp.logical_not(idle_first))
        def _():
            far_pass_on(2, 0)
            far_pass_on(2, 1)

        @pl.when(relays)
        def _():
            attend_swapped()
            far_pass_on(3, 0)

        far_arrive(2, 0)
        far_arrive(2, 1)

        def one(t, carry):
            attend_block(2, turn(2 * t), members, False)
            attend_block(2, turn(2 * t + 1), members, False)

            @pl.when(jnp.logical_and(t == 0, jnp.logical_and(relays, tp == 1)))
            def _():
                far_pass_on(3, 1)

            return carry

        lax.fori_loop(0, members // 2, one, 0)

    @pl.when(jnp.logical_not(relays))
    def _():
        attend_swapped()

    for load in loads[6:]:
        load.wait()

    @pl.when(in_lower)
    def _():
        block_pairs(finish_pair)

    @pl.when(in_upper)
    def _():
        @pl.when(tp == 0)
        def _():
            far_pass_on(3, 1)

        far_arrive(3, 0)
        far_arrive(3, 1)

        def last_pair(i, k):
            attend_block(3, i, members, False)
            attend_block(3, k, members, False)
            finish_pair(i, k)

        block_pairs(last_pair)

    @pl.when(sp > 0)
    def _():
        rim_copy.wait_recv()

    @pl.when(sp == 0)
    def _():
        rim[...] = jnp.zeros_like(rim)

    loads[4].wait()
    extended = jnp.concatenate([rim[...], pool_input], axis=0).astype(f32)
    group_width = pool_weight.shape[1]
    skirt = rim.shape[0]
    position = sp * rows + lax.broadcasted_iota(jnp.int32, (rows, group_width), 0)
    mixed = []
    for group in range(pool_weight.shape[0]):
        block = extended[:, group * group_width : (group + 1) * group_width]
        window = block
        reach = 1
        span = 2 ** (1 + group % 4)
        while reach < span:
            window = window + pltpu.roll(window, reach, 0)
            reach *= 2
        counts = jnp.minimum(position + 1, span).astype(f32)
        spread = (window[skirt:] / counts - block[skirt:]).astype(bf16)
        mixed.append(
            jnp.dot(spread, pool_weight[group], preferred_element_type=f32).astype(bf16)
        )
    pool_out = jnp.concatenate(mixed, axis=1)
    for start in range(0, model, chunk):
        pool_part[:, start : start + chunk] = jnp.dot(
            pool_out, pool_out_w[:, start : start + chunk], preferred_element_type=f32
        )

    pair_first.wait_send()
    for ch in range(chunks):
        swap(ch).wait_send()
        pair_copy(1, ch).wait_send()

        @pl.when(crosses)
        def _(ch=ch):
            own_up(ch).wait_send()
            low_up(ch).wait_send()

        @pl.when(relays)
        def _(ch=ch):
            for step in range(2, 4):
                pair_copy(step, ch).wait_send()
                for slot in range(4):

                    @pl.when(jnp.logical_not(far_stays(slot // 2, slot % 2)))
                    def _(step=step, slot=slot):
                        far_copy(step, ch, slot // 2, slot % 2).wait_send()

                @pl.when(own_goal)
                def _(step=step):
                    far_pass(step, member, ch).wait_send()

        @pl.when(in_upper)
        def _(ch=ch):
            for step in range(2, 4):
                for source in range(members):

                    @pl.when(far_passes(source))
                    def _(step=step, source=source):
                        far_pass(step, source, ch).wait_send()

    def drain(step, ch):
        for j in range(2):

            @pl.when(jnp.logical_not(own_stays(step, j)))
            def _(j=j):
                kv_copy(step, j, ch).wait_send()

            @pl.when(jnp.logical_not(query_stays(step, j)))
            def _(j=j):
                query_copy(step, j, ch).wait_send()

        @pl.when(own_forwards(step))
        def _():
            forward_copy(step, member, ch).wait_send()

        for source in range(members):

            @pl.when(passes_on(step, source))
            def _(source=source):
                forward_copy(step, source, ch).wait_send()

    for ch in range(chunks):
        drain(0, ch)
        drain(1, ch)

    @pl.when(sp + 1 < sp_count)
    def _():
        rim_copy.wait_send()

    loads[5].wait()
    def pair_of_heads(plane_side):
        heads = (2 * plane_side, 2 * plane_side + 1)
        for head in heads:

            @pl.when(jnp.logical_not(contrast_local(head)))
            def _(head=head):
                contrast_incoming(head).wait_recv()

        left = jnp.concatenate([contrasts[head] for head in heads], axis=1)
        taken = pl.ds(pl.multiple_of(plane_side * 2 * width, 2 * width), 2 * width)

        def product(span):
            part = jnp.dot(left, contrast_w[taken, span], preferred_element_type=f32)
            return part + pool_part[:, span]

        return product

    spans = [slice(start, start + chunk) for start in range(0, model, chunk)]
    product = pair_of_heads(side)
    for span in spans:
        pool_part[:, span] = product(span)

    product = pair_of_heads(1 - side)
    for span in spans:
        part = product(span)
        low, high = part[:half], part[half:]
        out_stage[:, span] = jnp.where(tp == 0, high, low).astype(bf16)
        out_copy(span.start).start()
        out_ref[:, span] = jnp.where(tp == 0, low, high).astype(bf16)

    for start in range(0, model, chunk):
        out_copy(start).wait()

    for i in range(members):

        @pl.when(jnp.logical_not(contrast_stays(i)))
        def _(i=i):
            contrast_copy(i).wait_send()


def kernel_scratch(members, half, model, width, pool_cols, heads, groups_here):
    bf16 = jnp.bfloat16
    rows = 2 * half
    group_width = pool_cols // groups_here
    dma = pltpu.SemaphoreType.DMA
    return [
        pltpu.VMEM((groups_here, group_width, group_width), bf16),
        pltpu.SMEM((heads,), jnp.float32),
        pltpu.VMEM((1, width), jnp.float32),
        pltpu.VMEM((model, members * width), bf16),
        pltpu.VMEM((model, members * width), bf16),
        pltpu.VMEM((model, members * width), bf16),
        pltpu.VMEM((model, pool_cols), bf16),
        pltpu.VMEM((members * width, model), bf16),
        pltpu.VMEM((pool_cols, model), bf16),
        pltpu.VMEM((4, 2, half, model), bf16),
        pltpu.VMEM((4, members, 2, half, 2 * width), bf16),
        pltpu.VMEM((2, 2, 2, half, 2 * width), bf16),
        pltpu.VMEM((2, 4, 2, half, 2 * width), bf16),
        pltpu.VMEM((members, 2, half, width), bf16),
        pltpu.VMEM((2, 2, 2, half, width), bf16),
        pltpu.VMEM((2, members, rows, 128), jnp.float32),
        pltpu.VMEM((2, members, rows, 128), jnp.float32),
        pltpu.VMEM((2, members, rows, width), jnp.float32),
        pltpu.VMEM((members, rows, width), bf16),
        pltpu.VMEM((members, rows, width), bf16),
        pltpu.VMEM((reach_back + 1, pool_cols), bf16),
        pltpu.VMEM((reach_back + 1, pool_cols), bf16),
        pltpu.VMEM((rows, model), jnp.float32),
        pltpu.VMEM((half, model), bf16),
        dma((11,)),
        dma,
        dma((4, 2)),
        dma((4, 2)),
        dma((4, 2)),
        dma((4, 2)),
        dma((2, 2, 2)),
        dma((2, members, 2)),
        dma((2, members, 2)),
        dma((2, 4, 2)),
        dma((2, members, 2)),
        dma((2, members, 2)),
        dma((2, 2, 2)),
        dma((members, 2)),
        dma((members,)),
        dma((members,)),
        dma,
        dma,
        dma((model // math.gcd(model, 512),)),
        dma((model // math.gcd(model, 512),)),
    ]


vmem_most = 67043328
kernel_grant = 54 * 2**20


def scratch_bytes(scratch):
    return sum(
        math.prod(item.shape) * jnp.dtype(item.dtype).itemsize
        for item in scratch
        if getattr(item, "memory_space", None) == pltpu.VMEM
    )


def whole_layer(
    normed,
    query_weight,
    key_weight,
    value_weight,
    pool_in_weight,
    pool_weight,
    map_balance,
    head_gain,
    contrast_out_weight,
    pool_out_weight,
):
    sp_count = lax.axis_size("sp")
    width = head_gain.shape[0]
    members = query_weight.shape[1] // width
    half, model = normed.shape
    pool_cols = pool_in_weight.shape[1]
    groups_here = pool_weight.shape[0]
    heads = map_balance.shape[0]
    scratch = kernel_scratch(
        max(members, 1), half, model, width, pool_cols, heads, groups_here
    )
    fits = (
        lax.axis_size("tp") == 2
        and members == 4
        and sp_count == 4 * members
        and groups_here % 4 == 0
        and scratch_bytes(scratch) < vmem_most * 3 // 4
    )
    if not fits:
        return per_device(
            normed,
            query_weight,
            key_weight,
            value_weight,
            pool_in_weight,
            pool_weight,
            map_balance,
            head_gain,
            contrast_out_weight,
            pool_out_weight,
        )
    vmem = pl.BlockSpec(memory_space=pltpu.VMEM)
    hbm = pl.BlockSpec(memory_space=pltpu.HBM)
    own_part, partner_part = pl.pallas_call(
        functools.partial(layer_kernel, sp_count, members),
        out_shape=[pltpu.VMEM((half, model), jnp.bfloat16)] * 2,
        in_specs=[hbm] * 10,
        out_specs=[vmem, vmem],
        scratch_shapes=scratch,
        compiler_params=pltpu.CompilerParams(
            collective_id=0, has_side_effects=True, vmem_limit_bytes=kernel_grant
        ),
    )(
        normed,
        pool_weight,
        map_balance,
        head_gain.reshape(1, width),
        query_weight,
        key_weight,
        value_weight,
        pool_in_weight,
        contrast_out_weight,
        pool_out_weight,
    )
    return (own_part.astype(jnp.float32) + partner_part.astype(jnp.float32)).astype(jnp.bfloat16)


def solution(mesh):
    return jax.shard_map(
        whole_layer,
        mesh=mesh,
        in_specs=(
            P(("sp", "tp"), None),
            P(None, "tp"),
            P(None, "tp"),
            P(None, "tp"),
            P(None, "tp"),
            P("tp", None, None),
            P(),
            P(),
            P("tp", None),
            P("tp", None),
        ),
        out_specs=P(("sp", "tp"), None),
        check_vma=False,
    )
```

```python
import functools
import math

import jax
import jax.numpy as jnp
from jax import lax
from jax.experimental import pallas as pl
from jax.experimental.pallas import tpu as pltpu
from jax.sharding import PartitionSpec as P

reach_back = 15
norm_epsilon = 1e-06


def passed_along(block, axis, distance):
    devices = range(lax.axis_size(axis))
    route = [(i - distance, i) for i in devices if i - distance in devices]
    return lax.ppermute(block, axis, route)


def from_partner(block, axis, stride):
    count = lax.axis_size(axis)
    route = []
    for low in range(count):
        high = low | 1 << stride
        if high != low and high < count:
            route += [(low, high), (high, low)]
    return lax.ppermute(block, axis, route)


def shifted(array, axis, by):
    size = lax.axis_size(axis)
    return lax.ppermute(array, axis, [(i, (i + by) % size) for i in range(size)])


def as_sent(array):

    def short(part):
        return part.astype(jnp.bfloat16) if part.dtype == jnp.float32 else part

    return jax.tree.map(short, array)


def attend(running, queries, key_rows, value_rows, query_first, key_first, score_scale):
    key_count = key_rows.shape[0]
    key_block = math.gcd(key_count, 1024)
    unit_count = queries.shape[1]
    heads_here = value_rows.shape[1]
    per_head = unit_count // heads_here
    query_count = queries.shape[0]
    query_order = query_first + lax.iota(jnp.int32, query_count)

    def key_step(block_index, carried):
        block_start = block_index * key_block

        def block_work(current):
            row_peak, row_total, weighted = current
            scores = (
                jnp.einsum("qud,kud->uqk", queries, key_rows, preferred_element_type=jnp.float32)
                * score_scale
            )
            key_order = key_first + block_start + lax.iota(jnp.int32, key_block)
            scores = jnp.where(
                key_order[None, None, :] <= query_order[None, :, None], scores, -jnp.inf
            )
            new_peak = jnp.maximum(row_peak, jnp.max(scores, axis=2))
            shrink = jnp.exp(row_peak - new_peak)
            raised = jnp.exp(scores - new_peak[:, :, None])
            row_total = row_total * shrink + jnp.sum(raised, axis=2)
            map_weights = raised.astype(jnp.bfloat16).reshape(
                heads_here, per_head, query_count, key_block
            )
            update = jnp.einsum(
                "hmqk,khe->hmqe", map_weights, value_rows, preferred_element_type=jnp.float32
            )
            weighted = weighted * shrink[:, :, None] + update.reshape(unit_count, query_count, -1)
            return (new_peak, row_total, weighted)

        def keep_state(current):
            return current

        return lax.cond(
            key_first + block_start <= query_first + query_count - 1,
            block_work,
            keep_state,
            carried,
        )

    return lax.fori_loop(0, key_count // key_block, key_step, running)


def fresh_state(unit_count, row_count, value_width):
    return (
        jnp.full((unit_count, row_count), -1e30, jnp.float32),
        jnp.zeros((unit_count, row_count), jnp.float32),
        jnp.zeros((unit_count, row_count, value_width), jnp.float32),
    )


def finished(running):
    row_peak, row_total, weighted = running
    return (weighted / row_total[:, :, None]).astype(jnp.bfloat16)


def joined_state(first, second):
    first_peak, first_total, first_weighted = first
    second_peak, second_total, second_weighted = second
    new_peak = jnp.maximum(first_peak, second_peak)
    first_shrink = jnp.exp(first_peak - new_peak)
    second_shrink = jnp.exp(second_peak - new_peak)
    new_total = first_total * first_shrink + second_total * second_shrink
    new_weighted = (
        first_weighted * first_shrink[:, :, None] + second_weighted * second_shrink[:, :, None]
    )
    return (new_peak, new_total, new_weighted)


def per_device(
    normed,
    query_weight,
    key_weight,
    value_weight,
    pool_in_weight,
    pool_weight,
    map_balance,
    head_gain,
    contrast_out_weight,
    pool_out_weight,
):
    tp_index = lax.axis_index("tp")
    sp_count = lax.axis_size("sp")
    sp_index = lax.axis_index("sp")
    head_dim = head_gain.shape[0] // 2
    value_width = 2 * head_dim
    query_cols = query_weight.shape[1]
    value_cols = value_weight.shape[1]
    unit_count = query_cols // head_dim
    heads_here = unit_count // 2
    project_incoming = lax.all_gather(normed, "tp", axis=0, tiled=True)
    products = [
        jnp.dot(project_incoming, weight_part, preferred_element_type=jnp.float32)
        for weight_part in (query_weight, key_weight, value_weight, pool_in_weight)
    ]
    joined = jnp.concatenate(products, axis=1).astype(jnp.bfloat16)
    row_count = joined.shape[0]
    queries = joined[:, :query_cols].reshape(row_count, unit_count, head_dim)
    key_rows = joined[:, query_cols : 2 * query_cols].reshape(row_count, unit_count, head_dim)
    value_rows = joined[:, 2 * query_cols : 2 * query_cols + value_cols].reshape(
        row_count, heads_here, value_width
    )
    pool_input = joined[:, 2 * query_cols + value_cols :]
    pool_cols = pool_input.shape[1]
    upper_rim = passed_along(pool_input[row_count - reach_back :], "sp", 1)
    extended = jnp.concatenate([upper_rim, pool_input], axis=0).astype(jnp.float32)
    groups_here = pool_weight.shape[0]
    group_width = pool_weight.shape[1]
    group_index = tp_index * groups_here + lax.iota(jnp.int32, pool_cols) // group_width
    widths = jnp.left_shift(jnp.int32(2), group_index % 4)
    window_sum = jnp.zeros((row_count, pool_cols), jnp.float32)
    for offset in range(reach_back + 1):
        window_sum = window_sum + extended[
            reach_back - offset : reach_back - offset + row_count
        ] * (offset < widths)[None, :].astype(jnp.float32)
    position = sp_index * row_count + lax.iota(jnp.int32, row_count)
    counts = jnp.minimum(position[:, None] + 1, widths[None, :]).astype(jnp.float32)
    spread = (window_sum / counts - extended[reach_back:]).astype(jnp.bfloat16)
    mixed_groups = jnp.einsum(
        "tgc,gce->tge",
        spread.reshape(row_count, groups_here, group_width),
        pool_weight,
        preferred_element_type=jnp.float32,
    )
    pool_out = mixed_groups.reshape(row_count, pool_cols).astype(jnp.bfloat16)
    score_scale = head_dim ** (-0.5)
    level_count = sp_count.bit_length() - 1
    low_levels = level_count // 2
    band_size = 1 << low_levels
    band_count = sp_count // band_size
    member = sp_index % band_size
    band = sp_index // band_size
    band_queries = queries
    for bit in range(low_levels):
        received = from_partner(band_queries, "sp", bit)
        upper = member >> bit & 1 == 1
        band_queries = jnp.where(
            upper,
            jnp.concatenate([received, band_queries], axis=0),
            jnp.concatenate([band_queries, received], axis=0),
        )
    band_first = band * band_size * row_count
    running = fresh_state(unit_count, band_size * row_count, value_width)
    for step in range(band_count):
        if step == 0:
            key_piece, value_piece = (key_rows, value_rows)
        else:
            key_piece, value_piece = shifted((key_rows, value_rows), "sp", step * band_size)
        source = (sp_index - step * band_size) % sp_count
        running = attend(
            running,
            band_queries,
            key_piece,
            value_piece,
            band_first,
            source * row_count,
            score_scale,
        )
    for bit in range(low_levels - 1, -1, -1):
        half = running[0].shape[1] // 2
        upper = member >> bit & 1 == 1
        lower_part = jax.tree.map(lambda item: item[:, :half], running)
        upper_part = jax.tree.map(lambda item: item[:, half:], running)
        outgoing = jax.tree.map(
            lambda low, high: jnp.where(upper, low, high), lower_part, upper_part
        )
        kept = jax.tree.map(lambda low, high: jnp.where(upper, high, low), lower_part, upper_part)
        incoming = from_partner(
            (as_sent(outgoing[0]), as_sent(outgoing[1]), as_sent(outgoing[2])), "sp", bit
        )
        running = joined_state(kept, incoming)
    maps = finished(running)
    paired = maps.reshape(heads_here, 2, row_count, value_width)
    paired = lax.optimization_barrier(paired).astype(jnp.float32)
    head_first = tp_index * heads_here
    balance_here = lax.dynamic_slice_in_dim(map_balance, head_first, heads_here, 0)
    contrast = paired[:, 0] - balance_here[:, None, None] * paired[:, 1]
    mean_square = jnp.mean(contrast * contrast, axis=2, keepdims=True)
    contrast = contrast * lax.rsqrt(mean_square + norm_epsilon) * head_gain
    contrast_out = (
        contrast.astype(jnp.bfloat16)
        .transpose(1, 0, 2)
        .reshape(row_count, heads_here * value_width)
    )
    partial_value = jnp.dot(contrast_out, contrast_out_weight, preferred_element_type=jnp.float32)
    return lax.psum_scatter(
        (
            partial_value + jnp.dot(pool_out, pool_out_weight, preferred_element_type=jnp.float32)
        ).astype(jnp.bfloat16),
        "tp",
        scatter_dimension=0,
        tiled=True,
    )


MESH = pl.DeviceIdType.MESH


def layer_kernel(
    sp_count,
    members,
    x_hbm,
    pool_weight_hbm,
    balance_hbm,
    gain_hbm,
    query_hbm,
    key_hbm,
    value_hbm,
    pool_in_hbm,
    contrast_hbm,
    pool_out_hbm,
    out_ref,
    out_recv,
    pool_weight,
    balance,
    gain,
    query_w,
    key_w,
    value_w,
    pool_in_w,
    contrast_w,
    pool_out_w,
    rows_in,
    kv,
    kv_stage,
    far_stage,
    queries,
    query_stage,
    peaks,
    totals,
    weighted,
    contrasts,
    contrast_stage,
    rim,
    rim_stage,
    pool_part,
    out_stage,
    weight_sem,
    local_sem,
    pair_send,
    pair_recv,
    relay_send,
    relay_recv,
    kv_send,
    kv_recv,
    forward_send,
    far_send,
    far_recv,
    far_forward,
    query_send,
    query_recv,
    contrast_send,
    contrast_recv,
    rim_send,
    rim_recv,
    out_send,
    out_recv_sem,
):
    f32 = jnp.float32
    bf16 = jnp.bfloat16
    sp = lax.axis_index("sp")
    tp = lax.axis_index("tp")
    other = 1 - tp
    plane = lax.div(sp, members)
    member = lax.rem(sp, members)
    upper = lax.div(plane, 2)
    side = lax.rem(plane, 2)
    across = lax.div(member, 2)
    along = lax.rem(member, 2)
    half_count = 2 * members
    half, model = x_hbm.shape
    rows = 2 * half
    width = gain.shape[1]
    head_dim = width // 2
    chunk = math.gcd(model, 512)
    chunks = 2
    piece = half // chunks
    in_lower = upper == 0
    in_upper = upper == 1
    crosses = plane == 1
    relays = plane == 2
    query_band = 2 * upper + tp
    bands_of = (plane, plane + 1 - 2 * side)

    keep = pltpu.make_async_copy(x_hbm, rows_in.at[0, tp], local_sem)
    keep.start()
    x_ref = rows_in.at[0, tp]

    near = pl.ds(pl.multiple_of(side * 2 * width, 2 * width), 2 * width)
    far = pl.ds(pl.multiple_of((1 - side) * 2 * width, 2 * width), 2 * width)
    far_loads = [
        pltpu.make_async_copy(src.at[:, far], dst.at[:, far], weight_sem.at[9 + i])
        for i, (src, dst) in enumerate(((key_hbm, key_w), (value_hbm, value_w)))
    ]
    loads = [
        pltpu.make_async_copy(src, dst, weight_sem.at[i])
        for i, (src, dst) in enumerate(
            (
                (query_hbm.at[:, near], query_w.at[:, near]),
                (key_hbm.at[:, near], key_w.at[:, near]),
                (value_hbm.at[:, near], value_w.at[:, near]),
                (pool_in_hbm, pool_in_w),
                (pool_out_hbm, pool_out_w),
                (contrast_hbm, contrast_w),
                (pool_weight_hbm, pool_weight),
                (balance_hbm, balance),
                (gain_hbm, gain),
            )
        )
    ]

    barrier = pltpu.get_barrier_semaphore()

    def greet(target):
        pl.semaphore_signal(barrier, inc=1, device_id=target, device_id_type=MESH)

    place = (side * members + member) * 2 + tp
    for d in range(1, 2 * half_count):
        goal = lax.rem(place + d, 2 * half_count)
        greet((upper * half_count + lax.div(goal, 2), lax.rem(goal, 2)))

    @pl.when(crosses)
    def _():
        greet((sp + members, tp))

    @pl.when(relays)
    def _():
        greet((sp - members, tp))

    @pl.when(sp == half_count - 1)
    def _():
        greet((sp + 1, tp))

    @pl.when(sp == half_count)
    def _():
        greet((sp - 1, tp))

    for load in loads[:3]:
        load.start()

    @pl.when(relays)
    def _():
        for load in far_loads:
            load.start()

    for load in loads[3:]:
        load.start()

    extra = jnp.where(jnp.logical_or(crosses, relays), 1, 0)
    extra = extra + jnp.where(jnp.logical_or(sp == half_count - 1, sp == half_count), 1, 0)
    pl.semaphore_wait(barrier, 2 * half_count - 1 + extra)

    def cut(ch):
        return pl.ds(ch * piece, piece)

    pair_first = pltpu.make_async_remote_copy(
        src_ref=x_ref,
        dst_ref=rows_in.at[0, tp],
        send_sem=pair_send.at[0, 0],
        recv_sem=pair_recv.at[0, 0],
        device_id=(sp, other),
        device_id_type=MESH,
    )

    def pair_copy(step, ch):
        return pltpu.make_async_remote_copy(
            src_ref=rows_in.at[step, tp, cut(ch)],
            dst_ref=rows_in.at[step, tp, cut(ch)],
            send_sem=pair_send.at[step, ch],
            recv_sem=pair_recv.at[step, ch],
            device_id=(sp, other),
            device_id_type=MESH,
        )

    def relay_copy(src, step, ch, target):
        return pltpu.make_async_remote_copy(
            src_ref=src.at[cut(ch)],
            dst_ref=rows_in.at[step, tp, cut(ch)],
            send_sem=relay_send.at[step, ch],
            recv_sem=relay_recv.at[step, ch],
            device_id=(target, tp),
            device_id_type=MESH,
        )

    def swap(ch):
        return relay_copy(x_ref, 1, ch, sp + members * (1 - 2 * side))

    def own_up(ch):
        return relay_copy(x_ref, 2, ch, sp + members)

    def low_up(ch):
        return relay_copy(rows_in.at[1, tp], 3, ch, sp + members)

    def top(step):
        return side == (1 if step == 0 else 0)

    def kv_copy(step, j, ch):
        goal = 2 * tp + j
        first = jnp.where(top(step), 1, along)
        return pltpu.make_async_remote_copy(
            src_ref=kv_stage.at[step, j, :, cut(ch)],
            dst_ref=kv.at[step, member, :, cut(ch)],
            send_sem=kv_send.at[step, j, ch],
            recv_sem=kv_recv.at[step, member, ch],
            device_id=(plane * members + goal, first),
            device_id_type=MESH,
        )

    def forward_copy(step, source, ch):
        return pltpu.make_async_remote_copy(
            src_ref=kv.at[step, source, :, cut(ch)],
            dst_ref=kv.at[step, source, :, cut(ch)],
            send_sem=forward_send.at[step, source, ch],
            recv_sem=kv_recv.at[step, source, ch],
            device_id=(sp, other),
            device_id_type=MESH,
        )

    def query_copy(step, j, ch):
        core = jnp.where(top(step), 1, 0)
        return pltpu.make_async_remote_copy(
            src_ref=query_stage.at[step, j, :, cut(ch)],
            dst_ref=queries.at[member, :, cut(ch)],
            send_sem=query_send.at[step, j, ch],
            recv_sem=query_recv.at[member, ch],
            device_id=(plane * members + 2 * tp + j, core),
            device_id_type=MESH,
        )

    own_goal = across == tp

    def far_copy(step, ch, goal_side, j):
        slot = goal_side * 2 + j
        goal = (2 * upper + goal_side) * members + 2 * tp + j
        return pltpu.make_async_remote_copy(
            src_ref=far_stage.at[step - 2, slot, ch],
            dst_ref=kv.at[step, member, ch],
            send_sem=far_send.at[step - 2, slot, ch],
            recv_sem=far_recv.at[step - 2, member, ch],
            device_id=(goal, along),
            device_id_type=MESH,
        )

    def far_pass(step, source, ch):
        return pltpu.make_async_remote_copy(
            src_ref=kv.at[step, source, ch],
            dst_ref=kv.at[step, source, ch],
            send_sem=far_forward.at[step - 2, source, ch],
            recv_sem=far_recv.at[step - 2, source, ch],
            device_id=(sp, other),
            device_id_type=MESH,
        )

    def far_stays(goal_side, j):
        return jnp.logical_and(goal_side == side, jnp.logical_and(own_goal, j == along))

    def far_here(source):
        return jnp.logical_and(relays, source == member)

    def far_passes(source):
        return jnp.logical_and(source % 2 == tp, jnp.logical_not(far_here(source)))

    def far_awaits(source):
        return jnp.logical_not(jnp.logical_and(far_here(source), own_goal))

    def own_stays(step, j):
        return jnp.logical_and(own_goal, j == along)

    def query_stays(step, j):
        return jnp.logical_and(own_stays(step, j), jnp.where(top(step), 1, 0) == tp)

    def own_forwards(step):
        return jnp.logical_and(
            own_goal, jnp.logical_or(jnp.logical_not(top(step)), tp == 0)
        )

    def passes_on(step, source):
        mine = jnp.logical_and(source % 2 == tp, jnp.logical_not(top(step)))
        return jnp.logical_and(source != member, mine)

    def awaits(step, source):
        needed = jnp.logical_or(tp == 1, jnp.logical_not(top(step)))
        made_here = jnp.logical_and(source == member, own_goal)
        return jnp.logical_and(needed, jnp.logical_not(made_here))

    def contrast_stays(i):
        return jnp.logical_and(
            jnp.logical_and(query_band == plane, i == member), across == tp
        )

    head_here = 2 * side + along

    def contrast_copy(i):
        return pltpu.make_async_remote_copy(
            src_ref=contrast_stage.at[i],
            dst_ref=contrasts.at[head_here],
            send_sem=contrast_send.at[i],
            recv_sem=contrast_recv.at[head_here],
            device_id=(query_band * members + i, across),
            device_id_type=MESH,
        )

    def contrast_incoming(head):
        return pltpu.make_async_remote_copy(
            src_ref=contrast_stage.at[0],
            dst_ref=contrasts.at[head],
            send_sem=contrast_send.at[0],
            recv_sem=contrast_recv.at[head],
            device_id=(sp, other),
            device_id_type=MESH,
        )

    def contrast_local(head):
        same = jnp.logical_and(head // 2 == side, 2 * tp + head % 2 == member)
        return jnp.logical_and(same, side == tp)

    rim_copy = pltpu.make_async_remote_copy(
        src_ref=rim_stage,
        dst_ref=rim,
        send_sem=rim_send,
        recv_sem=rim_recv,
        device_id=(lax.rem(sp + 1, sp_count), tp),
        device_id_type=MESH,
    )

    def out_copy(start):
        span = slice(start, start + chunk)
        return pltpu.make_async_remote_copy(
            src_ref=out_stage.at[:, span],
            dst_ref=out_recv.at[:, span],
            send_sem=out_send.at[start // chunk],
            recv_sem=out_recv_sem.at[start // chunk],
            device_id=(sp, other),
            device_id_type=MESH,
        )


    keep.wait()
    pair_first.start()
    for ch in range(chunks):
        swap(ch).start()

        @pl.when(crosses)
        def _(ch=ch):
            own_up(ch).start()

    peaks[...] = jnp.full(peaks.shape, -1e30, f32)
    totals[...] = jnp.zeros(totals.shape, f32)
    weighted[...] = jnp.zeros(weighted.shape, f32)

    def project(step, pieces):
        here = cut(pieces[0]) if len(pieces) == 1 else slice(None)

        def one(t, carry):
            j = jnp.where(t == 0, 1 - along, along)
            columns = pl.ds(pl.multiple_of((2 * side + j) * width, width), width)
            x = rows_in[step, :, here, :].reshape(-1, model)

            def through(held):
                dot = jnp.dot(x, held[:, columns], preferred_element_type=f32)
                return dot.astype(bf16).reshape(2, -1, width)

            mine = through(query_w)
            keys = through(key_w)
            values = through(value_w)
            kept = query_stays(step, j)
            stays = own_stays(step, j)

            @pl.when(jnp.logical_not(kept))
            def _():
                query_stage[step, j, :, here] = mine
                for ch in pieces:
                    query_copy(step, j, ch).start()

            @pl.when(kept)
            def _():
                queries[member, :, here] = mine

            @pl.when(jnp.logical_not(stays))
            def _():
                kv_stage[step, j, :, here, :width] = keys
                kv_stage[step, j, :, here, width:] = values
                for ch in pieces:
                    kv_copy(step, j, ch).start()

            @pl.when(stays)
            def _():
                kv[step, member, :, here, :width] = keys
                kv[step, member, :, here, width:] = values

                @pl.when(own_forwards(step))
                def _():
                    for ch in pieces:
                        forward_copy(step, member, ch).start()

            return carry

        lax.fori_loop(0, 2, one, 0)

    def project_far(step, ch):
        pair_copy(step, ch).wait_recv()

        def one(t, carry):
            goal_side = 1 - lax.div(t, 2)
            j = jnp.where(lax.rem(t, 2) == 0, 1 - along, along)
            columns = pl.ds(pl.multiple_of((2 * goal_side + j) * width, width), width)
            x = rows_in[step, :, cut(ch), :].reshape(half, model)
            keys = jnp.dot(x, key_w[:, columns], preferred_element_type=f32).astype(bf16)
            values = jnp.dot(x, value_w[:, columns], preferred_element_type=f32).astype(bf16)
            stays = far_stays(goal_side, j)

            @pl.when(jnp.logical_not(stays))
            def _():
                far_stage[step - 2, goal_side * 2 + j, ch, :, :width] = keys
                far_stage[step - 2, goal_side * 2 + j, ch, :, width:] = values
                far_copy(step, ch, goal_side, j).start()

            @pl.when(stays)
            def _():
                kv[step, member, ch, :, :width] = keys
                kv[step, member, ch, :, width:] = values
                far_pass(step, member, ch).start()

            return carry

        lax.fori_loop(0, 4, one, 0)

    def take_swap(ch):
        swap(ch).wait_recv()

        @pl.when(crosses)
        def _():
            low_up(ch).start()

        pair_copy(1, ch).start()

    def take_far(step, ch):
        (own_up(ch) if step == 2 else low_up(ch)).wait_recv()
        pair_copy(step, ch).start()

    def project_swap(ch):
        pair_copy(1, ch).wait_recv()
        project(1, (ch,))

    log_scale = head_dim ** (-0.5) * math.log2(math.e)

    def attend_block(step, i, seen, masked):
        for u in range(2):
            cols = slice(u * head_dim, (u + 1) * head_dim)
            keys = kv[step, :seen, :, :, cols].reshape(-1, head_dim)
            values = kv[step, :seen, :, :, width:].reshape(-1, width)
            scores = lax.dot_general(
                queries[i, :, :, cols].reshape(rows, head_dim), keys, (((1,), (1,)), ((), ())), preferred_element_type=f32
            )
            if masked:
                query_order = lax.broadcasted_iota(jnp.int32, scores.shape, 0) + (seen - 1) * rows
                key_order = lax.broadcasted_iota(jnp.int32, scores.shape, 1)
                scores = jnp.where(key_order <= query_order, scores, -jnp.inf)
            old = peaks[u, i][:, :1]
            peak = jnp.maximum(jnp.max(scores, axis=1, keepdims=True), old)
            shrink = jnp.exp2((old - peak) * log_scale)
            raised = jnp.exp2((scores - peak) * log_scale)
            total = jnp.sum(raised, axis=1, keepdims=True)
            update = jnp.dot(raised.astype(bf16), values, preferred_element_type=f32)
            total = total + totals[u, i][:, :1] * shrink
            update = update + weighted[u, i] * shrink
            peaks[u, i] = jnp.broadcast_to(peak, peaks.shape[2:])
            totals[u, i] = jnp.broadcast_to(total, totals.shape[2:])
            weighted[u, i] = update

    def finished_block(i):
        first = (weighted[0, i] * (1.0 / totals[0, i][:, :1])).astype(bf16).astype(f32)
        second = (weighted[1, i] * (1.0 / totals[1, i][:, :1])).astype(bf16).astype(f32)
        contrast = first - balance[across * members + head_here] * second
        mean_square = jnp.mean(contrast * contrast, axis=1, keepdims=True)
        return (contrast * lax.rsqrt(mean_square + norm_epsilon) * gain[...]).astype(bf16)

    def send_block(i, result):
        stays = contrast_stays(i)

        @pl.when(jnp.logical_not(stays))
        def _():
            contrast_stage[i] = result
            contrast_copy(i).start()

        @pl.when(stays)
        def _():
            contrasts[head_here] = result

    def turn(t):
        return lax.rem(member + 1 + t, members)

    def block_pairs(work):
        def one(t, carry):
            work(turn(2 * t), turn(2 * t + 1))
            return carry

        lax.fori_loop(0, members // 2, one, 0)

    def finish_pair(i, k):
        results = finished_block(i), finished_block(k)
        send_block(i, results[0])
        send_block(k, results[1])

    def lands_here(step, source):
        return jnp.logical_and(
            source != member, jnp.where(top(step), 1, source % 2) == tp
        )

    def pass_on(step):
        for ch in range(chunks):
            for source in range(members):

                @pl.when(lands_here(step, source))
                def _(source=source, ch=ch):
                    forward_copy(step, source, ch).wait_recv()

                @pl.when(passes_on(step, source))
                def _(source=source, ch=ch):
                    forward_copy(step, source, ch).start()

    def arrive(step):
        for ch in range(chunks):
            for source in range(members):
                passed = jnp.logical_not(lands_here(step, source))

                @pl.when(jnp.logical_and(awaits(step, source), passed))
                def _(source=source, ch=ch):
                    forward_copy(step, source, ch).wait_recv()

    def attend(step, between):
        band = bands_of[step]

        @pl.when(band == query_band)
        def _():
            for i in range(members):
                if i == members // 2:
                    between()
                attend_block(step, i, i + 1, True)

        @pl.when(band < query_band)
        def _():
            def one(t, carry):
                attend_block(step, turn(2 * t), members, False)
                attend_block(step, turn(2 * t + 1), members, False)

                @pl.when(t == 0)
                def _():
                    between()

                return carry

            lax.fori_loop(0, members // 2, one, 0)

        @pl.when(band > query_band)
        def _():
            between()

    def far_pass_on(step, ch):
        for source in range(members):

            @pl.when(far_passes(source))
            def _(source=source):
                far_pass(step, source, ch).wait_recv()
                far_pass(step, source, ch).start()

    def far_arrive(step, ch):
        for source in range(members):
            passed = jnp.logical_not(far_passes(source))

            @pl.when(jnp.logical_and(far_awaits(source), passed))
            def _(source=source):
                far_pass(step, source, ch).wait_recv()

    loads[0].wait()
    loads[1].wait()
    loads[2].wait()
    pair_first.wait_recv()
    project(0, tuple(range(chunks)))

    loads[3].wait()
    pool_input = jnp.dot(
        rows_in[0].reshape(rows, model), pool_in_w[...], preferred_element_type=f32
    ).astype(bf16)
    rim_stage[...] = pool_input[rows - rim.shape[0] :]

    @pl.when(sp + 1 < sp_count)
    def _():
        rim_copy.start()

    take_swap(0)

    @pl.when(relays)
    def _():
        take_far(2, 0)

    project_swap(0)

    @pl.when(relays)
    def _():
        for load in far_loads:
            load.wait()
        project_far(2, 0)

    take_swap(1)

    @pl.when(relays)
    def _():
        take_far(2, 1)

    project_swap(1)

    @pl.when(relays)
    def _():
        project_far(2, 1)
        take_far(3, 0)

    pass_on(0)

    @pl.when(relays)
    def _():
        project_far(3, 0)

    def query_incoming(source, ch):
        return pltpu.make_async_remote_copy(
            src_ref=query_stage.at[0, 0, :, cut(ch)],
            dst_ref=queries.at[source, :, cut(ch)],
            send_sem=query_send.at[0, 0, ch],
            recv_sem=query_recv.at[source, ch],
            device_id=(sp, other),
            device_id_type=MESH,
        )

    def take_queries():
        for source in range(members):

            @pl.when(jnp.logical_not(jnp.logical_and(source == member, own_goal)))
            def _(source=source):
                for ch in range(chunks):
                    query_incoming(source, ch).wait_recv()

    idle_first = jnp.logical_and(in_upper, jnp.logical_and(side == 1, tp == 0))

    @pl.when(idle_first)
    def _():
        far_pass_on(2, 0)
        far_pass_on(2, 1)

    @pl.when(jnp.logical_and(relays, tp == 1))
    def _():
        take_far(3, 1)

    take_queries()
    arrive(0)

    def last_rows():
        @pl.when(jnp.logical_and(relays, tp == 0))
        def _():
            take_far(3, 1)

        @pl.when(jnp.logical_and(relays, tp == 1))
        def _():
            project_far(3, 1)

    attend(0, last_rows)

    @pl.when(jnp.logical_and(relays, tp == 0))
    def _():
        project_far(3, 1)

    def last_passes():
        @pl.when(jnp.logical_and(in_upper, jnp.logical_and(side == 1, tp == 1)))
        def _():
            far_pass_on(3, 1)

    def nothing():
        pass

    def attend_swapped(between):
        @pl.when(jnp.logical_not(idle_first))
        def _():
            pass_on(1)

        @pl.when(jnp.logical_and(in_upper, side == 1))
        def _():
            far_pass_on(3, 0)

        arrive(1)
        attend(1, between)

    @pl.when(in_upper)
    def _():
        @pl.when(jnp.logical_not(idle_first))
        def _():
            far_pass_on(2, 0)
            far_pass_on(2, 1)

        @pl.when(relays)
        def _():
            attend_swapped(nothing)
            far_pass_on(3, 0)

        far_arrive(2, 0)
        far_arrive(2, 1)

        def one(t, carry):
            attend_block(2, turn(2 * t), members, False)
            attend_block(2, turn(2 * t + 1), members, False)

            @pl.when(jnp.logical_and(t == 0, jnp.logical_and(relays, tp == 1)))
            def _():
                far_pass_on(3, 1)

            @pl.when(jnp.logical_and(t == 0, idle_first))
            def _():
                pass_on(1)

            return carry

        lax.fori_loop(0, members // 2, one, 0)

    @pl.when(jnp.logical_not(relays))
    def _():
        attend_swapped(last_passes)

    for load in loads[6:]:
        load.wait()

    @pl.when(in_lower)
    def _():
        block_pairs(finish_pair)

    @pl.when(in_upper)
    def _():
        @pl.when(tp == 0)
        def _():
            far_pass_on(3, 1)

        far_arrive(3, 0)
        far_arrive(3, 1)

        def last_pair(i, k):
            attend_block(3, i, members, False)
            attend_block(3, k, members, False)
            finish_pair(i, k)

        block_pairs(last_pair)

    @pl.when(sp > 0)
    def _():
        rim_copy.wait_recv()

    @pl.when(sp == 0)
    def _():
        rim[...] = jnp.zeros_like(rim)

    loads[4].wait()
    extended = jnp.concatenate([rim[...], pool_input], axis=0).astype(f32)
    group_width = pool_weight.shape[1]
    skirt = rim.shape[0]
    position = sp * rows + lax.broadcasted_iota(jnp.int32, (rows, group_width), 0)
    mixed = []
    for group in range(pool_weight.shape[0]):
        block = extended[:, group * group_width : (group + 1) * group_width]
        window = block
        reach = 1
        span = 2 ** (1 + group % 4)
        while reach < span:
            window = window + pltpu.roll(window, reach, 0)
            reach *= 2
        counts = jnp.minimum(position + 1, span).astype(f32)
        spread = (window[skirt:] / counts - block[skirt:]).astype(bf16)
        mixed.append(
            jnp.dot(spread, pool_weight[group], preferred_element_type=f32).astype(bf16)
        )
    pool_out = jnp.concatenate(mixed, axis=1)
    for start in range(0, model, chunk):
        pool_part[:, start : start + chunk] = jnp.dot(
            pool_out, pool_out_w[:, start : start + chunk], preferred_element_type=f32
        )

    pair_first.wait_send()
    for ch in range(chunks):
        swap(ch).wait_send()
        pair_copy(1, ch).wait_send()

        @pl.when(crosses)
        def _(ch=ch):
            own_up(ch).wait_send()
            low_up(ch).wait_send()

        @pl.when(relays)
        def _(ch=ch):
            for step in range(2, 4):
                pair_copy(step, ch).wait_send()
                for slot in range(4):

                    @pl.when(jnp.logical_not(far_stays(slot // 2, slot % 2)))
                    def _(step=step, slot=slot):
                        far_copy(step, ch, slot // 2, slot % 2).wait_send()

                @pl.when(own_goal)
                def _(step=step):
                    far_pass(step, member, ch).wait_send()

        @pl.when(in_upper)
        def _(ch=ch):
            for step in range(2, 4):
                for source in range(members):

                    @pl.when(far_passes(source))
                    def _(step=step, source=source):
                        far_pass(step, source, ch).wait_send()

    def drain(step, ch):
        for j in range(2):

            @pl.when(jnp.logical_not(own_stays(step, j)))
            def _(j=j):
                kv_copy(step, j, ch).wait_send()

            @pl.when(jnp.logical_not(query_stays(step, j)))
            def _(j=j):
                query_copy(step, j, ch).wait_send()

        @pl.when(own_forwards(step))
        def _():
            forward_copy(step, member, ch).wait_send()

        for source in range(members):

            @pl.when(passes_on(step, source))
            def _(source=source):
                forward_copy(step, source, ch).wait_send()

    for ch in range(chunks):
        drain(0, ch)
        drain(1, ch)

    @pl.when(sp + 1 < sp_count)
    def _():
        rim_copy.wait_send()

    loads[5].wait()
    def pair_of_heads(plane_side):
        heads = (2 * plane_side, 2 * plane_side + 1)
        for head in heads:

            @pl.when(jnp.logical_not(contrast_local(head)))
            def _(head=head):
                contrast_incoming(head).wait_recv()

        left = jnp.concatenate([contrasts[head] for head in heads], axis=1)
        taken = pl.ds(pl.multiple_of(plane_side * 2 * width, 2 * width), 2 * width)

        def product(span):
            part = jnp.dot(left, contrast_w[taken, span], preferred_element_type=f32)
            return part + pool_part[:, span]

        return product

    spans = [slice(start, start + chunk) for start in range(0, model, chunk)]
    product = pair_of_heads(side)
    for span in spans:
        pool_part[:, span] = product(span)

    product = pair_of_heads(1 - side)
    for span in spans:
        part = product(span)
        low, high = part[:half], part[half:]
        out_stage[:, span] = jnp.where(tp == 0, high, low).astype(bf16)
        out_copy(span.start).start()
        out_ref[:, span] = jnp.where(tp == 0, low, high).astype(bf16)

    for start in range(0, model, chunk):
        out_copy(start).wait()

    for i in range(members):

        @pl.when(jnp.logical_not(contrast_stays(i)))
        def _(i=i):
            contrast_copy(i).wait_send()


def kernel_scratch(members, half, model, width, pool_cols, heads, groups_here):
    bf16 = jnp.bfloat16
    rows = 2 * half
    group_width = pool_cols // groups_here
    dma = pltpu.SemaphoreType.DMA
    return [
        pltpu.VMEM((groups_here, group_width, group_width), bf16),
        pltpu.SMEM((heads,), jnp.float32),
        pltpu.VMEM((1, width), jnp.float32),
        pltpu.VMEM((model, members * width), bf16),
        pltpu.VMEM((model, members * width), bf16),
        pltpu.VMEM((model, members * width), bf16),
        pltpu.VMEM((model, pool_cols), bf16),
        pltpu.VMEM((members * width, model), bf16),
        pltpu.VMEM((pool_cols, model), bf16),
        pltpu.VMEM((4, 2, half, model), bf16),
        pltpu.VMEM((4, members, 2, half, 2 * width), bf16),
        pltpu.VMEM((2, 2, 2, half, 2 * width), bf16),
        pltpu.VMEM((2, 4, 2, half, 2 * width), bf16),
        pltpu.VMEM((members, 2, half, width), bf16),
        pltpu.VMEM((2, 2, 2, half, width), bf16),
        pltpu.VMEM((2, members, rows, 128), jnp.float32),
        pltpu.VMEM((2, members, rows, 128), jnp.float32),
        pltpu.VMEM((2, members, rows, width), jnp.float32),
        pltpu.VMEM((members, rows, width), bf16),
        pltpu.VMEM((members, rows, width), bf16),
        pltpu.VMEM((reach_back + 1, pool_cols), bf16),
        pltpu.VMEM((reach_back + 1, pool_cols), bf16),
        pltpu.VMEM((rows, model), jnp.float32),
        pltpu.VMEM((half, model), bf16),
        dma((11,)),
        dma,
        dma((4, 2)),
        dma((4, 2)),
        dma((4, 2)),
        dma((4, 2)),
        dma((2, 2, 2)),
        dma((2, members, 2)),
        dma((2, members, 2)),
        dma((2, 4, 2)),
        dma((2, members, 2)),
        dma((2, members, 2)),
        dma((2, 2, 2)),
        dma((members, 2)),
        dma((members,)),
        dma((members,)),
        dma,
        dma,
        dma((model // math.gcd(model, 512),)),
        dma((model // math.gcd(model, 512),)),
    ]


vmem_most = 67043328
kernel_grant = 54 * 2**20


def scratch_bytes(scratch):
    return sum(
        math.prod(item.shape) * jnp.dtype(item.dtype).itemsize
        for item in scratch
        if getattr(item, "memory_space", None) == pltpu.VMEM
    )


def whole_layer(
    normed,
    query_weight,
    key_weight,
    value_weight,
    pool_in_weight,
    pool_weight,
    map_balance,
    head_gain,
    contrast_out_weight,
    pool_out_weight,
):
    sp_count = lax.axis_size("sp")
    width = head_gain.shape[0]
    members = query_weight.shape[1] // width
    half, model = normed.shape
    pool_cols = pool_in_weight.shape[1]
    groups_here = pool_weight.shape[0]
    heads = map_balance.shape[0]
    scratch = kernel_scratch(
        max(members, 1), half, model, width, pool_cols, heads, groups_here
    )
    fits = (
        lax.axis_size("tp") == 2
        and members == 4
        and sp_count == 4 * members
        and groups_here % 4 == 0
        and scratch_bytes(scratch) < vmem_most * 3 // 4
    )
    if not fits:
        return per_device(
            normed,
            query_weight,
            key_weight,
            value_weight,
            pool_in_weight,
            pool_weight,
            map_balance,
            head_gain,
            contrast_out_weight,
            pool_out_weight,
        )
    vmem = pl.BlockSpec(memory_space=pltpu.VMEM)
    hbm = pl.BlockSpec(memory_space=pltpu.HBM)
    own_part, partner_part = pl.pallas_call(
        functools.partial(layer_kernel, sp_count, members),
        out_shape=[pltpu.VMEM((half, model), jnp.bfloat16)] * 2,
        in_specs=[hbm] * 10,
        out_specs=[vmem, vmem],
        scratch_shapes=scratch,
        compiler_params=pltpu.CompilerParams(
            collective_id=0, has_side_effects=True, vmem_limit_bytes=kernel_grant
        ),
    )(
        normed,
        pool_weight,
        map_balance,
        head_gain.reshape(1, width),
        query_weight,
        key_weight,
        value_weight,
        pool_in_weight,
        contrast_out_weight,
        pool_out_weight,
    )
    return (own_part.astype(jnp.float32) + partner_part.astype(jnp.float32)).astype(jnp.bfloat16)


def solution(mesh):
    return jax.shard_map(
        whole_layer,
        mesh=mesh,
        in_specs=(
            P(("sp", "tp"), None),
            P(None, "tp"),
            P(None, "tp"),
            P(None, "tp"),
            P(None, "tp"),
            P("tp", None, None),
            P(),
            P(),
            P("tp", None),
            P("tp", None),
        ),
        out_specs=P(("sp", "tp"), None),
        check_vma=False,
    )
```
